256 devices in a mesh: sp: 32 (over z, x), tp: 8 (over y, core).
Axes of the slice: x: 4, y: 4, z: 8, core: 2. Of those that a mesh axis runs over, the one named last changes fastest.
Arguments:
- tokens: bfloat16 [16384, 2048], P(('sp', 'tp')), may hold values from -6 to 6
- norm_gain: float32 [2048], replicated, may hold values from 0.1 to 1.9
- rec_query: bfloat16 [2048, 1024], P(None, 'tp'), may hold values from -0.125 to 0.125
- fwd_gate: bfloat16 [2048, 1024], P(None, 'tp'), may hold values from -0.125 to 0.125
- bwd_gate: bfloat16 [2048, 1024], P(None, 'tp'), may hold values from -0.125 to 0.125
- rec_value: bfloat16 [2048, 1024], P(None, 'tp'), may hold values from -0.125 to 0.125
- gate_leak: float32 [2, 1024], P(None, 'tp'), may hold values from 0 to 0.08, as said below
- log_decay: float32 [2, 16384, 8], P(None, 'sp', 'tp'), may hold values from -2.2 to 0, as said below
- rec_gain: float32 [128], replicated, may hold values from 0.1 to 1.9
- att_query: bfloat16 [2048, 1024], P(None, 'tp'), as said below
- att_key: bfloat16 [2048, 1024], P(None, 'tp')
- att_value: bfloat16 [2048, 1024], P(None, 'tp'), may hold values from -0.125 to 0.125
- lambdas: float32 [8], P('tp'), may hold values from 0.3 to 0.8
- att_gain: float32 [128], replicated, may hold values from 0.1 to 1.9
- out_rec: bfloat16 [1024, 2048], replicated, may hold values from -0.125 to 0.125
- out_att: bfloat16 [1024, 2048], replicated, may hold values from -0.125 to 0.125
Outputs:
- layer_out: bfloat16 [16384, 2048], P(('sp', 'tp'))
The draws below stay inside these ranges and needn't reach their ends.
Inputs may be any that keep to these rules, and one draw needn't show every extreme that they name: `gate_leak`: positive, by direction and channel. `log_decay`: never positive. `att_query`: entries of order 2048 to the power -1/2.
All inputs are finite; a program needn't handle non-finite values.
Results may differ from the reference program's by a relative error of at most 0.011.
Values may be sent and summed in bfloat16 or wider, within the bound.
A program may use at most 128 MiB of HBM per device.

```python
import jax
import jax.numpy as jnp
from jax import lax

D = 2048
HR = 8
HK = 128
HV = 128
HA = 8
AK = 64
AV = 128
BLOCK = 64
TOK_DEV = 512
SEQ = 16384


def draw_gate_leak(key, part):
    pick_key, slow_key, fast_key = jax.random.split(jax.random.fold_in(key, 3), 3)
    slow_share = 0.5
    slow_heads = jax.random.uniform(pick_key, (2, HR, 1), jnp.float32) < slow_share
    slow_rates = jnp.exp(jax.random.uniform(slow_key, (2, HR, HK), jnp.float32, jnp.log(0.3), jnp.log(1.0))) / SEQ
    fast_rates = jnp.exp(jax.random.uniform(fast_key, (2, HR, HK), jnp.float32, jnp.log(0.03), jnp.log(0.08)))
    return jnp.where(slow_heads, slow_rates, fast_rates).reshape(2, HR * HK)


def draw_log_decay(key, part):
    rate_key, spot_key, depth_key = jax.random.split(jax.random.fold_in(key, 5), 3)
    low_rate = 0.3
    high_rate = 1.2
    block_count = SEQ // TOK_DEV
    rates = jnp.exp(jax.random.uniform(rate_key, (2, block_count, 1, HR), jnp.float32, jnp.log(low_rate), jnp.log(high_rate)))
    stable_baseline = jnp.broadcast_to(-rates / SEQ, (2, block_count, TOK_DEV, HR)).reshape(2, SEQ, HR)
    marked_locations = jax.random.randint(spot_key, (2, 3, 1, HR), 0, SEQ)
    layer_depth_list = jax.random.uniform(depth_key, (2, 3, 1, HR), jnp.float32, jnp.log(0.5), jnp.log(0.8))
    token_locations = jnp.arange(SEQ, dtype=jnp.int32)[None, None, :, None]
    spike_events = jnp.sum(jnp.where(token_locations == marked_locations, layer_depth_list, 0.0), axis=1)
    return stable_baseline + spike_events


def attention_pair(key):
    base_key, own_key = jax.random.split(jax.random.fold_in(key, 7), 2)
    columns = HA * 2 * AK
    query_table = jax.random.normal(base_key, (D, columns), jnp.float32) * (3.0 / D) ** 0.5
    key_table = jax.random.normal(own_key, (D, columns), jnp.float32) / D ** 0.5
    return (query_table, key_table)


def draw_att_query(key, part):
    return attention_pair(key)[0].astype(jnp.bfloat16)


def draw_att_key(key, part):
    return attention_pair(key)[1].astype(jnp.bfloat16)


def shard_levels(key, extent, pieces, low, largest):
    factor_of, own = 1.0, jax.random.fold_in(key, 6)
    for dim, blocks in pieces:
        draws = jnp.exp(jax.random.uniform(jax.random.fold_in(own, dim), (blocks,), jnp.float32, low / len(pieces), largest / len(pieces)))
        factor_of = factor_of * jnp.repeat(draws, extent[dim] // blocks).reshape([-1 if axis == dim else 1 for axis in range(len(extent))])
    return factor_of


def bell_draw(rng, extent, deviation, limit, pieces=(), kind=jnp.bfloat16):
    level = shard_levels(rng, extent, pieces, -0.22, 0.18) if pieces else 1.0
    result = jax.random.normal(rng, extent, jnp.float32) * deviation * level
    return jnp.minimum(jnp.maximum(result, -limit), limit).astype(kind)


def setup_inputs(seed: int = 0) -> dict:
    arg_keys = jax.random.split(jax.random.key(seed), 17)
    return {
        "tokens": bell_draw(arg_keys[0], (SEQ, D), 1.0, 6.0, ((0, 256),)),
        "norm_gain": jnp.clip(1.0 + 0.18 * jax.random.normal(arg_keys[1], (D,), jnp.float32), 0.1, 1.9),
        "rec_query": bell_draw(arg_keys[2], (D, HR * HK), D ** -0.5, 0.125, ((1, 8),)),
        "fwd_gate": bell_draw(arg_keys[3], (D, HR * HK), D ** -0.5, 0.125, ((1, 8),)),
        "bwd_gate": bell_draw(arg_keys[4], (D, HR * HK), D ** -0.5, 0.125, ((1, 8),)),
        "rec_value": bell_draw(arg_keys[5], (D, HR * HV), D ** -0.5, 0.125, ((1, 8),)),
        "gate_leak": draw_gate_leak(jax.random.fold_in(arg_keys[16], 71), 0),
        "log_decay": draw_log_decay(jax.random.fold_in(arg_keys[16], 71), 0),
        "rec_gain": jnp.clip(1.0 + 0.18 * jax.random.normal(arg_keys[8], (HV,), jnp.float32), 0.1, 1.9),
        "att_query": draw_att_query(jax.random.fold_in(arg_keys[16], 71), 0),
        "att_key": draw_att_key(jax.random.fold_in(arg_keys[16], 71), 0),
        "att_value": bell_draw(arg_keys[11], (D, HA * AV), D ** -0.5, 0.125, ((1, 8),)),
        "lambdas": jnp.clip(0.3 + 0.5 * jax.random.uniform(arg_keys[12], (HA,), jnp.float32) ** shard_levels(arg_keys[12], (HA,), ((0, 8),), -0.2, 0.2), 0.3, 0.8),
        "att_gain": jnp.clip(1.0 + 0.18 * jax.random.normal(arg_keys[13], (AV,), jnp.float32), 0.1, 1.9),
        "out_rec": bell_draw(arg_keys[14], (HR * HV, D), (HR * HV + HA * AV) ** -0.5, 0.125),
        "out_att": bell_draw(arg_keys[15], (HA * AV, D), (HR * HV + HA * AV) ** -0.5, 0.125),
    }


EPS = 1e-06
THETA = 500000.0
HIGHEST = lax.Precision.HIGHEST

def rms_scale(values, gain):
    return values * lax.rsqrt(lax.optimization_barrier(jnp.mean(values * values, axis=-1, keepdims=True)) + EPS) * gain

def block_recurrence(queries, keys_in, values, log_forget):
    head_count, length, key_width = queries.shape
    value_width = values.shape[-1]
    block_count = length // BLOCK
    block_shape = (head_count, block_count, BLOCK, key_width)
    query_blocks = queries.reshape(block_shape)
    key_blocks = keys_in.reshape(block_shape)
    value_blocks = values.reshape(head_count, block_count, BLOCK, value_width)
    cumulative = jnp.cumsum(log_forget.reshape(block_shape), axis=2)
    middle = cumulative[:, :, BLOCK // 2 - 1:BLOCK // 2]
    block_last = cumulative[:, :, BLOCK - 1:]
    scores = jnp.einsum('hntd,hnsd->hnts', query_blocks * jnp.exp(cumulative - middle), key_blocks * jnp.exp(middle - cumulative), precision=HIGHEST)
    causal_mask = jnp.arange(BLOCK)[:, None] >= jnp.arange(BLOCK)[None, :]
    scores = jnp.where(causal_mask, scores, 0.0)
    within_out = jnp.einsum('hnts,hnsv->hntv', scores, value_blocks, precision=HIGHEST)
    per_block_state = jnp.einsum('hnsd,hnsv->hndv', key_blocks * jnp.exp(block_last - cumulative), value_blocks, precision=HIGHEST)
    block_decay = jnp.exp(block_last[:, :, 0])

    def advance(running, inputs_now):
        factor, added_state = inputs_now
        return (factor[..., None] * running + added_state, running)
    initial = jnp.zeros((head_count, key_width, value_width), jnp.float32)
    end_state, before = lax.scan(advance, initial, (jnp.moveaxis(block_decay, 1, 0), jnp.moveaxis(per_block_state, 1, 0)))
    before = jnp.moveaxis(before, 0, 1)
    carried = jnp.einsum('hntd,hndv->hntv', query_blocks * jnp.exp(cumulative), before, precision=HIGHEST)
    return ((within_out + carried).reshape(head_count, length, value_width), end_state, cumulative)

def rotate(vectors, positions):
    half_width = AK // 2
    frequency = THETA ** (-(jnp.arange(half_width, dtype=jnp.float32) * 2.0 / AK))
    angles = positions[:, None] * frequency[None, :]
    cosine = jnp.cos(angles)[:, None, None, :]
    sines = jnp.sin(angles)[:, None, None, :]
    first_half = vectors[..., :half_width]
    second = vectors[..., half_width:]
    return jnp.concatenate([first_half * cosine - second * sines, second * cosine + first_half * sines], axis=-1)

def reference(tokens, norm_gain, rec_query, fwd_gate, bwd_gate, rec_value, gate_leak, log_decay, rec_gain, att_query, att_key, att_value, lambdas, att_gain, out_rec, out_att):
    normed = rms_scale(tokens.astype(jnp.float32), norm_gain).astype(jnp.bfloat16)

    def project(weight):
        return jnp.dot(normed, weight, preferred_element_type=jnp.float32).astype(jnp.bfloat16)

    def split_heads(table, width):
        return table.astype(jnp.float32).reshape(SEQ, -1, width).transpose(1, 0, 2)
    queries = jax.nn.silu(split_heads(project(rec_query), HK))
    values = split_heads(project(rec_value), HV)
    key_fwd = gate_leak[0].reshape(HR, 1, HK) * jax.nn.sigmoid(-split_heads(project(fwd_gate), HK))
    key_bwd = gate_leak[1].reshape(HR, 1, HK) * jax.nn.sigmoid(-split_heads(project(bwd_gate), HK))
    log_fwd = jnp.log1p(-key_fwd) + log_decay[0].T[:, :, None]
    log_bwd = jnp.log1p(-key_bwd) + log_decay[1].T[:, :, None]
    out_fwd = block_recurrence(queries, key_fwd, values, log_fwd)[0]
    flipped = block_recurrence(jnp.flip(queries, 1), jnp.flip(key_bwd, 1), jnp.flip(values, 1), jnp.flip(log_bwd, 1))[0]
    rec_rows = rms_scale(out_fwd + jnp.flip(flipped, 1), rec_gain)
    rec_rows = rec_rows.transpose(1, 0, 2).reshape(SEQ, HR * HV).astype(jnp.bfloat16)
    positions = jnp.arange(SEQ, dtype=jnp.int32).astype(jnp.float32)
    att_queries = (rotate(project(att_query).astype(jnp.float32).reshape(SEQ, HA, 2, AK), positions) * AK ** (-0.5)).astype(jnp.bfloat16)
    att_keys = rotate(project(att_key).astype(jnp.float32).reshape(SEQ, HA, 2, AK), positions).astype(jnp.bfloat16)
    att_values = project(att_value).reshape(SEQ, HA, AV)

    def attend_head(inputs_now):
        head_queries, head_keys, head_values, weight = inputs_now
        keys_wide = head_keys.astype(jnp.float32)
        values_wide = head_values.astype(jnp.float32)

        def attend_rows(query_block):
            scores = jnp.einsum('qmd,kmd->mqk', query_block.astype(jnp.float32), keys_wide, precision=HIGHEST)
            weights_raw = jnp.exp(scores - lax.optimization_barrier(jnp.max(scores, axis=-1, keepdims=True)))
            totals = lax.optimization_barrier(jnp.sum(weights_raw, axis=-1))
            rounded = lax.optimization_barrier(weights_raw.astype(jnp.bfloat16)).astype(jnp.float32)
            summed = jnp.einsum('mqk,kv->mqv', rounded, values_wide, precision=HIGHEST)
            return summed[0] / totals[0][:, None] - weight * summed[1] / totals[1][:, None]
        blocks = head_queries.reshape(SEQ // TOK_DEV, TOK_DEV, 2, AK)
        return lax.map(attend_rows, blocks).reshape(SEQ, AV)
    mixed_heads = lax.map(attend_head, (jnp.moveaxis(att_queries, 1, 0), jnp.moveaxis(att_keys, 1, 0), jnp.moveaxis(att_values, 1, 0), lambdas))
    att_rows = rms_scale(mixed_heads, att_gain).transpose(1, 0, 2).reshape(SEQ, HA * AV).astype(jnp.bfloat16)
    projected = jnp.dot(rec_rows, out_rec, preferred_element_type=jnp.float32) + jnp.dot(att_rows, out_att, preferred_element_type=jnp.float32)
    return projected.astype(jnp.bfloat16)
```

```python
import math

import jax
import jax.numpy as jnp
import numpy as np
from jax import lax
from jax.experimental import pallas as pl
from jax.experimental.pallas import tpu as pltpu
from jax.sharding import Mesh
from jax.sharding import PartitionSpec as P

HK = 128
AK = 64
BLOCK = 64
SP = ("sp_0", "sp_1")
SP_TP = ("sp_0", "sp_1", "tp")
NZ, NX, NY = 8, 4, 4
ROWS = 64
LEN = 512
D = 2048
NCOL = 896
EPS = 1e-06
THETA = 500000.0
LOG2E = 1.4426950408889634
F32 = jnp.float32
BF16 = jnp.bfloat16
MESH = pl.DeviceIdType.MESH
VMEM_SPEC = pl.BlockSpec(memory_space=pltpu.VMEM)
ANY_SPEC = pl.BlockSpec(memory_space=pl.ANY)
VMEM_LIMIT = 60 * 1024 * 1024


def remote(src, dst, send_sem, recv_sem, device):
    return pltpu.make_async_remote_copy(
        src_ref=src,
        dst_ref=dst,
        send_sem=send_sem,
        recv_sem=recv_sem,
        device_id=device,
        device_id_type=MESH,
    )


def meet(devices):
    barrier = pltpu.get_barrier_semaphore()
    for device in devices:
        pl.semaphore_signal(barrier, inc=1, device_id=device, device_id_type=MESH)
    pl.semaphore_wait(barrier, len(devices))


def dot(a, b):
    return jnp.dot(a, b, preferred_element_type=F32)


def dot_nt(a, b):
    return lax.dot_general(a, b, (((1,), (1,)), ((), ())), preferred_element_type=F32)


def project_kernel(
    tok_ref, gain_ref, cos_a, sin_a, cos_b, sin_b, *refs
):
    weights = refs[:7]
    qt_ref, kv_ref, rec_ref = refs[7:10]
    xbuf, wbuf, attbuf, wsem, send, recv = refs[10:]
    t = lax.axis_index("tp")
    y, c = t // 2, t % 2
    right = lax.rem(y + 1, NY) * 2 + c
    left = lax.rem(y + NY - 1, NY) * 2 + c
    far = lax.rem(y + 2, NY) * 2 + c
    partner = 2 * y + 1 - c

    loads = [
        pltpu.make_async_copy(w, wbuf.at[:, pl.ds(128 * k, 128)], wsem.at[k])
        for k, w in enumerate(weights)
    ]
    for load in loads:
        load.start()
    meet([{"tp": right}, {"tp": left}, {"tp": partner}])

    half = ROWS // 2
    part = (pl.ds(0, half), pl.ds(half, half))
    own = [tok_ref.at[p] for p in part]

    def to(src, slot, k, number, device):
        return remote(src, xbuf.at[slot, part[k]], send.at[number], recv.at[number], {"tp": device})

    copies = {}

    def launch(src, slot, k, number, device):
        copies[number] = to(src, slot, k, number, device)
        copies[number].start()

    launch(own[0], t, 0, 0, right)
    launch(own[1], t, 1, 3, left)
    launch(own[1], t, 1, 1, right)
    launch(own[0], t, 0, 2, left)
    launch(own[0], t, 0, 4, partner)
    launch(own[1], t, 1, 5, partner)

    def arrived(slot, k, number):
        to(own[k], slot, k, number, right).wait_recv()

    xbuf[t] = tok_ref[...]
    for load in loads:
        load.wait()

    z, x = lax.axis_index("sp_0"), lax.axis_index("sp_1")
    block = z * NX + x
    cb = cos_b[pl.ds(block, 1), :]
    sb = sin_b[pl.ds(block, 1), :]
    lane = lax.broadcasted_iota(jnp.int32, (1, 128), 1)
    low = lax.rem(lane, 64) < 32

    def turned(v, cosine, sine):
        other = jnp.where(low, pltpu.roll(v, 96, 1), pltpu.roll(v, 32, 1))
        return v * cosine + other * sine

    def process(yy):
        pair = xbuf[pl.ds(2 * yy, 2)].reshape(2 * ROWS, D).astype(F32)
        scale = lax.rsqrt(jnp.mean(pair * pair, axis=1, keepdims=True) + EPS)
        normed = (pair * scale * gain_ref[...]).astype(BF16)
        out = dot(normed, wbuf[...])
        rows = pl.ds(pl.multiple_of(yy * 128, 128), 128)
        rec_ref[rows, :] = out[:, :512].astype(BF16)
        ca, sa = cos_a[rows, :], sin_a[rows, :]
        cosine = ca * cb - sa * sb
        sine = sa * cb + ca * sb
        signed = jnp.where(low, -sine, sine)
        raw = out[:, 512:].astype(BF16).astype(F32)
        attbuf[0, rows, :] = turned(raw[:, 0:128], cosine, signed) * (AK**-0.5 * LOG2E)
        attbuf[1, rows, :] = turned(raw[:, 128:256], cosine, signed)
        attbuf[2, rows, :] = raw[:, 256:384]

    slot_l, slot_r = left, right
    arrived(partner, 0, 4)
    arrived(partner, 1, 5)
    process(y)

    arrived(slot_l, 0, 0)
    launch(xbuf.at[slot_l, part[0]], slot_l, 0, 6, right)
    launch(xbuf.at[slot_l, part[0]], slot_l, 0, 8, partner)
    arrived(slot_r, 1, 3)
    launch(xbuf.at[slot_r, part[1]], slot_r, 1, 7, left)
    launch(xbuf.at[slot_r, part[1]], slot_r, 1, 9, partner)
    arrived(slot_l, 1, 1)
    launch(xbuf.at[slot_l, part[1]], slot_l, 1, 10, partner)
    arrived(slot_r, 0, 2)
    launch(xbuf.at[slot_r, part[0]], slot_r, 0, 11, partner)
    mate_l, mate_r, mate_far = left + 1 - 2 * c, right + 1 - 2 * c, far + 1 - 2 * c
    arrived(mate_l, 0, 8)
    arrived(mate_l, 1, 10)
    process(left // 2)
    arrived(mate_r, 1, 9)
    arrived(mate_r, 0, 11)
    process(right // 2)
    arrived(far, 0, 6)
    launch(xbuf.at[far, part[0]], far, 0, 12, partner)
    arrived(far, 1, 7)
    launch(xbuf.at[far, part[1]], far, 1, 13, partner)
    arrived(mate_far, 0, 12)
    arrived(mate_far, 1, 13)
    process(far // 2)

    qt_ref[...] = attbuf[0].T.astype(BF16)
    value_t = attbuf[2].T.astype(BF16)
    for s in range(2):
        kv_ref[s, 0:256, :] = attbuf[1, 256 * s : 256 * (s + 1), :].astype(BF16)
        kv_ref[s, 256:384, :] = value_t[:, 256 * s : 256 * s + 128]
        kv_ref[s, 384:512, :] = value_t[:, 256 * s + 128 : 256 * s + 256]
    for number in range(14):
        copies[number].wait_send()


def rotary_tables():
    i = np.arange(AK // 2, dtype=np.float64)
    freq = THETA ** (-(i * 2.0 / AK))
    freq = np.tile(freq, 4)[None, :]
    within = np.arange(LEN, dtype=np.float64)[:, None] * freq
    starts = np.arange(NZ * NX, dtype=np.float64)[:, None] * LEN * freq
    return [
        jnp.asarray(f(v).astype(np.float32)) for v in (within, starts) for f in (np.cos, np.sin)
    ]


def project(tokens, norm_gain, weights):
    cos_a, sin_a, cos_b, sin_b = rotary_tables()
    return pl.pallas_call(
        project_kernel,
        out_shape=(
            jax.ShapeDtypeStruct((128, LEN), BF16),
            jax.ShapeDtypeStruct((2, 512, 128), BF16),
            jax.ShapeDtypeStruct((LEN, 512), BF16),
        ),
        in_specs=[VMEM_SPEC] * 6 + [ANY_SPEC] * 7,
        out_specs=(VMEM_SPEC,) * 3,
        scratch_shapes=[
            pltpu.VMEM((8, ROWS, D), BF16),
            pltpu.VMEM((D, NCOL), BF16),
            pltpu.VMEM((3, LEN, 128), F32),
            pltpu.SemaphoreType.DMA((7,)),
            pltpu.SemaphoreType.DMA((14,)),
            pltpu.SemaphoreType.DMA((14,)),
        ],
        compiler_params=pltpu.CompilerParams(
            collective_id=0, has_side_effects=True, vmem_limit_bytes=VMEM_LIMIT
        ),
        name="gather_project",
    )(tokens, norm_gain.reshape(1, D), cos_a, sin_a, cos_b, sin_b, *weights)


def exact_cumulative(triangle, logs):
    first = logs.astype(BF16)
    rest = logs - first.astype(F32)
    second = rest.astype(BF16)
    third = (rest - second.astype(F32)).astype(BF16)
    return dot(triangle, first) + dot(triangle, second) + dot(triangle, third)


def recurrence_kernel(rec_ref, leak_ref, decay_ref, out_ref, read_ref, state_ref):
    blocks = LEN // BLOCK
    raw_q = rec_ref[:, 0:128].astype(F32)
    rq = raw_q / (1.0 + jnp.exp(-raw_q))
    value = rec_ref[:, 384:512]
    value_t = value.astype(F32).T.astype(BF16)
    row = lax.broadcasted_iota(jnp.int32, (256, 256), 0)
    col = lax.broadcasted_iota(jnp.int32, (256, 256), 1)
    same = (row // BLOCK) == (col // BLOCK)
    upper = lax.broadcasted_iota(jnp.int32, (128, 1), 0) < BLOCK
    total_out = None
    for side in range(2):
        raw = rec_ref[:, 128 * (side + 1) : 128 * (side + 2)].astype(F32)
        key = leak_ref[side : side + 1, :] / (1.0 + jnp.exp(raw))
        logs = jnp.log1p(-key) + decay_ref[side]
        mask = same & ((row >= col) if side == 0 else (row <= col))
        triangle = mask.astype(F32).astype(BF16)
        cum = jnp.concatenate(
            [exact_cumulative(triangle, logs[256 * h : 256 * (h + 1)]) for h in range(2)], axis=0
        )
        cum3 = cum.reshape(blocks, BLOCK, 128)
        at_mid, at_last = (BLOCK // 2 - 1, BLOCK - 1) if side == 0 else (BLOCK // 2, 0)
        middle = cum3[:, at_mid : at_mid + 1, :]
        last = cum3[:, at_last : at_last + 1, :]
        key3, rq3 = key.reshape(cum3.shape), rq.reshape(cum3.shape)
        qs = (rq3 * jnp.exp(cum3 - middle)).reshape(LEN, 128).astype(BF16)
        ks = (key3 * jnp.exp(middle - cum3)).reshape(LEN, 128).astype(BF16)
        kl = (key3 * jnp.exp(last - cum3)).reshape(LEN, 128)
        qc = (rq3 * jnp.exp(cum3)).reshape(LEN, 128).astype(BF16)
        within = []
        for h in range(2):
            part = slice(256 * h, 256 * (h + 1))
            scores = jnp.where(mask, dot_nt(qs[part], ks[part]), 0.0).astype(BF16)
            within.append(dot(scores, value[part]))
        order = range(blocks) if side == 0 else reversed(range(blocks))
        state = jnp.zeros((128, 128), F32)
        carried, before = [None] * blocks, [None] * blocks
        running = jnp.zeros((1, 128), F32)
        for b in order:
            carried[b] = dot_nt(qc[BLOCK * b : BLOCK * (b + 1)], state.astype(BF16))
            pair = b // 2
            keys = kl[128 * pair : 128 * (pair + 1)]
            keys = jnp.where(upper if b % 2 == 0 else ~upper, keys, 0.0).astype(BF16)
            added = dot(value_t[:, 128 * pair : 128 * (pair + 1)], keys)
            before[b] = running
            running = running + last[b]
            state = state * jnp.exp(last[b]) + added
        out = jnp.concatenate(within, axis=0) + jnp.concatenate(carried, axis=0)
        total_out = out if total_out is None else total_out + out
        reach = (cum3 + jnp.stack(before, axis=0)).reshape(LEN, 128)
        read_ref[side] = (rq * jnp.exp(reach)).astype(BF16)
        state_ref[side, 0:128, :] = state.astype(BF16)
        state_ref[side, 128:144, :] = jnp.broadcast_to(jnp.exp(running), (16, 128)).astype(BF16)
    out_ref[...] = total_out


def recurrence(rec, gate_leak, log_decay):
    return pl.pallas_call(
        recurrence_kernel,
        out_shape=(
            jax.ShapeDtypeStruct((LEN, 128), F32),
            jax.ShapeDtypeStruct((2, LEN, 128), BF16),
            jax.ShapeDtypeStruct((2, 144, 128), BF16),
        ),
        in_specs=[VMEM_SPEC] * 3,
        out_specs=(VMEM_SPEC,) * 3,
        compiler_params=pltpu.CompilerParams(vmem_limit_bytes=VMEM_LIMIT),
        name="local_recurrence",
    )(rec, gate_leak, log_decay)


def mix_kernel(
    qt_ref, kv_ref, recout_ref, read_ref, state_ref, lam_ref, attgain_ref, recgain_ref,
    mixed_ref,
    kvbuf, qbuf, qz, acc, peak, sendo, recvo, sendm, recvm, stbuf, totals, inside, chain_in, chain_out,
    r_send, r_recv, l_send, l_recv, q_send, q_recv, o_send, o_recv, m_send, m_recv, s_send, s_recv,
    c_send, c_recv,
):
    z, x = lax.axis_index("sp_0"), lax.axis_index("sp_1")
    up = {"sp_0": lax.rem(z + 1, NZ)}
    down = {"sp_0": lax.rem(z + NZ - 1, NZ)}
    beside = [None] + [{"sp_1": lax.rem(x + p, NX)} for p in range(1, NX)]
    meet([up, down] + beside[1:])

    ring = {}

    def rightward(step, s):
        src = kv_ref.at[s] if step == 0 else kvbuf.at[NZ - step, s]
        return remote(
            src, kvbuf.at[NZ - 1 - step, s], r_send.at[step, s], r_recv.at[step, s], up
        )

    def leftward(step, s):
        src = kv_ref.at[s] if step == 0 else kvbuf.at[step, s]
        return remote(src, kvbuf.at[step + 1, s], l_send.at[step, s], l_recv.at[step, s], down)

    def start_right(step, s):
        ring["r", step, s] = rightward(step, s)
        ring["r", step, s].start()

    def start_left(step, s):
        ring["l", step, s] = leftward(step, s)
        ring["l", step, s].start()

    q_copies = [
        remote(qt_ref, qbuf.at[NX - p], q_send.at[p], q_recv.at[NX - p], beside[p])
        for p in range(1, NX)
    ]
    s_copies = [
        remote(state_ref, stbuf.at[NX - p], s_send.at[p], s_recv.at[NX - p], beside[p])
        for p in range(1, NX)
    ]
    for copy in q_copies:
        copy.start()
    for s in range(2):
        start_right(0, s)
        start_left(0, s)
    for copy in s_copies:
        copy.start()

    kvbuf[0] = kv_ref[...]
    stbuf[0] = state_ref[...]
    upper = lax.broadcasted_iota(jnp.int32, (128, 1), 0) < AK

    def spread(p, source):
        for h in range(2):
            piece = source[:, 256 * h : 256 * (h + 1)].astype(F32)
            qz[p, h] = jnp.where(upper, piece, 0.0).astype(BF16)
            qz[p, 2 + h] = jnp.where(upper, 0.0, piece).astype(BF16)

    ones = jnp.ones((16, 256), BF16)

    def flash(p, slots, first):
        def tile(k, carry):
            query = qz[p, k]
            scores = [
                dot(kvbuf[r, s, 0:256, :], query) for r in slots for s in range(2)
            ]
            top = None
            for piece in scores:
                here = jnp.max(piece, axis=0, keepdims=True)
                top = here if top is None else jnp.maximum(top, here)
            if not first:
                old = peak[p, k, 0:1, :]
                top = jnp.maximum(top, old)
            weights = [jnp.exp2(piece - top).astype(BF16) for piece in scores]
            summed = None
            n = 0
            for r in slots:
                for s in range(2):
                    values = jnp.concatenate(
                        [kvbuf[r, s, 256:384, :], kvbuf[r, s, 384:512, :]], axis=1
                    )
                    values = jnp.concatenate([values, ones], axis=0)
                    term = dot(values, weights[n])
                    summed = term if summed is None else summed + term
                    n += 1
            if first:
                acc[p, k] = summed
            else:
                acc[p, k] = acc[p, k] * jnp.exp2(old - top) + summed
            peak[p, k] = jnp.broadcast_to(top, (8, 256))
            return carry

        lax.fori_loop(0, 4, tile, 0)

    spread(0, qt_ref[...])
    flash(0, (0,), True)
    for p in range(1, NX):
        q_copies[NX - p - 1].wait_recv()
        spread(p, qbuf[p])

    def forward(step):
        for s in range(2):
            rightward(step - 1, s).wait_recv()
            if step < 3 or s == 0:
                start_right(step, s)
            leftward(step - 1, s).wait_recv()
            if step < 3 or s == 1:
                start_left(step, s)

    forward(1)
    for p in range(1, NX):
        s_copies[NX - p - 1].wait_recv()

    for side in range(2):
        order = range(NX) if side == 0 else reversed(range(NX))
        total_s, total_d = jnp.zeros((128, 128), F32), jnp.ones((1, 128), F32)
        inside_s, inside_d = total_s, total_d
        for k in order:
            rel = lax.rem(k - x + NX, NX)
            piece_s = stbuf[rel, side, 0:128, :].astype(F32)
            piece_d = stbuf[rel, side, 128:144, :].astype(F32)[0:1, :]
            total_s = total_s * piece_d + piece_s
            total_d = total_d * piece_d
            passed = (k < x) if side == 0 else (k > x)
            inside_s = jnp.where(passed, total_s, inside_s)
            inside_d = jnp.where(passed, total_d, inside_d)
        totals[side, 0:128, :] = total_s
        totals[side, 128:136, :] = jnp.broadcast_to(total_d, (8, 128))
        inside[side, 0:128, :] = inside_s
        inside[side, 128:136, :] = jnp.broadcast_to(inside_d, (8, 128))

    @pl.when(z == 0)
    def _():
        chain_in[0] = jnp.zeros((128, 128), F32)

    @pl.when(z == NZ - 1)
    def _():
        chain_in[1] = jnp.zeros((128, 128), F32)

    def chain_copy(side):
        return remote(
            chain_out.at[side], chain_in.at[side], c_send.at[side], c_recv.at[side],
            up if side == 0 else down,
        )

    def chain(hop):
        for side in range(2):
            turn = (z == hop) if side == 0 else (z == NZ - 1 - hop)

            @pl.when(turn)
            def _():
                if hop > 0:
                    chain_copy(side).wait_recv()
                if hop < NZ - 1:
                    chain_out[side] = (
                        chain_in[side] * totals[side, 128:129, :] + totals[side, 0:128, :]
                    )
                    chain_copy(side).start()

    chain(0)
    for p in range(1, NX):
        flash(p, (0, 7, 1), True)
        chain(p)
    flash(0, (7, 1), False)
    forward(2)
    chain(4)
    for p in range(NX):
        flash(p, (6, 2), False)
        if p < 3:
            chain(5 + p)
    forward(3)
    rightward(3, 0).wait_recv()
    leftward(3, 1).wait_recv()

    o_copies = {}
    for p in (2, 1, 3):
        flash(p, (5, 3, 4), False)
        for k in range(4):
            inverse = 1.0 / acc[p, k, 128:129, :]
            sendo[p, k] = (acc[p, k, 0:128, :] * inverse).astype(BF16)
            sendm[p, k, 0:8, :] = peak[p, k]
            sendm[p, k, 8:16, :] = acc[p, k, 128:136, :]
        o_copies[p] = (
            remote(sendo.at[p], recvo.at[NX - p], o_send.at[p], o_recv.at[NX - p], beside[p]),
            remote(sendm.at[p], recvm.at[NX - p], m_send.at[p], m_recv.at[NX - p], beside[p]),
        )
        for copy in o_copies[p]:
            copy.start()
    flash(0, (5, 3, 4), False)

    out = recout_ref[...]
    for side in range(2):
        entry = chain_in[side] * inside[side, 128:129, :] + inside[side, 0:128, :]
        out = out + dot_nt(read_ref[side], entry.astype(BF16))
    out = out * lax.rsqrt(jnp.mean(out * out, axis=1, keepdims=True) + EPS) * recgain_ref[...]
    mixed_ref[:, 0:128] = out.astype(BF16)

    for p in (2, 3, 1):
        for copy in o_copies[NX - p]:
            copy.wait_recv()
    lam = lam_ref[0:1, 0:1]
    for h in range(2):
        maps = []
        for m in range(2):
            k = 2 * m + h
            tops = [peak[0, k, 0:1, :]] + [recvm[p, k, 0:1, :] for p in range(1, NX)]
            sums = [acc[0, k, 128:129, :]] + [recvm[p, k, 8:9, :] for p in range(1, NX)]
            top = tops[0]
            for other in tops[1:]:
                top = jnp.maximum(top, other)
            shares = [a * jnp.exp2(b - top) for a, b in zip(sums, tops)]
            whole = shares[0] + shares[1] + shares[2] + shares[3]
            inverse = 1.0 / whole
            value = acc[0, k, 0:128, :] * (jnp.exp2(tops[0] - top) * inverse)
            for p in range(1, NX):
                value = value + recvo[p, k].astype(F32) * (shares[p] * inverse)
            maps.append(value)
        mixed = maps[0] - lam * maps[1]
        mixed = mixed * lax.rsqrt(jnp.mean(mixed * mixed, axis=0, keepdims=True) + EPS)
        mixed = mixed * attgain_ref[...]
        mixed_ref[256 * h : 256 * (h + 1), 128:256] = mixed.T.astype(BF16)

    for copy in ring.values():
        copy.wait_send()
    for copy in q_copies + s_copies:
        copy.wait_send()
    for pair in o_copies.values():
        for copy in pair:
            copy.wait_send()

    @pl.when(z < NZ - 1)
    def _():
        chain_copy(0).wait_send()

    @pl.when(z > 0)
    def _():
        chain_copy(1).wait_send()


def mix(qt, kv, recout, read, state, lambdas, att_gain, rec_gain):
    dma = pltpu.SemaphoreType.DMA
    return pl.pallas_call(
        mix_kernel,
        out_shape=jax.ShapeDtypeStruct((LEN, 256), BF16),
        in_specs=[VMEM_SPEC] * 8,
        out_specs=VMEM_SPEC,
        scratch_shapes=[
            pltpu.VMEM((NZ, 2, 512, 128), BF16),
            pltpu.VMEM((NX, 128, LEN), BF16),
            pltpu.VMEM((NX, 4, 128, 256), BF16),
            pltpu.VMEM((NX, 4, 144, 256), F32),
            pltpu.VMEM((NX, 4, 8, 256), F32),
            pltpu.VMEM((NX, 4, 128, 256), BF16),
            pltpu.VMEM((NX, 4, 128, 256), BF16),
            pltpu.VMEM((NX, 4, 16, 256), F32),
            pltpu.VMEM((NX, 4, 16, 256), F32),
            pltpu.VMEM((NX, 2, 144, 128), BF16),
            pltpu.VMEM((2, 136, 128), F32),
            pltpu.VMEM((2, 136, 128), F32),
            pltpu.VMEM((2, 128, 128), F32),
            pltpu.VMEM((2, 128, 128), F32),
            dma((4, 2)), dma((4, 2)), dma((4, 2)), dma((4, 2)),
            dma((NX,)), dma((NX,)), dma((NX,)), dma((NX,)), dma((NX,)), dma((NX,)),
            dma((NX,)), dma((NX,)), dma((2,)), dma((2,)),
        ],
        compiler_params=pltpu.CompilerParams(
            collective_id=1, has_side_effects=True, vmem_limit_bytes=VMEM_LIMIT
        ),
        name="attend_and_link",
    )(
        qt, kv, recout, read, state, lambdas.reshape(1, 1), att_gain.reshape(128, 1),
        rec_gain.reshape(1, 128),
    )


def output_kernel(mixed_ref, wrec_ref, watt_ref, out_ref, got, wr, wa, wsem, send, recv):
    t = lax.axis_index("tp")
    loads = [
        pltpu.make_async_copy(wrec_ref, wr, wsem.at[0]),
        pltpu.make_async_copy(watt_ref, wa, wsem.at[1]),
    ]
    for load in loads:
        load.start()
    others = [lax.rem(t + k, 8) for k in range(1, 8)]
    meet([{"tp": o} for o in others])
    copies = []
    for k, o in enumerate(others):
        rows = pl.ds(pl.multiple_of(o * ROWS, ROWS), ROWS)
        copies.append(
            remote(mixed_ref.at[rows, :], got.at[7 - k], send.at[k], recv.at[7 - k], {"tp": o})
        )
        copies[-1].start()
    mine = pl.ds(pl.multiple_of(t * ROWS, ROWS), ROWS)
    got[0] = mixed_ref[mine, :]
    for load in loads:
        load.wait()
    total = None
    for k in range(8):
        if k > 0:
            remote(
                mixed_ref.at[mine, :], got.at[k], send.at[0], recv.at[k], {"tp": others[0]}
            ).wait_recv()
        source = lax.rem(t + k, 8)
        rows = pl.ds(pl.multiple_of(source * 128, 128), 128)
        term = dot(got[k, :, 0:128], wr[rows, :]) + dot(got[k, :, 128:256], wa[rows, :])
        total = term if total is None else total + term
    out_ref[...] = total.astype(BF16)
    for copy in copies:
        copy.wait_send()


def output(mixed, out_rec, out_att):
    dma = pltpu.SemaphoreType.DMA
    return pl.pallas_call(
        output_kernel,
        out_shape=jax.ShapeDtypeStruct((ROWS, D), BF16),
        in_specs=[VMEM_SPEC, ANY_SPEC, ANY_SPEC],
        out_specs=VMEM_SPEC,
        scratch_shapes=[
            pltpu.VMEM((8, ROWS, 256), BF16),
            pltpu.VMEM((1024, D), BF16),
            pltpu.VMEM((1024, D), BF16),
            dma((2,)), dma((8,)), dma((8,)),
        ],
        compiler_params=pltpu.CompilerParams(
            collective_id=2, has_side_effects=True, vmem_limit_bytes=VMEM_LIMIT
        ),
        name="exchange_output",
    )(mixed, out_rec, out_att)


def on_device(
    tokens, norm_gain, rec_query, fwd_gate, bwd_gate, rec_value, gate_leak, log_decay, rec_gain,
    att_query, att_key, att_value, lambdas, att_gain, out_rec, out_att,
):
    weights = (rec_query, fwd_gate, bwd_gate, rec_value, att_query, att_key, att_value)
    qt, kv, rec = project(tokens, norm_gain, weights)
    recout, read, state = recurrence(rec, gate_leak, log_decay)
    mixed = mix(qt, kv, recout, read, state, lambdas, att_gain, rec_gain)
    return output(mixed, out_rec, out_att)


def solution(mesh):
    torus = Mesh(mesh.devices.reshape(NZ, NX, mesh.shape["tp"]), SP_TP)
    tp = P(None, "tp")
    in_specs = (
        P(SP_TP, None), P(), tp, tp, tp, tp, tp, P(None, SP, "tp"), P(), tp, tp, tp, P("tp"), P(),
        P(), P(),
    )
    return jax.shard_map(
        on_device, mesh=torus, in_specs=in_specs, out_specs=P(SP_TP, None), check_vma=False
    )
```

```python
import math

import jax
import jax.numpy as jnp
import numpy as np
from jax import lax
from jax.experimental import pallas as pl
from jax.experimental.pallas import tpu as pltpu
from jax.sharding import Mesh
from jax.sharding import PartitionSpec as P

HK = 128
AK = 64
BLOCK = 64
SP = ("sp_0", "sp_1")
SP_TP = ("sp_0", "sp_1", "tp")
NZ, NX, NY = 8, 4, 4
ROWS = 64
LEN = 512
D = 2048
NCOL = 896
EPS = 1e-06
THETA = 500000.0
LOG2E = 1.4426950408889634
F32 = jnp.float32
BF16 = jnp.bfloat16
MESH = pl.DeviceIdType.MESH
VMEM_SPEC = pl.BlockSpec(memory_space=pltpu.VMEM)
ANY_SPEC = pl.BlockSpec(memory_space=pl.ANY)
VMEM_LIMIT = 60 * 1024 * 1024


def remote(src, dst, send_sem, recv_sem, device):
    return pltpu.make_async_remote_copy(
        src_ref=src,
        dst_ref=dst,
        send_sem=send_sem,
        recv_sem=recv_sem,
        device_id=device,
        device_id_type=MESH,
    )


def meet(devices):
    barrier = pltpu.get_barrier_semaphore()
    for device in devices:
        pl.semaphore_signal(barrier, inc=1, device_id=device, device_id_type=MESH)
    pl.semaphore_wait(barrier, len(devices))


def dot(a, b):
    return jnp.dot(a, b, preferred_element_type=F32)


def dot_nt(a, b):
    return lax.dot_general(a, b, (((1,), (1,)), ((), ())), preferred_element_type=F32)


def rotary_tables():
    i = np.arange(AK // 2, dtype=np.float64)
    freq = THETA ** (-(i * 2.0 / AK))
    freq = np.tile(freq, 4)[None, :]
    within = np.arange(LEN, dtype=np.float64)[:, None] * freq
    starts = np.arange(NZ * NX, dtype=np.float64)[:, None] * LEN * freq
    return [
        jnp.asarray(f(v).astype(np.float32)) for v in (within, starts) for f in (np.cos, np.sin)
    ]


def exact_cumulative(triangle, logs):
    first = logs.astype(BF16)
    rest = logs - first.astype(F32)
    second = rest.astype(BF16)
    third = (rest - second.astype(F32)).astype(BF16)
    return dot(triangle, first) + dot(triangle, second) + dot(triangle, third)


def recurrence(rec_ref, leak_ref, decay_ref, out_ref, read_ref, state_ref):
    blocks = LEN // BLOCK
    raw_q = rec_ref[:, 0:128].astype(F32)
    rq = raw_q / (1.0 + jnp.exp(-raw_q))
    value = rec_ref[:, 384:512]
    value_t = value.astype(F32).T.astype(BF16)
    row = lax.broadcasted_iota(jnp.int32, (256, 256), 0)
    col = lax.broadcasted_iota(jnp.int32, (256, 256), 1)
    same = (row // BLOCK) == (col // BLOCK)
    upper = lax.broadcasted_iota(jnp.int32, (128, 1), 0) < BLOCK
    total_out = None
    for side in range(2):
        raw = rec_ref[:, 128 * (side + 1) : 128 * (side + 2)].astype(F32)
        key = leak_ref[side : side + 1, :] / (1.0 + jnp.exp(raw))
        added_log = jnp.broadcast_to(decay_ref[side : side + 1, :], (128, LEN)).T
        logs = jnp.log1p(-key) + added_log
        mask = same & ((row >= col) if side == 0 else (row <= col))
        triangle = mask.astype(F32).astype(BF16)
        cum = jnp.concatenate(
            [exact_cumulative(triangle, logs[256 * h : 256 * (h + 1)]) for h in range(2)], axis=0
        )
        cum3 = cum.reshape(blocks, BLOCK, 128)
        at_mid, at_last = (BLOCK // 2 - 1, BLOCK - 1) if side == 0 else (BLOCK // 2, 0)
        middle = cum3[:, at_mid : at_mid + 1, :]
        last = cum3[:, at_last : at_last + 1, :]
        key3, rq3 = key.reshape(cum3.shape), rq.reshape(cum3.shape)
        qs = (rq3 * jnp.exp(cum3 - middle)).reshape(LEN, 128).astype(BF16)
        ks = (key3 * jnp.exp(middle - cum3)).reshape(LEN, 128).astype(BF16)
        kl = (key3 * jnp.exp(last - cum3)).reshape(LEN, 128)
        qc = (rq3 * jnp.exp(cum3)).reshape(LEN, 128).astype(BF16)
        within = []
        for h in range(2):
            part = slice(256 * h, 256 * (h + 1))
            scores = jnp.where(mask, dot_nt(qs[part], ks[part]), 0.0).astype(BF16)
            within.append(dot(scores, value[part]))
        order = range(blocks) if side == 0 else reversed(range(blocks))
        state = jnp.zeros((128, 128), F32)
        carried, before = [None] * blocks, [None] * blocks
        running = jnp.zeros((1, 128), F32)
        for b in order:
            carried[b] = dot_nt(qc[BLOCK * b : BLOCK * (b + 1)], state.astype(BF16))
            pair = b // 2
            keys = kl[128 * pair : 128 * (pair + 1)]
            keys = jnp.where(upper if b % 2 == 0 else ~upper, keys, 0.0).astype(BF16)
            added = dot(value_t[:, 128 * pair : 128 * (pair + 1)], keys)
            before[b] = running
            running = running + last[b]
            state = state * jnp.exp(last[b]) + added
        out = jnp.concatenate(within, axis=0) + jnp.concatenate(carried, axis=0)
        total_out = out if total_out is None else total_out + out
        reach = (cum3 + jnp.stack(before, axis=0)).reshape(LEN, 128)
        read_ref[side] = (rq * jnp.exp(reach)).astype(BF16)
        state_ref[side, 0:128, :] = state.astype(BF16)
        state_ref[side, 128:144, :] = jnp.broadcast_to(jnp.exp(running), (16, 128)).astype(BF16)
    out_ref[...] = total_out


def flash(jobs, kvbuf, qz, acc, peak):
    ones = jnp.ones((16, 256), BF16)
    tiles = [(q, k, pieces, first) for q, pieces, first in jobs for k in range(4)]
    count = len(tiles)
    tops, olds, sums = [None] * count, [None] * count, [None] * count
    scores, weights = [{} for _ in tiles], [{} for _ in tiles]

    def score(i, n):
        if not (0 <= i < count and n < len(tiles[i][2])):
            return
        q, k, pieces, first = tiles[i]
        if n == 0 and not first:
            olds[i] = tops[i] = peak[q, k, 0:1, :]
        r, s = pieces[n]
        scores[i][n] = dot(kvbuf[r, s, 0:256, :], qz[q, k])
        here = jnp.max(scores[i][n], axis=0, keepdims=True)
        tops[i] = here if tops[i] is None else jnp.maximum(tops[i], here)

    def weigh(i, n):
        if not (0 <= i < count and n < len(tiles[i][2])):
            return
        weights[i][n] = jnp.exp2(scores[i].pop(n) - tops[i]).astype(BF16)

    def gather(i, n):
        if not (0 <= i < count and n < len(tiles[i][2])):
            return
        q, k, pieces, first = tiles[i]
        r, s = pieces[n]
        values = jnp.concatenate([kvbuf[r, s, 256:384, :], kvbuf[r, s, 384:512, :]], axis=1)
        term = dot(jnp.concatenate([values, ones], axis=0), weights[i].pop(n))
        sums[i] = term if sums[i] is None else sums[i] + term
        if n == len(pieces) - 1:
            if first:
                acc[q, k] = sums[i]
            else:
                acc[q, k] = acc[q, k] * jnp.exp2(olds[i] - tops[i]) + sums[i]
            peak[q, k] = jnp.broadcast_to(tops[i], (8, 256))

    longest = max(len(t[2]) for t in tiles)
    for i in range(-2, count):
        for n in range(longest):
            score(i + 2, n)
            weigh(i + 1, n)
            gather(i, n)


REACH = (2, 1, 3, 0)


def layer_kernel(
    tok_ref, gain_ref, cos_a, sin_a, cos_b, sin_b, leak_ref, decay_ref, lam_ref, attgain_ref,
    recgain_ref,
    w0, w1, w2, w3, w4, w5, w6, wrec_ref, watt_ref,
    out_ref,
    xbuf, wbuf, attbuf, recraw, recout, read,
    kvbuf, qown, qbuf, qz, acc, peak, sendo, recvo, sendm, recvm, stbuf, totals, inside, chain_in,
    chain_out, mixrec, mixatt, gotrec, gotatt, wr, wa,
    wsem, y_send, y_recv,
    r_send, r_recv, l_send, l_recv, q_send, q_recv, o_send, o_recv, m_send, m_recv, s_send, s_recv,
    c_send, c_recv, tr_send, tr_recv, ta_send, ta_recv,
):
    z, x, t = lax.axis_index("sp_0"), lax.axis_index("sp_1"), lax.axis_index("tp")
    y, c = t // 2, t % 2
    right = lax.rem(y + 1, NY) * 2 + c
    left = lax.rem(y + NY - 1, NY) * 2 + c
    far = lax.rem(y + 2, NY) * 2 + c
    partner = 2 * y + 1 - c
    up = {"sp_0": lax.rem(z + 1, NZ)}
    down = {"sp_0": lax.rem(z + NZ - 1, NZ)}
    beside = [None] + [{"sp_1": lax.rem(x + p, NX)} for p in range(1, NX)]
    mates = [None] + [lax.rem(t + d, 8) for d in range(1, 8)]

    loads = [
        pltpu.make_async_copy(w, wbuf.at[:, pl.ds(128 * k, 128)], wsem.at[k])
        for k, w in enumerate((w0, w1, w2, w3, w4, w5, w6))
    ]
    late_loads = [
        pltpu.make_async_copy(wrec_ref, wr, wsem.at[7]),
        pltpu.make_async_copy(watt_ref, wa, wsem.at[8]),
    ]
    for load in loads:
        load.start()
    meet([up, down] + beside[1:] + [{"tp": m} for m in mates[1:]])

    half = ROWS // 2
    part = (pl.ds(0, half), pl.ds(half, half))
    own = [tok_ref.at[p] for p in part]
    copies = {}

    def to(src, slot, k, number, device):
        return remote(
            src, xbuf.at[slot, part[k]], y_send.at[number], y_recv.at[number], {"tp": device}
        )

    def launch(src, slot, k, number, device):
        copies[number] = to(src, slot, k, number, device)
        copies[number].start()

    def arrived(slot, k, number):
        to(own[k], slot, k, number, right).wait_recv()

    launch(own[0], t, 0, 0, right)
    launch(own[1], t, 1, 3, left)
    launch(own[1], t, 1, 1, right)
    launch(own[0], t, 0, 2, left)
    launch(own[0], t, 0, 4, partner)
    launch(own[1], t, 1, 5, partner)
    xbuf[t] = tok_ref[...]
    for load in loads:
        load.wait()
    for load in late_loads:
        load.start()

    block = z * NX + x
    cb = cos_b[pl.ds(block, 1), :]
    sb = sin_b[pl.ds(block, 1), :]
    lane = lax.broadcasted_iota(jnp.int32, (1, 128), 1)
    low = lax.rem(lane, 64) < 32

    def turned(v, cosine, sine):
        other = jnp.where(low, pltpu.roll(v, 96, 1), pltpu.roll(v, 32, 1))
        return v * cosine + other * sine

    def process(yy):
        pair = xbuf[pl.ds(2 * yy, 2)].reshape(2 * ROWS, D).astype(F32)
        scale = lax.rsqrt(jnp.mean(pair * pair, axis=1, keepdims=True) + EPS)
        normed = (pair * scale * gain_ref[...]).astype(BF16)
        out = dot(normed, wbuf[...])
        rows = pl.ds(pl.multiple_of(yy * 128, 128), 128)
        recraw[rows, :] = out[:, :512].astype(BF16)
        ca, sa = cos_a[rows, :], sin_a[rows, :]
        cosine = ca * cb - sa * sb
        sine = sa * cb + ca * sb
        signed = jnp.where(low, -sine, sine)
        raw = out[:, 512:].astype(BF16).astype(F32)
        attbuf[0, rows, :] = turned(raw[:, 0:128], cosine, signed) * (AK**-0.5 * LOG2E)
        attbuf[1, rows, :] = turned(raw[:, 128:256], cosine, signed)
        attbuf[2, rows, :] = raw[:, 256:384]

    arrived(partner, 0, 4)
    arrived(partner, 1, 5)
    process(y)
    arrived(left, 0, 0)
    launch(xbuf.at[left, part[0]], left, 0, 6, right)
    launch(xbuf.at[left, part[0]], left, 0, 8, partner)
    arrived(right, 1, 3)
    launch(xbuf.at[right, part[1]], right, 1, 7, left)
    launch(xbuf.at[right, part[1]], right, 1, 9, partner)
    arrived(left, 1, 1)
    launch(xbuf.at[left, part[1]], left, 1, 10, partner)
    arrived(right, 0, 2)
    launch(xbuf.at[right, part[0]], right, 0, 11, partner)
    mate_l, mate_r, mate_far = left + 1 - 2 * c, right + 1 - 2 * c, far + 1 - 2 * c
    arrived(mate_l, 0, 8)
    arrived(mate_l, 1, 10)
    process(left // 2)
    arrived(mate_r, 1, 9)
    arrived(mate_r, 0, 11)
    process(right // 2)
    arrived(far, 0, 6)
    launch(xbuf.at[far, part[0]], far, 0, 12, partner)
    arrived(far, 1, 7)
    launch(xbuf.at[far, part[1]], far, 1, 13, partner)
    arrived(mate_far, 0, 12)
    arrived(mate_far, 1, 13)
    process(far // 2)

    qown[...] = attbuf[0].T.astype(BF16)
    value_t = attbuf[2].T.astype(BF16)
    for s in range(2):
        kvbuf[0, s, 0:256, :] = attbuf[1, 256 * s : 256 * (s + 1), :].astype(BF16)
        kvbuf[0, s, 256:384, :] = value_t[:, 256 * s : 256 * s + 128]
        kvbuf[0, s, 384:512, :] = value_t[:, 256 * s + 128 : 256 * s + 256]

    ring = {}

    def rightward(step, s):
        src = kvbuf.at[(NZ - step) % NZ, s]
        return remote(
            src, kvbuf.at[NZ - 1 - step, s], r_send.at[step, s], r_recv.at[step, s], up
        )

    def leftward(step, s):
        src = kvbuf.at[step, s]
        return remote(src, kvbuf.at[step + 1, s], l_send.at[step, s], l_recv.at[step, s], down)

    def start_right(step, s):
        ring["r", step, s] = rightward(step, s)
        ring["r", step, s].start()

    def start_left(step, s):
        ring["l", step, s] = leftward(step, s)
        ring["l", step, s].start()

    def forward(step, s):
        rightward(step - 1, s).wait_recv()
        if step < 3 or s == 0:
            start_right(step, s)
        leftward(step - 1, s).wait_recv()
        if step < 3 or s == 1:
            start_left(step, s)

    q_copies = [None] + [
        remote(qown, qbuf.at[NX - p], q_send.at[p], q_recv.at[NX - p], beside[p])
        for p in range(1, NX)
    ]
    for p in (2, 1, 3):
        q_copies[p].start()
    for s in range(2):
        start_right(0, s)
        start_left(0, s)

    recurrence(recraw, leak_ref, decay_ref, recout, read, stbuf.at[0])
    s_copies = [None] + [
        remote(stbuf.at[0], stbuf.at[NX - p], s_send.at[p], s_recv.at[NX - p], beside[p])
        for p in range(1, NX)
    ]
    for p in range(1, NX):
        s_copies[p].start()

    upper = lax.broadcasted_iota(jnp.int32, (128, 1), 0) < AK

    def spread(q, source):
        for h in range(2):
            piece = source[:, 256 * h : 256 * (h + 1)].astype(F32)
            qz[q, h] = jnp.where(upper, piece, 0.0).astype(BF16)
            qz[q, 2 + h] = jnp.where(upper, 0.0, piece).astype(BF16)

    def attend(*jobs):
        flash(jobs, kvbuf, qz, acc, peak)

    def pieces(*slots):
        return [(r, s) for r in slots for s in range(2)]

    spread(3, qown[...])
    attend((3, pieces(0), True))
    forward(1, 0)
    for q in range(3):
        p = REACH[q]
        q_copies[NX - p].wait_recv()
        spread(q, qbuf[p])
    forward(1, 1)
    attend(*[(q, pieces(0), True) for q in range(3)])

    for p in range(1, NX):
        s_copies[NX - p].wait_recv()
    for side in range(2):
        order = range(NX) if side == 0 else reversed(range(NX))
        total_s, total_d = jnp.zeros((128, 128), F32), jnp.ones((1, 128), F32)
        inside_s, inside_d = total_s, total_d
        for k in order:
            rel = lax.rem(k - x + NX, NX)
            piece_s = stbuf[rel, side, 0:128, :].astype(F32)
            piece_d = stbuf[rel, side, 128:144, :].astype(F32)[0:1, :]
            total_s = total_s * piece_d + piece_s
            total_d = total_d * piece_d
            passed = (k < x) if side == 0 else (k > x)
            inside_s = jnp.where(passed, total_s, inside_s)
            inside_d = jnp.where(passed, total_d, inside_d)
        totals[side, 0:128, :] = total_s
        totals[side, 128:136, :] = jnp.broadcast_to(total_d, (8, 128))
        inside[side, 0:128, :] = inside_s
        inside[side, 128:136, :] = jnp.broadcast_to(inside_d, (8, 128))

    @pl.when(z == 0)
    def _():
        chain_in[0] = jnp.zeros((128, 128), F32)

    @pl.when(z == NZ - 1)
    def _():
        chain_in[1] = jnp.zeros((128, 128), F32)

    def chain_copy(side):
        return remote(
            chain_out.at[side], chain_in.at[side], c_send.at[side], c_recv.at[side],
            up if side == 0 else down,
        )

    def chain(hop, first=False, last=False):
        for side in range(2):
            turn = (z == hop) if side == 0 else (z == NZ - 1 - hop)

            @pl.when(turn)
            def _():
                if not first:
                    chain_copy(side).wait_recv()
                if not last:
                    chain_out[side] = (
                        chain_in[side] * totals[side, 128:129, :] + totals[side, 0:128, :]
                    )
                    chain_copy(side).start()

    chain(0, first=True)

    def both(start, *slots):
        def step(j, carry):
            attend((2 * j, pieces(*slots), False), (2 * j + 1, pieces(*slots), False))
            chain(start + j)
            return carry

        lax.fori_loop(0, 2, step, 0)

    both(1, 7, 1)
    forward(2, 0)
    forward(2, 1)
    both(3, 6, 2)
    forward(3, 0)
    forward(3, 1)
    o_copies = {}

    def give(q):
        p = REACH[q]
        for k in range(4):
            inverse = 1.0 / acc[q, k, 128:129, :]
            sendo[p, k] = (acc[q, k, 0:128, :] * inverse).astype(BF16)
            sendm[p, k, 0:8, :] = peak[q, k]
            sendm[p, k, 8:16, :] = acc[q, k, 128:136, :]
        o_copies[p] = (
            remote(sendo.at[p], recvo.at[NX - p], o_send.at[p], o_recv.at[NX - p], beside[p]),
            remote(sendm.at[p], recvm.at[NX - p], m_send.at[p], m_recv.at[NX - p], beside[p]),
        )
        for copy in o_copies[p]:
            copy.start()

    attend((0, pieces(5, 3), False), (1, pieces(5, 3), False))
    chain(5)
    rightward(3, 0).wait_recv()
    leftward(3, 1).wait_recv()
    attend((0, pieces(4), False), (1, pieces(4), False))
    give(0)
    give(1)
    chain(6)
    attend((2, pieces(5, 3, 4), False))
    give(2)
    chain(NZ - 1, last=True)

    out = recout[...]
    for side in range(2):
        entry = chain_in[side] * inside[side, 128:129, :] + inside[side, 0:128, :]
        out = out + dot_nt(read[side], entry.astype(BF16))
    out = out * lax.rsqrt(jnp.mean(out * out, axis=1, keepdims=True) + EPS) * recgain_ref[...]
    mixrec[...] = out.astype(BF16)

    def rows_of(device):
        return pl.ds(pl.multiple_of(device * ROWS, ROWS), ROWS)

    def deal(source, got, send, recv):
        sent = [
            remote(source.at[rows_of(mates[d]), :], got.at[t], send.at[d], recv.at[8 - d],
                   {"tp": mates[d]})
            for d in range(1, 8)
        ]
        for copy in sent:
            copy.start()
        return sent

    def collect(source, got, send, recv):
        for d in range(1, 8):
            remote(
                source.at[rows_of(t), :], got.at[mates[d]], send.at[d], recv.at[d],
                {"tp": mates[d]},
            ).wait_recv()

    rec_sent = deal(mixrec, gotrec, tr_send, tr_recv)
    gotrec[t] = mixrec[rows_of(t), :]

    attend((3, pieces(5, 3, 4), False))

    for load in late_loads:
        load.wait()
    collect(mixrec, gotrec, tr_send, tr_recv)
    rec_term = dot(jnp.concatenate([gotrec[k] for k in range(8)], axis=1), wr[...])

    for p in (2, 3, 1):
        for copy in o_copies[NX - p]:
            copy.wait_recv()
    lam = lam_ref[0:1, 0:1]
    for h in range(2):
        maps = []
        for m in range(2):
            k = 2 * m + h
            tops = [peak[3, k, 0:1, :]] + [recvm[p, k, 0:1, :] for p in range(1, NX)]
            sums = [acc[3, k, 128:129, :]] + [recvm[p, k, 8:9, :] for p in range(1, NX)]
            top = tops[0]
            for other in tops[1:]:
                top = jnp.maximum(top, other)
            shares = [a * jnp.exp2(b - top) for a, b in zip(sums, tops)]
            whole = shares[0] + shares[1] + shares[2] + shares[3]
            inverse = 1.0 / whole
            value = acc[3, k, 0:128, :] * (jnp.exp2(tops[0] - top) * inverse)
            for p in range(1, NX):
                value = value + recvo[p, k].astype(F32) * (shares[p] * inverse)
            maps.append(value)
        mixed = maps[0] - lam * maps[1]
        mixed = mixed * lax.rsqrt(jnp.mean(mixed * mixed, axis=0, keepdims=True) + EPS)
        mixatt[256 * h : 256 * (h + 1), :] = (mixed.T * attgain_ref[...]).astype(BF16)
    att_sent = deal(mixatt, gotatt, ta_send, ta_recv)
    gotatt[t] = mixatt[rows_of(t), :]
    collect(mixatt, gotatt, ta_send, ta_recv)
    att_term = dot(jnp.concatenate([gotatt[k] for k in range(8)], axis=1), wa[...])
    out_ref[...] = (rec_term + att_term).astype(BF16)

    for copy in list(copies.values()) + list(ring.values()) + q_copies[1:] + s_copies[1:]:
        copy.wait_send()
    for pair in o_copies.values():
        for copy in pair:
            copy.wait_send()
    for copy in rec_sent + att_sent:
        copy.wait_send()

    @pl.when(z < NZ - 1)
    def _():
        chain_copy(0).wait_send()

    @pl.when(z > 0)
    def _():
        chain_copy(1).wait_send()


def on_device(
    tokens, norm_gain, rec_query, fwd_gate, bwd_gate, rec_value, gate_leak, log_decay, rec_gain,
    att_query, att_key, att_value, lambdas, att_gain, out_rec, out_att,
):
    weights = (rec_query, fwd_gate, bwd_gate, rec_value, att_query, att_key, att_value)
    dma = pltpu.SemaphoreType.DMA
    four = [dma((NX,))] * 8
    return pl.pallas_call(
        layer_kernel,
        out_shape=jax.ShapeDtypeStruct((ROWS, D), BF16),
        in_specs=[VMEM_SPEC] * 11 + [ANY_SPEC] * 9,
        out_specs=VMEM_SPEC,
        scratch_shapes=[
            pltpu.VMEM((8, ROWS, D), BF16),
            pltpu.VMEM((D, NCOL), BF16),
            pltpu.VMEM((3, LEN, 128), F32),
            pltpu.VMEM((LEN, 512), BF16),
            pltpu.VMEM((LEN, 128), F32),
            pltpu.VMEM((2, LEN, 128), BF16),
            pltpu.VMEM((NZ, 2, 512, 128), BF16),
            pltpu.VMEM((128, LEN), BF16),
            pltpu.VMEM((NX, 128, LEN), BF16),
            pltpu.VMEM((NX, 4, 128, 256), BF16),
            pltpu.VMEM((NX, 4, 144, 256), F32),
            pltpu.VMEM((NX, 4, 8, 256), F32),
            pltpu.VMEM((NX, 4, 128, 256), BF16),
            pltpu.VMEM((NX, 4, 128, 256), BF16),
            pltpu.VMEM((NX, 4, 16, 256), F32),
            pltpu.VMEM((NX, 4, 16, 256), F32),
            pltpu.VMEM((NX, 2, 144, 128), BF16),
            pltpu.VMEM((2, 136, 128), F32),
            pltpu.VMEM((2, 136, 128), F32),
            pltpu.VMEM((2, 128, 128), F32),
            pltpu.VMEM((2, 128, 128), F32),
            pltpu.VMEM((LEN, 128), BF16),
            pltpu.VMEM((LEN, 128), BF16),
            pltpu.VMEM((8, ROWS, 128), BF16),
            pltpu.VMEM((8, ROWS, 128), BF16),
            pltpu.VMEM((1024, D), BF16),
            pltpu.VMEM((1024, D), BF16),
            dma((9,)), dma((14,)), dma((14,)),
            dma((4, 2)), dma((4, 2)), dma((4, 2)), dma((4, 2)),
            *four,
            dma((2,)), dma((2,)), dma((8,)), dma((8,)), dma((8,)), dma((8,)),
        ],
        compiler_params=pltpu.CompilerParams(
            collective_id=0, has_side_effects=True, vmem_limit_bytes=VMEM_LIMIT,
        ),
        name="layer",
    )(
        tokens, norm_gain.reshape(1, D), *rotary_tables(), gate_leak, log_decay.reshape(2, LEN),
        lambdas.reshape(1, 1), att_gain.reshape(1, 128), rec_gain.reshape(1, 128), *weights,
        out_rec, out_att,
    )


def solution(mesh):
    torus = Mesh(mesh.devices.reshape(NZ, NX, mesh.shape["tp"]), SP_TP)
    tp = P(None, "tp")
    in_specs = (
        P(SP_TP, None), P(), tp, tp, tp, tp, tp, P(None, SP, "tp"), P(), tp, tp, tp, P("tp"), P(),
        P(), P(),
    )
    return jax.shard_map(
        on_device, mesh=torus, in_specs=in_specs, out_specs=P(SP_TP, None), check_vma=False
    )
```

```python
import math

import jax
import jax.numpy as jnp
import numpy as np
from jax import lax
from jax.experimental import pallas as pl
from jax.experimental.pallas import tpu as pltpu
from jax.sharding import Mesh
from jax.sharding import PartitionSpec as P

HK = 128
AK = 64
BLOCK = 64
SP = ("sp_0", "sp_1")
SP_TP = ("sp_0", "sp_1", "tp")
NZ, NX, NY = 8, 4, 4
ROWS = 64
LEN = 512
D = 2048
NCOL = 896
EPS = 1e-06
THETA = 500000.0
LOG2E = 1.4426950408889634
F32 = jnp.float32
BF16 = jnp.bfloat16
MESH = pl.DeviceIdType.MESH
VMEM_SPEC = pl.BlockSpec(memory_space=pltpu.VMEM)
ANY_SPEC = pl.BlockSpec(memory_space=pl.ANY)
VMEM_LIMIT = 60 * 1024 * 1024


def remote(src, dst, send_sem, recv_sem, device):
    return pltpu.make_async_remote_copy(
        src_ref=src,
        dst_ref=dst,
        send_sem=send_sem,
        recv_sem=recv_sem,
        device_id=device,
        device_id_type=MESH,
    )


def meet(devices):
    barrier = pltpu.get_barrier_semaphore()
    for device in devices:
        pl.semaphore_signal(barrier, inc=1, device_id=device, device_id_type=MESH)
    pl.semaphore_wait(barrier, len(devices))


def dot(a, b):
    return jnp.dot(a, b, preferred_element_type=F32)


def dot_nt(a, b):
    return lax.dot_general(a, b, (((1,), (1,)), ((), ())), preferred_element_type=F32)


def rotary_tables():
    i = np.arange(AK // 2, dtype=np.float64)
    freq = THETA ** (-(i * 2.0 / AK))
    freq = np.tile(freq, 4)[None, :]
    within = np.arange(LEN, dtype=np.float64)[:, None] * freq
    starts = np.arange(NZ * NX, dtype=np.float64)[:, None] * LEN * freq
    return [
        jnp.asarray(f(v).astype(np.float32)) for v in (within, starts) for f in (np.cos, np.sin)
    ]


def exact_cumulative(triangle, logs):
    first = logs.astype(BF16)
    rest = logs - first.astype(F32)
    second = rest.astype(BF16)
    third = (rest - second.astype(F32)).astype(BF16)
    return dot(triangle, first) + dot(triangle, second) + dot(triangle, third)


def recurrence(rec_ref, leak_ref, decay_ref, out_ref, read_ref, state_ref):
    blocks = LEN // BLOCK
    raw_q = rec_ref[:, 0:128].astype(F32)
    rq = raw_q / (1.0 + jnp.exp(-raw_q))
    value = rec_ref[:, 384:512]
    value_t = value.astype(F32).T.astype(BF16)
    row = lax.broadcasted_iota(jnp.int32, (256, 256), 0)
    col = lax.broadcasted_iota(jnp.int32, (256, 256), 1)
    same = (row // BLOCK) == (col // BLOCK)
    upper = lax.broadcasted_iota(jnp.int32, (128, 1), 0) < BLOCK
    total_out = None
    for side in range(2):
        raw = rec_ref[:, 128 * (side + 1) : 128 * (side + 2)].astype(F32)
        key = leak_ref[side : side + 1, :] / (1.0 + jnp.exp(raw))
        added_log = jnp.concatenate(
            [
                jnp.broadcast_to(decay_ref[4 * side + k : 4 * side + k + 1, :], (128, 128)).T
                for k in range(4)
            ],
            axis=0,
        )
        logs = jnp.log1p(-key) + added_log
        mask = same & ((row >= col) if side == 0 else (row <= col))
        triangle = mask.astype(F32).astype(BF16)
        cum = jnp.concatenate(
            [exact_cumulative(triangle, logs[256 * h : 256 * (h + 1)]) for h in range(2)], axis=0
        )
        cum3 = cum.reshape(blocks, BLOCK, 128)
        at_mid, at_last = (BLOCK // 2 - 1, BLOCK - 1) if side == 0 else (BLOCK // 2, 0)
        middle = cum3[:, at_mid : at_mid + 1, :]
        last = cum3[:, at_last : at_last + 1, :]
        key3, rq3 = key.reshape(cum3.shape), rq.reshape(cum3.shape)
        qs = (rq3 * jnp.exp(cum3 - middle)).reshape(LEN, 128).astype(BF16)
        ks = (key3 * jnp.exp(middle - cum3)).reshape(LEN, 128).astype(BF16)
        kl = (key3 * jnp.exp(last - cum3)).reshape(LEN, 128)
        qc = (rq3 * jnp.exp(cum3)).reshape(LEN, 128).astype(BF16)
        within = []
        for h in range(2):
            part = slice(256 * h, 256 * (h + 1))
            scores = jnp.where(mask, dot_nt(qs[part], ks[part]), 0.0).astype(BF16)
            within.append(dot(scores, value[part]))
        order = range(blocks) if side == 0 else reversed(range(blocks))
        state = jnp.zeros((128, 128), F32)
        carried, before = [None] * blocks, [None] * blocks
        running = jnp.zeros((1, 128), F32)
        for b in order:
            carried[b] = dot_nt(qc[BLOCK * b : BLOCK * (b + 1)], state.astype(BF16))
            pair = b // 2
            keys = kl[128 * pair : 128 * (pair + 1)]
            keys = jnp.where(upper if b % 2 == 0 else ~upper, keys, 0.0).astype(BF16)
            added = dot(value_t[:, 128 * pair : 128 * (pair + 1)], keys)
            before[b] = running
            running = running + last[b]
            state = state * jnp.exp(last[b]) + added
        out = jnp.concatenate(within, axis=0) + jnp.concatenate(carried, axis=0)
        total_out = out if total_out is None else total_out + out
        reach = (cum3 + jnp.stack(before, axis=0)).reshape(LEN, 128)
        read_ref[side] = (rq * jnp.exp(reach)).astype(BF16)
        state_ref[side, 0:128, :] = state.astype(BF16)
        state_ref[side, 128:144, :] = jnp.broadcast_to(jnp.exp(running), (16, 128)).astype(BF16)
    out_ref[...] = total_out


def flash(jobs, kvbuf, qz, acc, peak):
    ones = jnp.ones((16, 256), BF16)
    tiles = [(q, k, pieces, first) for q, pieces, first in jobs for k in range(4)]
    count = len(tiles)
    tops, olds, sums = [None] * count, [None] * count, [None] * count
    scores, weights = [{} for _ in tiles], [{} for _ in tiles]

    def score(i, n):
        if not (0 <= i < count and n < len(tiles[i][2])):
            return
        q, k, pieces, first = tiles[i]
        if n == 0 and not first:
            olds[i] = tops[i] = peak[q, k, 0:1, :]
        r, s = pieces[n]
        keys = jnp.concatenate([kvbuf[r, 2 * s, 0:128, :], kvbuf[r, 2 * s + 1, 0:128, :]], axis=0)
        scores[i][n] = dot(keys, qz[q, k])
        here = jnp.max(scores[i][n], axis=0, keepdims=True)
        tops[i] = here if tops[i] is None else jnp.maximum(tops[i], here)

    def weigh(i, n):
        if not (0 <= i < count and n < len(tiles[i][2])):
            return
        weights[i][n] = jnp.exp2(scores[i].pop(n) - tops[i]).astype(BF16)

    def gather(i, n):
        if not (0 <= i < count and n < len(tiles[i][2])):
            return
        q, k, pieces, first = tiles[i]
        r, s = pieces[n]
        values = [kvbuf[r, 2 * s, 128:256, :], kvbuf[r, 2 * s + 1, 128:256, :]]
        values = jnp.concatenate(values, axis=1)
        term = dot(jnp.concatenate([values, ones], axis=0), weights[i].pop(n))
        sums[i] = term if sums[i] is None else sums[i] + term
        if n == len(pieces) - 1:
            if first:
                acc[q, k] = sums[i]
            else:
                acc[q, k] = acc[q, k] * jnp.exp2(olds[i] - tops[i]) + sums[i]
            peak[q, k] = jnp.broadcast_to(tops[i], (8, 256))

    longest = max(len(t[2]) for t in tiles)
    for i in range(-2, count):
        for n in range(longest):
            score(i + 2, n)
            weigh(i + 1, n)
            gather(i, n)


REACH = (2, 1, 3, 0)


def layer_kernel(
    lam_ref, tok_ref, *refs,
):
    small, weights, (wrec_ref, watt_ref, out_ref) = refs[:9], refs[9:16], refs[16:19]
    (
        gain_ref, cos_a, sin_a, cos_b, sin_b, leak_ref, decay_ref, attgain_ref, recgain_ref,
        xbuf, wbuf, recraw, recout, read,
        kvbuf, qown, qbuf, qz, acc, peak, farout, farin, farouts, farins, nearout, nearin,
        nearouts, nearins, stbuf, totals, inside, chain_in, chain_out, half_in, half_out,
        mixrec, mixatt, gotrec, gotatt, wr, wa,
        wsem, y_send, y_recv,
        r_send, r_recv, l_send, l_recv, q_send, q_recv, s_send, s_recv,
        c_send, c_recv, h_send, h_recv, f_send, f_recv, n_send, n_recv,
        tr_send, tr_recv, ta_send, ta_recv,
    ) = refs[19:]
    z, x, t = lax.axis_index("sp_0"), lax.axis_index("sp_1"), lax.axis_index("tp")
    y, c = t // 2, t % 2
    right = lax.rem(y + 1, NY) * 2 + c
    left = lax.rem(y + NY - 1, NY) * 2 + c
    far = lax.rem(y + 2, NY) * 2 + c
    partner = 2 * y + 1 - c
    up = {"sp_0": lax.rem(z + 1, NZ)}
    down = {"sp_0": lax.rem(z + NZ - 1, NZ)}
    beside = [None] + [{"sp_1": lax.rem(x + p, NX)} for p in range(1, NX)]
    mates = [None] + [lax.rem(t + d, 8) for d in range(1, 8)]

    own_load = pltpu.make_async_copy(tok_ref, xbuf.at[t], wsem.at[9])
    own_load.start()
    loads = [
        pltpu.make_async_copy(w, wbuf.at[:, pl.ds(128 * k, 128)], wsem.at[k])
        for k, w in enumerate(weights)
    ]
    homes = (gain_ref, cos_a, sin_a, cos_b, sin_b, leak_ref, decay_ref, attgain_ref, recgain_ref)
    loads += [
        pltpu.make_async_copy(a, b, wsem.at[10 + k]) for k, (a, b) in enumerate(zip(small, homes))
    ]
    late_loads = [
        pltpu.make_async_copy(wrec_ref, wr, wsem.at[7]),
        pltpu.make_async_copy(watt_ref, wa, wsem.at[8]),
    ]
    for load in loads:
        load.start()
    far_z = [{"sp_0": lax.rem(z + d, NZ)} for d in range(2, NZ - 1)]
    meet([up, down] + far_z + beside[1:] + [{"tp": m} for m in mates[1:]])
    own_load.wait()

    half = ROWS // 2
    part = (pl.ds(0, half), pl.ds(half, half))
    own = [xbuf.at[t, p] for p in part]
    copies = {}

    def to(src, slot, k, number, device):
        return remote(
            src, xbuf.at[slot, part[k]], y_send.at[number], y_recv.at[number], {"tp": device}
        )

    def launch(src, slot, k, number, device):
        copies[number] = to(src, slot, k, number, device)
        copies[number].start()

    def arrived(slot, k, number):
        to(own[k], slot, k, number, right).wait_recv()

    launch(own[0], t, 0, 0, right)
    launch(own[1], t, 1, 3, left)
    launch(own[1], t, 1, 1, right)
    launch(own[0], t, 0, 2, left)
    launch(own[0], t, 0, 4, partner)
    launch(own[1], t, 1, 5, partner)
    for load in loads:
        load.wait()
    for load in late_loads:
        load.start()

    block = z * NX + x
    cb = cos_b[pl.ds(block, 1), :]
    sb = sin_b[pl.ds(block, 1), :]
    lane = lax.broadcasted_iota(jnp.int32, (1, 128), 1)
    low = lax.rem(lane, 64) < 32

    def turned(v, cosine, sine):
        other = jnp.where(low, pltpu.roll(v, 96, 1), pltpu.roll(v, 32, 1))
        return v * cosine + other * sine

    ring = {}

    def rightward(step, j):
        src = kvbuf.at[(NZ - step) % NZ, j]
        return remote(
            src, kvbuf.at[NZ - 1 - step, j], r_send.at[step, j], r_recv.at[step, j], up
        )

    def leftward(step, j):
        src = kvbuf.at[step, j]
        return remote(src, kvbuf.at[step + 1, j], l_send.at[step, j], l_recv.at[step, j], down)

    def start_right(step, j):
        ring["r", step, j] = rightward(step, j)
        ring["r", step, j].start()

    def start_left(step, j):
        ring["l", step, j] = leftward(step, j)
        ring["l", step, j].start()

    def forward(step, j):
        rightward(step - 1, j).wait_recv()
        if step < 3 or j < 2:
            start_right(step, j)
        leftward(step - 1, j).wait_recv()
        if step < 3 or j >= 2:
            start_left(step, j)

    q_copies = {}

    def process(yy, j):
        pair = xbuf[pl.ds(2 * yy, 2)].reshape(2 * ROWS, D).astype(F32)
        scale = lax.rsqrt(jnp.mean(pair * pair, axis=1, keepdims=True) + EPS)
        normed = (pair * scale * gain_ref[...]).astype(BF16)
        out = dot(normed, wbuf[...])
        rows = pl.ds(pl.multiple_of(yy * 128, 128), 128)
        ca, sa = cos_a[rows, :], sin_a[rows, :]
        cosine = ca * cb - sa * sb
        sine = sa * cb + ca * sb
        signed = jnp.where(low, -sine, sine)
        raw = out[:, 512:].astype(BF16).astype(F32)
        kvbuf[0, j, 0:128, :] = turned(raw[:, 128:256], cosine, signed).astype(BF16)
        kvbuf[0, j, 128:256, :] = raw[:, 256:384].T.astype(BF16)
        query = turned(raw[:, 0:128], cosine, signed) * (AK**-0.5 * LOG2E)
        qown[j] = query.T.astype(BF16)
        recraw[rows, :] = out[:, :512].astype(BF16)
        start_right(0, j)
        start_left(0, j)
        for p in (2, 1, 3):
            q_copies[p, j] = remote(
                qown.at[j], qbuf.at[NX - p, j], q_send.at[p, j], q_recv.at[NX - p, j], beside[p]
            )
            q_copies[p, j].start()

    arrived(partner, 0, 4)
    arrived(partner, 1, 5)
    process(y, 0)
    arrived(left, 0, 0)
    launch(xbuf.at[left, part[0]], left, 0, 6, right)
    launch(xbuf.at[left, part[0]], left, 0, 8, partner)
    arrived(right, 1, 3)
    launch(xbuf.at[right, part[1]], right, 1, 7, left)
    launch(xbuf.at[right, part[1]], right, 1, 9, partner)
    forward(1, 0)
    arrived(left, 1, 1)
    launch(xbuf.at[left, part[1]], left, 1, 10, partner)
    arrived(right, 0, 2)
    launch(xbuf.at[right, part[0]], right, 0, 11, partner)
    mate_l, mate_r, mate_far = left + 1 - 2 * c, right + 1 - 2 * c, far + 1 - 2 * c
    arrived(mate_l, 0, 8)
    arrived(mate_l, 1, 10)
    process(left // 2, 1)
    forward(2, 0)
    arrived(mate_r, 1, 9)
    arrived(mate_r, 0, 11)
    process(right // 2, 2)
    arrived(far, 0, 6)
    launch(xbuf.at[far, part[0]], far, 0, 12, partner)
    arrived(far, 1, 7)
    launch(xbuf.at[far, part[1]], far, 1, 13, partner)
    arrived(mate_far, 0, 12)
    arrived(mate_far, 1, 13)
    process(far // 2, 3)
    forward(1, 1)
    forward(3, 0)

    recurrence(recraw, leak_ref, decay_ref, recout, read, stbuf.at[0])
    s_copies = [None] + [
        remote(stbuf.at[0], stbuf.at[NX - p], s_send.at[p], s_recv.at[NX - p], beside[p])
        for p in range(1, NX)
    ]
    for p in range(1, NX):
        s_copies[p].start()
    forward(1, 2)

    upper = lax.broadcasted_iota(jnp.int32, (128, 1), 0) < AK

    def spread(q, source):
        for h in range(2):
            piece = jnp.concatenate([source(2 * h), source(2 * h + 1)], axis=1).astype(F32)
            qz[q, h] = jnp.where(upper, piece, 0.0).astype(BF16)
            qz[q, 2 + h] = jnp.where(upper, 0.0, piece).astype(BF16)

    def attend(*jobs):
        flash(jobs, kvbuf, qz, acc, peak)

    def pieces(*slots):
        return [(r, s) for r in slots for s in range(2)]

    spread(3, lambda j: qown[j])
    attend((3, pieces(0), True))
    for q in range(3):
        p = REACH[q]
        for j in range(4):
            q_copies[NX - p, j].wait_recv()
        spread(q, lambda j: qbuf[p, j])
    attend(*[(q, pieces(0), True) for q in range(3)])
    forward(1, 3)

    for p in range(1, NX):
        s_copies[NX - p].wait_recv()
    for side in range(2):
        order = range(NX) if side == 0 else reversed(range(NX))
        total_s, total_d = jnp.zeros((128, 128), F32), jnp.ones((1, 128), F32)
        inside_s, inside_d = total_s, total_d
        for k in order:
            rel = lax.rem(k - x + NX, NX)
            piece_s = stbuf[rel, side, 0:128, :].astype(F32)
            piece_d = stbuf[rel, side, 128:144, :].astype(F32)[0:1, :]
            total_s = total_s * piece_d + piece_s
            total_d = total_d * piece_d
            passed = (k < x) if side == 0 else (k > x)
            inside_s = jnp.where(passed, total_s, inside_s)
            inside_d = jnp.where(passed, total_d, inside_d)
        totals[side, 0:128, :] = total_s
        totals[side, 128:136, :] = jnp.broadcast_to(total_d, (8, 128))
        inside[side, 0:128, :] = inside_s
        inside[side, 128:136, :] = jnp.broadcast_to(inside_d, (8, 128))

    quarter = NZ // 2
    place = (lax.rem(z, quarter), quarter - 1 - lax.rem(z, quarter))
    giver = (quarter - 1, quarter)
    takes = (z >= quarter, z < quarter)

    for side in range(2):

        @pl.when(place[side] == 0)
        def _():
            chain_in[side, 0:128, :] = jnp.zeros((128, 128), BF16)
            chain_in[side, 128:144, :] = jnp.ones((16, 128), BF16)

        @pl.when(jnp.logical_not(takes[side]))
        def _():
            half_in[side] = jnp.zeros((128, 128), BF16)

    def chain_copy(side):
        return remote(
            chain_out.at[side], chain_in.at[side], c_send.at[side], c_recv.at[side],
            up if side == 0 else down,
        )

    def half_copy(side, k):
        device = quarter + k if side == 0 else quarter - 1 - k
        return remote(
            half_out.at[side], half_in.at[side], h_send.at[side, k], h_recv.at[side],
            {"sp_0": device},
        )

    def chain(hop):
        for side in range(2):

            @pl.when(place[side] == hop)
            def _():
                if hop > 0:
                    chain_copy(side).wait_recv()
                entered = chain_in[side].astype(F32)
                decay = totals[side, 128:129, :]
                state = entered[0:128, :] * decay + totals[side, 0:128, :]
                if hop < quarter - 1:
                    chain_out[side, 0:128, :] = state.astype(BF16)
                    chain_out[side, 128:144, :] = (entered[128:144, :] * decay).astype(BF16)
                    chain_copy(side).start()
                else:

                    @pl.when(z == giver[side])
                    def _():
                        half_out[side] = state.astype(BF16)
                        for k in range(quarter):
                            half_copy(side, k).start()

    chain(0)
    attend((0, pieces(7, 1), False), (1, pieces(7, 1), False))
    forward(2, 1)
    forward(2, 2)
    chain(1)
    attend((2, pieces(7, 1), False), (3, pieces(7, 1), False))
    forward(2, 3)
    chain(2)
    attend((0, pieces(6, 2), False), (1, pieces(6, 2), False))
    forward(3, 1)
    forward(3, 2)
    chain(3)
    attend((2, pieces(6, 2), False), (3, pieces(6, 2), False))
    forward(3, 3)
    attend((0, pieces(5, 3), False), (1, pieces(5, 3), False))
    for j in range(2):
        rightward(3, j).wait_recv()
        leftward(3, 2 + j).wait_recv()

    shallow = lax.broadcasted_iota(jnp.int32, (8, 256), 0) < 4
    o_copies = []

    def pack(q, m, out, stat):
        for h in range(2):
            k = 2 * m + h
            total = acc[q, k, 128:129, :]
            out[h] = (acc[q, k, 0:128, :] * (1.0 / total)).astype(BF16)
            stat[h] = jnp.where(shallow, peak[q, k], acc[q, k, 128:136, :])

    def pack_merged(q, m, out, stat, other, others):
        for h in range(2):
            k = 2 * m + h
            top_a, top_b = peak[q, k, 0:1, :], others[h, 0:1, :]
            top = jnp.maximum(top_a, top_b)
            scale = jnp.exp2(top_a - top)
            share = others[h, 4:5, :] * jnp.exp2(top_b - top)
            total = acc[q, k, 128:129, :] * scale + share
            inverse = 1.0 / total
            merged = acc[q, k, 0:128, :] * (scale * inverse)
            merged = merged + other[h].astype(F32) * (share * inverse)
            out[h] = merged.astype(BF16)
            stat[h] = jnp.where(shallow, top, total)

    def far_copies(m):
        device = beside[1] if m == 0 else beside[3]
        return [
            remote(farout.at[m], farin.at[m], f_send.at[m, 0], f_recv.at[m, 0], device),
            remote(farouts.at[m], farins.at[m], f_send.at[m, 1], f_recv.at[m, 1], device),
        ]

    def near_copies(w, m):
        device = beside[1] if w == 0 else beside[3]
        return [
            remote(
                nearout.at[w, m], nearin.at[w, m], n_send.at[w, m, 0], n_recv.at[w, m, 0], device
            ),
            remote(
                nearouts.at[w, m], nearins.at[w, m], n_send.at[w, m, 1], n_recv.at[w, m, 1], device
            ),
        ]

    def post(pair):
        for copy in pair:
            copy.start()
            o_copies.append(copy)

    def received(pair):
        for copy in pair:
            copy.wait_recv()

    attend((0, pieces(4), False))
    for m in range(2):
        pack(0, m, farout.at[m], farouts.at[m])
        post(far_copies(m))
    attend((1, pieces(4), False), (2, pieces(5, 3, 4), False))
    pack(1, 1, nearout.at[0, 1], nearouts.at[0, 1])
    post(near_copies(0, 1))
    pack(2, 0, nearout.at[1, 0], nearouts.at[1, 0])
    post(near_copies(1, 0))

    for side in range(2):

        @pl.when(takes[side])
        def _():
            half_copy(side, 0).wait_recv()

    out = recout[...]
    for side in range(2):
        entered = chain_in[side].astype(F32)
        entry = entered[0:128, :] + half_in[side].astype(F32) * entered[128:129, :]
        entry = entry * inside[side, 128:129, :] + inside[side, 0:128, :]
        out = out + dot_nt(read[side], entry.astype(BF16))
    out = out * lax.rsqrt(jnp.mean(out * out, axis=1, keepdims=True) + EPS) * recgain_ref[...]
    mixrec[...] = out.astype(BF16)

    def rows_of(device):
        return pl.ds(pl.multiple_of(device * ROWS, ROWS), ROWS)

    def deal(source, got, send, recv):
        sent = [
            remote(source.at[rows_of(mates[d]), :], got.at[t], send.at[d], recv.at[8 - d],
                   {"tp": mates[d]})
            for d in range(1, 8)
        ]
        for copy in sent:
            copy.start()
        return sent

    def collect(source, got, send, recv):
        for d in range(1, 8):
            remote(
                source.at[rows_of(t), :], got.at[mates[d]], send.at[d], recv.at[d],
                {"tp": mates[d]},
            ).wait_recv()

    rec_sent = deal(mixrec, gotrec, tr_send, tr_recv)
    gotrec[t] = mixrec[rows_of(t), :]

    received(far_copies(0))
    pack_merged(1, 0, nearout.at[0, 0], nearouts.at[0, 0], farin.at[0], farins.at[0])
    post(near_copies(0, 0))
    received(far_copies(1))
    pack_merged(2, 1, nearout.at[1, 1], nearouts.at[1, 1], farin.at[1], farins.at[1])
    post(near_copies(1, 1))

    attend((3, pieces(5, 3, 4), False))

    for load in late_loads:
        load.wait()
    collect(mixrec, gotrec, tr_send, tr_recv)
    rec_term = dot(jnp.concatenate([gotrec[k] for k in range(8)], axis=1), wr[...])

    for copy in list(copies.values()) + list(ring.values()) + list(q_copies.values()):
        copy.wait_send()
    for copy in s_copies[1:] + rec_sent:
        copy.wait_send()
    for side in range(2):

        @pl.when(place[side] < quarter - 1)
        def _():
            chain_copy(side).wait_send()

        @pl.when(z == giver[side])
        def _():
            for k in range(quarter):
                half_copy(side, k).wait_send()

    lam = lam_ref[0:1, 0:1]
    for w, m in ((0, 1), (1, 0), (0, 0), (1, 1)):
        received(near_copies(w, m))
    for h in range(2):
        maps = []
        for m in range(2):
            k = 2 * m + h
            tops = [peak[3, k, 0:1, :]] + [nearins[w, m, h, 0:1, :] for w in range(2)]
            sums = [acc[3, k, 128:129, :]] + [nearins[w, m, h, 4:5, :] for w in range(2)]
            top = jnp.maximum(jnp.maximum(tops[0], tops[1]), tops[2])
            shares = [a * jnp.exp2(b - top) for a, b in zip(sums, tops)]
            inverse = 1.0 / (shares[0] + shares[1] + shares[2])
            value = acc[3, k, 0:128, :] * (jnp.exp2(tops[0] - top) * inverse)
            for w in range(2):
                value = value + nearin[w, m, h].astype(F32) * (shares[w + 1] * inverse)
            maps.append(value)
        mixed = maps[0] - lam * maps[1]
        mixed = mixed * lax.rsqrt(jnp.mean(mixed * mixed, axis=0, keepdims=True) + EPS)
        rows = (mixed.T * attgain_ref[...]).astype(BF16)
        for half_of, yy in zip(range(2), ((y, left // 2), (right // 2, far // 2))[h]):
            at = pl.ds(pl.multiple_of(yy * 128, 128), 128)
            mixatt[at, :] = rows[128 * half_of : 128 * (half_of + 1), :]
    att_sent = deal(mixatt, gotatt, ta_send, ta_recv)
    gotatt[t] = mixatt[rows_of(t), :]
    for copy in o_copies:
        copy.wait_send()
    collect(mixatt, gotatt, ta_send, ta_recv)
    att_term = dot(jnp.concatenate([gotatt[k] for k in range(8)], axis=1), wa[...])
    out_ref[...] = (rec_term + att_term).astype(BF16)
    for copy in att_sent:
        copy.wait_send()


def on_device(
    tokens, norm_gain, rec_query, fwd_gate, bwd_gate, rec_value, gate_leak, log_decay, rec_gain,
    att_query, att_key, att_value, lambdas, att_gain, out_rec, out_att,
):
    weights = (rec_query, fwd_gate, bwd_gate, rec_value, att_query, att_key, att_value)
    dma = pltpu.SemaphoreType.DMA
    return pl.pallas_call(
        layer_kernel,
        out_shape=jax.ShapeDtypeStruct((ROWS, D), BF16),
        in_specs=[VMEM_SPEC] + [ANY_SPEC] * 19,
        out_specs=VMEM_SPEC,
        scratch_shapes=[
            pltpu.VMEM((1, D), F32),
            pltpu.VMEM((LEN, 128), F32),
            pltpu.VMEM((LEN, 128), F32),
            pltpu.VMEM((NZ * NX, 128), F32),
            pltpu.VMEM((NZ * NX, 128), F32),
            pltpu.VMEM((2, 128), F32),
            pltpu.VMEM((8, 128), F32),
            pltpu.VMEM((1, 128), F32),
            pltpu.VMEM((1, 128), F32),
            pltpu.VMEM((8, ROWS, D), BF16),
            pltpu.VMEM((D, NCOL), BF16),
            pltpu.VMEM((LEN, 512), BF16),
            pltpu.VMEM((LEN, 128), F32),
            pltpu.VMEM((2, LEN, 128), BF16),
            pltpu.VMEM((NZ, 4, 256, 128), BF16),
            pltpu.VMEM((4, 128, 128), BF16),
            pltpu.VMEM((NX, 4, 128, 128), BF16),
            pltpu.VMEM((NX, 4, 128, 256), BF16),
            pltpu.VMEM((NX, 4, 144, 256), F32),
            pltpu.VMEM((NX, 4, 8, 256), F32),
            pltpu.VMEM((2, 2, 128, 256), BF16),
            pltpu.VMEM((2, 2, 128, 256), BF16),
            pltpu.VMEM((2, 2, 8, 256), F32),
            pltpu.VMEM((2, 2, 8, 256), F32),
            pltpu.VMEM((2, 2, 2, 128, 256), BF16),
            pltpu.VMEM((2, 2, 2, 128, 256), BF16),
            pltpu.VMEM((2, 2, 2, 8, 256), F32),
            pltpu.VMEM((2, 2, 2, 8, 256), F32),
            pltpu.VMEM((NX, 2, 144, 128), BF16),
            pltpu.VMEM((2, 136, 128), F32),
            pltpu.VMEM((2, 136, 128), F32),
            pltpu.VMEM((2, 144, 128), BF16),
            pltpu.VMEM((2, 144, 128), BF16),
            pltpu.VMEM((2, 128, 128), BF16),
            pltpu.VMEM((2, 128, 128), BF16),
            pltpu.VMEM((LEN, 128), BF16),
            pltpu.VMEM((LEN, 128), BF16),
            pltpu.VMEM((8, ROWS, 128), BF16),
            pltpu.VMEM((8, ROWS, 128), BF16),
            pltpu.VMEM((1024, D), BF16),
            pltpu.VMEM((1024, D), BF16),
            dma((19,)), dma((14,)), dma((14,)),
            dma((4, 4)), dma((4, 4)), dma((4, 4)), dma((4, 4)), dma((NX, 4)), dma((NX, 4)),
            dma((NX,)), dma((NX,)), dma((2,)), dma((2,)), dma((2, 4)), dma((2,)),
            dma((2, 2)), dma((2, 2)), dma((2, 2, 2)), dma((2, 2, 2)),
            dma((8,)), dma((8,)), dma((8,)), dma((8,)),
        ],
        compiler_params=pltpu.CompilerParams(
            collective_id=0, has_side_effects=True, vmem_limit_bytes=VMEM_LIMIT,
        ),
        name="layer",
    )(
        lambdas.reshape(1, 1), tokens, norm_gain.reshape(1, D), *rotary_tables(), gate_leak,
        log_decay.reshape(8, 128), att_gain.reshape(1, 128), rec_gain.reshape(1, 128), *weights,
        out_rec, out_att,
    )


def solution(mesh):
    torus = Mesh(mesh.devices.reshape(NZ, NX, mesh.shape["tp"]), SP_TP)
    tp = P(None, "tp")
    in_specs = (
        P(SP_TP, None), P(), tp, tp, tp, tp, tp, P(None, SP, "tp"), P(), tp, tp, tp, P("tp"), P(),
        P(), P(),
    )
    return jax.shard_map(
        on_device, mesh=torus, in_specs=in_specs, out_specs=P(SP_TP, None), check_vma=False
    )
```

```python
import math

import jax
import jax.numpy as jnp
import numpy as np
from jax import lax
from jax.experimental import pallas as pl
from jax.experimental.pallas import tpu as pltpu
from jax.sharding import Mesh
from jax.sharding import PartitionSpec as P

HK = 128
AK = 64
BLOCK = 64
SP = ("sp_0", "sp_1")
SP_TP = ("sp_0", "sp_1", "tp")
NZ, NX, NY = 8, 4, 4
ROWS = 64
LEN = 512
D = 2048
NCOL = 896
EPS = 1e-06
THETA = 500000.0
LOG2E = 1.4426950408889634
F32 = jnp.float32
BF16 = jnp.bfloat16
MESH = pl.DeviceIdType.MESH
VMEM_SPEC = pl.BlockSpec(memory_space=pltpu.VMEM)
ANY_SPEC = pl.BlockSpec(memory_space=pl.ANY)
VMEM_LIMIT = 60 * 1024 * 1024


def remote(src, dst, send_sem, recv_sem, device):
    return pltpu.make_async_remote_copy(
        src_ref=src,
        dst_ref=dst,
        send_sem=send_sem,
        recv_sem=recv_sem,
        device_id=device,
        device_id_type=MESH,
    )


def meet(devices):
    barrier = pltpu.get_barrier_semaphore()
    for device in devices:
        pl.semaphore_signal(barrier, inc=1, device_id=device, device_id_type=MESH)
    pl.semaphore_wait(barrier, len(devices))


def dot(a, b):
    return jnp.dot(a, b, preferred_element_type=F32)


def dot_nt(a, b):
    return lax.dot_general(a, b, (((1,), (1,)), ((), ())), preferred_element_type=F32)


def rotary_tables():
    i = np.arange(AK // 2, dtype=np.float64)
    freq = THETA ** (-(i * 2.0 / AK))
    freq = np.tile(freq, 4)[None, :]
    within = np.arange(LEN, dtype=np.float64)[:, None] * freq
    starts = np.arange(NZ * NX, dtype=np.float64)[:, None] * LEN * freq
    tables = [f(v) for v in (within, starts) for f in (np.cos, np.sin)]
    return jnp.asarray(np.concatenate(tables, axis=0).astype(np.float32))


def exact_cumulative(triangle, logs):
    first = logs.astype(BF16)
    rest = logs - first.astype(F32)
    second = rest.astype(BF16)
    third = (rest - second.astype(F32)).astype(BF16)
    return dot(triangle, first) + dot(triangle, second) + dot(triangle, third)


def recurrence(rec_ref, leak_ref, decay_ref, out_ref, read_ref, state_ref):
    blocks = LEN // BLOCK
    raw_q = rec_ref[:, 0:128].astype(F32)
    rq = raw_q / (1.0 + jnp.exp(-raw_q))
    value = rec_ref[:, 384:512]
    value_t = value.astype(F32).T.astype(BF16)
    row = lax.broadcasted_iota(jnp.int32, (256, 256), 0)
    col = lax.broadcasted_iota(jnp.int32, (256, 256), 1)
    same = (row // BLOCK) == (col // BLOCK)
    upper = lax.broadcasted_iota(jnp.int32, (128, 1), 0) < BLOCK
    total_out = None
    for side in range(2):
        raw = rec_ref[:, 128 * (side + 1) : 128 * (side + 2)].astype(F32)
        key = leak_ref[side : side + 1, :] / (1.0 + jnp.exp(raw))
        added_log = jnp.concatenate(
            [
                jnp.broadcast_to(decay_ref[4 * side + k : 4 * side + k + 1, :], (128, 128)).T
                for k in range(4)
            ],
            axis=0,
        )
        logs = jnp.log1p(-key) + added_log
        mask = same & ((row >= col) if side == 0 else (row <= col))
        triangle = mask.astype(F32).astype(BF16)
        cum = jnp.concatenate(
            [exact_cumulative(triangle, logs[256 * h : 256 * (h + 1)]) for h in range(2)], axis=0
        )
        cum3 = cum.reshape(blocks, BLOCK, 128)
        at_mid, at_last = (BLOCK // 2 - 1, BLOCK - 1) if side == 0 else (BLOCK // 2, 0)
        middle = cum3[:, at_mid : at_mid + 1, :]
        last = cum3[:, at_last : at_last + 1, :]
        key3, rq3 = key.reshape(cum3.shape), rq.reshape(cum3.shape)
        qs = (rq3 * jnp.exp(cum3 - middle)).reshape(LEN, 128).astype(BF16)
        ks = (key3 * jnp.exp(middle - cum3)).reshape(LEN, 128).astype(BF16)
        kl = (key3 * jnp.exp(last - cum3)).reshape(LEN, 128)
        qc = (rq3 * jnp.exp(cum3)).reshape(LEN, 128).astype(BF16)
        within = []
        for h in range(2):
            part = slice(256 * h, 256 * (h + 1))
            scores = jnp.where(mask, dot_nt(qs[part], ks[part]), 0.0).astype(BF16)
            within.append(dot(scores, value[part]))
        order = range(blocks) if side == 0 else reversed(range(blocks))
        state = jnp.zeros((128, 128), F32)
        carried, before = [None] * blocks, [None] * blocks
        running = jnp.zeros((1, 128), F32)
        for b in order:
            carried[b] = dot_nt(qc[BLOCK * b : BLOCK * (b + 1)], state.astype(BF16))
            pair = b // 2
            keys = kl[128 * pair : 128 * (pair + 1)]
            keys = jnp.where(upper if b % 2 == 0 else ~upper, keys, 0.0).astype(BF16)
            added = dot(value_t[:, 128 * pair : 128 * (pair + 1)], keys)
            before[b] = running
            running = running + last[b]
            state = state * jnp.exp(last[b]) + added
        out = jnp.concatenate(within, axis=0) + jnp.concatenate(carried, axis=0)
        total_out = out if total_out is None else total_out + out
        reach = (cum3 + jnp.stack(before, axis=0)).reshape(LEN, 128)
        read_ref[side] = (rq * jnp.exp(reach)).astype(BF16)
        state_ref[side, 0:128, :] = state.astype(BF16)
        state_ref[side, 128:144, :] = jnp.broadcast_to(jnp.exp(running), (16, 128)).astype(BF16)
    out_ref[...] = total_out


def flash(plan, kvbuf, qz, acc, peak):
    ones = jnp.ones((16, 256), BF16)
    tiles, ahead, behind = [], {}, {}
    for item in plan:
        if item[0] == "pre":
            ahead.setdefault(len(tiles), []).append(item[1])
        elif item[0] == "post":
            behind.setdefault(len(tiles) - 1, []).append(item[1])
        else:
            tiles += [(item[0], k, item[1], item[2]) for k in range(4)]
    count = len(tiles)
    tops, olds, sums = [None] * count, [None] * count, [None] * count
    scores, weights = [{} for _ in tiles], [{} for _ in tiles]

    def has(i, n):
        return 0 <= i < count and n < len(tiles[i][2])

    def score(i, n):
        q, k, pieces, first = tiles[i]
        if n == 0 and not first:
            before = [b for b in range(max(0, i - 2), i) if tiles[b][:2] == (q, k)]
            olds[i] = tops[i] = tops[before[-1]] if before else peak[q, k, 0:1, :]
        r, s = pieces[n]
        keys = jnp.concatenate([kvbuf[r, 2 * s, 0:128, :], kvbuf[r, 2 * s + 1, 0:128, :]], axis=0)
        scores[i][n] = dot(keys, qz[q, k])
        here = jnp.max(scores[i][n], axis=0, keepdims=True)
        tops[i] = here if tops[i] is None else jnp.maximum(tops[i], here)

    def weigh(i, n):
        weights[i][n] = jnp.exp2(scores[i].pop(n) - tops[i]).astype(BF16)

    def gather(i, n):
        q, k, pieces, first = tiles[i]
        r, s = pieces[n]
        values = [kvbuf[r, 2 * s, 128:256, :], kvbuf[r, 2 * s + 1, 128:256, :]]
        values = jnp.concatenate(values, axis=1)
        term = dot(jnp.concatenate([values, ones], axis=0), weights[i].pop(n))
        sums[i] = term if sums[i] is None else sums[i] + term
        if n == len(pieces) - 1:
            if first:
                acc[q, k] = sums[i]
            else:
                acc[q, k] = acc[q, k] * jnp.exp2(olds[i] - tops[i]) + sums[i]
            peak[q, k] = jnp.broadcast_to(tops[i], (8, 256))

    longest = max(len(t[2]) for t in tiles)
    for i in range(-2, count):
        for call in ahead.get(i + 2, []):
            call()
        for n in range(longest):
            for stage, at in ((score, i + 2), (weigh, i + 1), (gather, i)):
                if has(at, n):
                    stage(at, n)
        for call in behind.get(i, []):
            call()


REACH = (2, 1, 3, 0)


def layer_kernel(
    lam_ref, tok_ref, *refs,
):
    small, weights, (wrec_ref, watt_ref, out_ref) = refs[:6], refs[6:13], refs[13:16]
    (
        gain_ref, tables, leak_ref, decay_ref, attgain_ref, recgain_ref,
        xbuf, wbuf, recraw, recout, read,
        kvbuf, qown, qbuf, qz, acc, peak, farout, farin, farouts, farins, nearout, nearin,
        nearouts, nearins, stbuf, totals, inside, chain_in, chain_out, half_in, half_out,
        mixrec, mixatt, gotrec, gotatt, wr, wa,
        wsem, y_send, y_recv, k_send, k_recv, q_send, q_recv, s_send, s_recv,
        c_send, c_recv, h_send, h_recv, f_send, f_recv, n_send, n_recv,
        t_send, t_recv,
    ) = refs[16:]
    z, x, t = lax.axis_index("sp_0"), lax.axis_index("sp_1"), lax.axis_index("tp")
    y, c = t // 2, t % 2
    right = lax.rem(y + 1, NY) * 2 + c
    left = lax.rem(y + NY - 1, NY) * 2 + c
    far = lax.rem(y + 2, NY) * 2 + c
    partner = 2 * y + 1 - c
    up = {"sp_0": lax.rem(z + 1, NZ)}
    down = {"sp_0": lax.rem(z + NZ - 1, NZ)}
    beside = [None] + [{"sp_1": lax.rem(x + p, NX)} for p in range(1, NX)]
    mates = [None] + [lax.rem(t + d, 8) for d in range(1, 8)]

    own_load = pltpu.make_async_copy(tok_ref, xbuf.at[t], wsem.at[0])
    own_load.start()
    loads = [
        pltpu.make_async_copy(w, wbuf.at[:, pl.ds(128 * k, 128)], wsem.at[1])
        for k, w in enumerate(weights)
    ]
    homes = (gain_ref, tables, leak_ref, decay_ref, attgain_ref, recgain_ref)
    small_loads = [
        pltpu.make_async_copy(a, b, wsem.at[4 + k]) for k, (a, b) in enumerate(zip(small, homes))
    ]
    late_loads = [
        pltpu.make_async_copy(wrec_ref, wr, wsem.at[2]),
        pltpu.make_async_copy(watt_ref, wa, wsem.at[3]),
    ]
    for load in loads + small_loads:
        load.start()
    meet([up, down] + beside[1:] + [{"tp": m} for m in mates[1:]])

    def drain(ref, sem):
        pltpu.make_async_copy(ref, ref, sem).wait()

    own_load.wait()

    half = ROWS // 2
    part = (pl.ds(0, half), pl.ds(half, half))
    own = [xbuf.at[t, p] for p in part]

    def to(src, slot, k, number, device):
        return remote(
            src, xbuf.at[slot, part[k]], y_send, y_recv.at[number], {"tp": device}
        )

    def launch(src, slot, k, number, device):
        to(src, slot, k, number, device).start()

    def arrived(slot, k, number):
        to(own[k], slot, k, number, right).wait_recv()

    launch(own[0], t, 0, 0, right)
    launch(own[1], t, 1, 3, left)
    launch(own[1], t, 1, 1, right)
    launch(own[0], t, 0, 2, left)
    launch(own[0], t, 0, 4, partner)
    launch(own[1], t, 1, 5, partner)
    for load in small_loads:
        load.wait()
    drain(wbuf, wsem.at[1])
    for load in late_loads:
        load.start()

    block = z * NX + x
    cb = tables[pl.ds(2 * LEN + block, 1), :]
    sb = tables[pl.ds(2 * LEN + NZ * NX + block, 1), :]
    lane = lax.broadcasted_iota(jnp.int32, (1, 128), 1)
    low = lax.rem(lane, 64) < 32

    def turned(v, cosine, sine):
        other = jnp.where(low, pltpu.roll(v, 96, 1), pltpu.roll(v, 32, 1))
        return v * cosine + other * sine

    def arrival(step, j):
        return k_recv.at[4 * step + j if step < 3 else 12]

    def start_right(step, j):
        src = kvbuf.at[(NZ - step) % NZ, j]
        remote(src, kvbuf.at[NZ - 1 - step, j], k_send, arrival(step, j), up).start()

    def start_left(step, j):
        src = kvbuf.at[step, j]
        remote(src, kvbuf.at[step + 1, j], k_send, arrival(step, j), down).start()

    def forward(step, j):
        drain(kvbuf.at[0, 0:2], arrival(step - 1, j))
        if step < 3 or j < 2:
            start_right(step, j)
        if step < 3 or j >= 2:
            start_left(step, j)

    def process(yy, j):
        pair = xbuf[pl.ds(2 * yy, 2)].reshape(2 * ROWS, D).astype(F32)
        scale = lax.rsqrt(jnp.mean(pair * pair, axis=1, keepdims=True) + EPS)
        normed = (pair * scale * gain_ref[...]).astype(BF16)
        out = dot(normed, wbuf[...])
        rows = pl.ds(pl.multiple_of(yy * 128, 128), 128)
        ca = tables[rows, :]
        sa = tables[pl.ds(pl.multiple_of(LEN + yy * 128, 128), 128), :]
        cosine = ca * cb - sa * sb
        sine = sa * cb + ca * sb
        signed = jnp.where(low, -sine, sine)
        raw = out[:, 512:].astype(BF16).astype(F32)
        kvbuf[0, j, 0:128, :] = turned(raw[:, 128:256], cosine, signed).astype(BF16)
        kvbuf[0, j, 128:256, :] = raw[:, 256:384].T.astype(BF16)
        query = turned(raw[:, 0:128], cosine, signed) * (AK**-0.5 * LOG2E)
        qown[j] = query.T.astype(BF16)
        recraw[rows, :] = out[:, :512].astype(BF16)
        start_right(0, j)
        start_left(0, j)
        for p in (2, 1, 3):
            remote(
                qown.at[j], qbuf.at[NX - p, j], q_send, q_recv.at[NX - p], beside[p]
            ).start()

    arrived(partner, 0, 4)
    arrived(partner, 1, 5)
    process(y, 0)
    arrived(left, 0, 0)
    launch(xbuf.at[left, part[0]], left, 0, 6, right)
    launch(xbuf.at[left, part[0]], left, 0, 8, partner)
    arrived(right, 1, 3)
    launch(xbuf.at[right, part[1]], right, 1, 7, left)
    launch(xbuf.at[right, part[1]], right, 1, 9, partner)
    forward(1, 0)
    arrived(left, 1, 1)
    launch(xbuf.at[left, part[1]], left, 1, 10, partner)
    arrived(right, 0, 2)
    launch(xbuf.at[right, part[0]], right, 0, 11, partner)
    mate_l, mate_r, mate_far = left + 1 - 2 * c, right + 1 - 2 * c, far + 1 - 2 * c
    arrived(mate_l, 0, 8)
    arrived(mate_l, 1, 10)
    process(left // 2, 1)
    forward(2, 0)
    arrived(mate_r, 1, 9)
    arrived(mate_r, 0, 11)
    process(right // 2, 2)
    arrived(far, 0, 6)
    launch(xbuf.at[far, part[0]], far, 0, 12, partner)
    arrived(far, 1, 7)
    launch(xbuf.at[far, part[1]], far, 1, 13, partner)
    arrived(mate_far, 0, 12)
    arrived(mate_far, 1, 13)
    process(far // 2, 3)
    forward(1, 1)
    forward(3, 0)

    recurrence(recraw, leak_ref, decay_ref, recout, read, stbuf.at[0])
    for p in range(1, NX):
        remote(stbuf.at[0], stbuf.at[NX - p], s_send, s_recv, beside[p]).start()
    forward(1, 2)

    upper = lax.broadcasted_iota(jnp.int32, (128, 1), 0) < AK

    def spread(q, source):
        for h in range(2):
            piece = jnp.concatenate([source(2 * h), source(2 * h + 1)], axis=1).astype(F32)
            qz[q, h] = jnp.where(upper, piece, 0.0).astype(BF16)
            qz[q, 2 + h] = jnp.where(upper, 0.0, piece).astype(BF16)

    def pieces(*slots):
        return [(r, s) for r in slots for s in range(2)]

    spread(3, lambda j: qown[j])

    def queries(q):
        def call():
            p = REACH[q]
            drain(qbuf.at[p], q_recv.at[p])
            spread(q, lambda j: qbuf[p, j])

        return call

    def join_states():
        drain(stbuf.at[1:4], s_recv)
        for side in range(2):
            order = range(NX) if side == 0 else reversed(range(NX))
            total_s, total_d = jnp.zeros((128, 128), F32), jnp.ones((1, 128), F32)
            inside_s, inside_d = total_s, total_d
            for k in order:
                rel = lax.rem(k - x + NX, NX)
                piece_s = stbuf[rel, side, 0:128, :].astype(F32)
                piece_d = stbuf[rel, side, 128:144, :].astype(F32)[0:1, :]
                total_s = total_s * piece_d + piece_s
                total_d = total_d * piece_d
                passed = (k < x) if side == 0 else (k > x)
                inside_s = jnp.where(passed, total_s, inside_s)
                inside_d = jnp.where(passed, total_d, inside_d)
            totals[side, 0:128, :] = total_s
            totals[side, 128:136, :] = jnp.broadcast_to(total_d, (8, 128))
            inside[side, 0:128, :] = inside_s
            inside[side, 128:136, :] = jnp.broadcast_to(inside_d, (8, 128))
        chain(0)

    quarter = NZ // 2
    place = (lax.rem(z, quarter), quarter - 1 - lax.rem(z, quarter))
    giver = (quarter - 1, quarter)
    takes = (z >= quarter, z < quarter)

    for side in range(2):

        @pl.when(place[side] == 0)
        def _():
            chain_in[side, 0:128, :] = jnp.zeros((128, 128), BF16)
            chain_in[side, 128:144, :] = jnp.ones((16, 128), BF16)

        @pl.when(jnp.logical_not(takes[side]))
        def _():
            half_in[side] = jnp.zeros((128, 128), BF16)

    def chain_copy(side):
        return remote(
            chain_out.at[side], chain_in.at[side], c_send.at[side], c_recv.at[side],
            up if side == 0 else down,
        )

    def half_copy(side, k):
        device = quarter + k if side == 0 else quarter - 1 - k
        return remote(
            half_out.at[side], half_in.at[side], h_send.at[side], h_recv.at[side],
            {"sp_0": device},
        )

    def chain(hop):
        for side in range(2):

            @pl.when(place[side] == hop)
            def _():
                if hop > 0:
                    chain_copy(side).wait_recv()
                entered = chain_in[side].astype(F32)
                decay = totals[side, 128:129, :]
                state = entered[0:128, :] * decay + totals[side, 0:128, :]
                if hop < quarter - 1:
                    chain_out[side, 0:128, :] = state.astype(BF16)
                    chain_out[side, 128:144, :] = (entered[128:144, :] * decay).astype(BF16)
                    chain_copy(side).start()
                else:

                    @pl.when(z == giver[side])
                    def _():
                        half_out[side] = state.astype(BF16)
                        for k in range(quarter):
                            half_copy(side, k).start()

    shallow = lax.broadcasted_iota(jnp.int32, (8, 256), 0) < 4

    def pack(q, m, out, stat):
        for h in range(2):
            k = 2 * m + h
            total = acc[q, k, 128:129, :]
            out[h] = (acc[q, k, 0:128, :] * (1.0 / total)).astype(BF16)
            stat[h] = jnp.where(shallow, peak[q, k], acc[q, k, 128:136, :])

    def pack_merged(q, m, out, stat, other, others):
        for h in range(2):
            k = 2 * m + h
            top_a, top_b = peak[q, k, 0:1, :], others[h, 0:1, :]
            top = jnp.maximum(top_a, top_b)
            scale = jnp.exp2(top_a - top)
            share = others[h, 4:5, :] * jnp.exp2(top_b - top)
            total = acc[q, k, 128:129, :] * scale + share
            inverse = 1.0 / total
            merged = acc[q, k, 0:128, :] * (scale * inverse)
            merged = merged + other[h].astype(F32) * (share * inverse)
            out[h] = merged.astype(BF16)
            stat[h] = jnp.where(shallow, top, total)

    def far_copies(m):
        device = beside[1] if m == 0 else beside[3]
        return [
            remote(farout.at[m], farin.at[m], f_send.at[0], f_recv.at[m, 0], device),
            remote(farouts.at[m], farins.at[m], f_send.at[1], f_recv.at[m, 1], device),
        ]

    def near_copies(w, m):
        device = beside[1] if w == 0 else beside[3]
        return [
            remote(nearout.at[w, m], nearin.at[w, m], n_send.at[0], n_recv.at[w, m, 0], device),
            remote(nearouts.at[w, m], nearins.at[w, m], n_send.at[1], n_recv.at[w, m, 1], device),
        ]

    def post(pair):
        for copy in pair:
            copy.start()

    def received(pair):
        for copy in pair:
            copy.wait_recv()

    def give_far():
        for m in range(2):
            pack(0, m, farout.at[m], farouts.at[m])
            post(far_copies(m))

    def give_near(w, m):
        def call():
            pack(w + 1, m, nearout.at[w, m], nearouts.at[w, m])
            post(near_copies(w, m))

        return call

    def merge_near(w, m):
        received(far_copies(w))
        pack_merged(w + 1, m, nearout.at[w, m], nearouts.at[w, m], farin.at[w], farins.at[w])
        post(near_copies(w, m))

    def pre(call, *args):
        return ("pre", lambda: call(*args))

    flash(
        [
            (3, pieces(0), True),
            ("pre", queries(0)), (0, pieces(0), True),
            ("pre", queries(1)), pre(forward, 1, 3), (1, pieces(0), True),
            ("pre", queries(2)), (2, pieces(0), True),
            (0, pieces(7, 1), False),
            pre(forward, 2, 1), (1, pieces(7, 1), False),
            pre(forward, 2, 2), (2, pieces(7, 1), False),
            pre(forward, 2, 3), (3, pieces(7, 1), False),
            pre(join_states), (0, pieces(6, 2), False),
            pre(forward, 3, 1), (1, pieces(6, 2), False),
            pre(forward, 3, 2), (2, pieces(6, 2), False),
            pre(forward, 3, 3), pre(chain, 1), (1, pieces(5, 3), False),
            (2, pieces(5, 3), False),
            (0, pieces(5, 3), False),
            pre(drain, kvbuf.at[0], arrival(3, 0)), pre(chain, 2),
            (0, pieces(4), False),
            ("post", give_far),
            (1, pieces(4), False),
            ("post", give_near(0, 1)),
            (2, pieces(4), False),
            ("post", give_near(1, 0)),
            (3, pieces(6, 2), False),
            pre(chain, 3), (3, pieces(5, 3, 4), False),
        ],
        kvbuf, qz, acc, peak,
    )
    merge_near(0, 0)
    merge_near(1, 1)

    for side in range(2):

        @pl.when(takes[side])
        def _():
            half_copy(side, 0).wait_recv()

    out = recout[...]
    for side in range(2):
        entered = chain_in[side].astype(F32)
        entry = entered[0:128, :] + half_in[side].astype(F32) * entered[128:129, :]
        entry = entry * inside[side, 128:129, :] + inside[side, 0:128, :]
        out = out + dot_nt(read[side], entry.astype(BF16))
    out = out * lax.rsqrt(jnp.mean(out * out, axis=1, keepdims=True) + EPS) * recgain_ref[...]
    mixrec[...] = out.astype(BF16)

    def rows_of(device):
        return pl.ds(pl.multiple_of(device * ROWS, ROWS), ROWS)

    def deal(source, got, which):
        for d in range(1, 8):
            remote(
                source.at[rows_of(mates[d]), :], got.at[t], t_send.at[which], t_recv.at[which],
                {"tp": mates[d]},
            ).start()
        got[t] = source[rows_of(t), :]

    deal(mixrec, gotrec, 0)

    drain(xbuf.at[0:7], y_send)
    drain(kvbuf.at[0:7], k_send)
    drain(qbuf.at[0:3], q_send)
    drain(stbuf.at[0:3], s_send)
    drain(farout, f_send.at[0])
    drain(farouts, f_send.at[1])
    for load in late_loads:
        load.wait()
    for side in range(2):

        @pl.when(place[side] < quarter - 1)
        def _():
            chain_copy(side).wait_send()

        @pl.when(z == giver[side])
        def _():
            drain(qbuf.at[0], h_send.at[side])

    lam = lam_ref[0:1, 0:1]
    for w, m in ((0, 1), (1, 0), (0, 0), (1, 1)):
        received(near_copies(w, m))
    for h in range(2):
        maps = []
        for m in range(2):
            k = 2 * m + h
            tops = [peak[3, k, 0:1, :]] + [nearins[w, m, h, 0:1, :] for w in range(2)]
            sums = [acc[3, k, 128:129, :]] + [nearins[w, m, h, 4:5, :] for w in range(2)]
            top = jnp.maximum(jnp.maximum(tops[0], tops[1]), tops[2])
            shares = [a * jnp.exp2(b - top) for a, b in zip(sums, tops)]
            inverse = 1.0 / (shares[0] + shares[1] + shares[2])
            value = acc[3, k, 0:128, :] * (jnp.exp2(tops[0] - top) * inverse)
            for w in range(2):
                value = value + nearin[w, m, h].astype(F32) * (shares[w + 1] * inverse)
            maps.append(value)
        mixed = maps[0] - lam * maps[1]
        mixed = mixed * lax.rsqrt(jnp.mean(mixed * mixed, axis=0, keepdims=True) + EPS)
        rows = (mixed.T * attgain_ref[...]).astype(BF16)
        for half_of, yy in zip(range(2), ((y, left // 2), (right // 2, far // 2))[h]):
            at = pl.ds(pl.multiple_of(yy * 128, 128), 128)
            mixatt[at, :] = rows[128 * half_of : 128 * (half_of + 1), :]
    deal(mixatt, gotatt, 1)
    drain(nearout, n_send.at[0])
    drain(nearouts, n_send.at[1])
    drain(gotrec.at[0:7], t_recv.at[0])
    rec_term = dot(jnp.concatenate([gotrec[k] for k in range(8)], axis=1), wr[...])
    drain(gotatt.at[0:7], t_recv.at[1])
    att_term = dot(jnp.concatenate([gotatt[k] for k in range(8)], axis=1), wa[...])
    out_ref[...] = (rec_term + att_term).astype(BF16)
    drain(gotrec.at[0:7], t_send.at[0])
    drain(gotatt.at[0:7], t_send.at[1])


def on_device(
    tokens, norm_gain, rec_query, fwd_gate, bwd_gate, rec_value, gate_leak, log_decay, rec_gain,
    att_query, att_key, att_value, lambdas, att_gain, out_rec, out_att,
):
    weights = (rec_query, fwd_gate, bwd_gate, rec_value, att_query, att_key, att_value)
    dma = pltpu.SemaphoreType.DMA
    return pl.pallas_call(
        layer_kernel,
        out_shape=jax.ShapeDtypeStruct((ROWS, D), BF16),
        in_specs=[VMEM_SPEC] + [ANY_SPEC] * 16,
        out_specs=VMEM_SPEC,
        scratch_shapes=[
            pltpu.VMEM((1, D), F32),
            pltpu.VMEM((2 * LEN + 2 * NZ * NX, 128), F32),
            pltpu.VMEM((2, 128), F32),
            pltpu.VMEM((8, 128), F32),
            pltpu.VMEM((1, 128), F32),
            pltpu.VMEM((1, 128), F32),
            pltpu.VMEM((8, ROWS, D), BF16),
            pltpu.VMEM((D, NCOL), BF16),
            pltpu.VMEM((LEN, 512), BF16),
            pltpu.VMEM((LEN, 128), F32),
            pltpu.VMEM((2, LEN, 128), BF16),
            pltpu.VMEM((NZ, 4, 256, 128), BF16),
            pltpu.VMEM((4, 128, 128), BF16),
            pltpu.VMEM((NX, 4, 128, 128), BF16),
            pltpu.VMEM((NX, 4, 128, 256), BF16),
            pltpu.VMEM((NX, 4, 144, 256), F32),
            pltpu.VMEM((NX, 4, 8, 256), F32),
            pltpu.VMEM((2, 2, 128, 256), BF16),
            pltpu.VMEM((2, 2, 128, 256), BF16),
            pltpu.VMEM((2, 2, 8, 256), F32),
            pltpu.VMEM((2, 2, 8, 256), F32),
            pltpu.VMEM((2, 2, 2, 128, 256), BF16),
            pltpu.VMEM((2, 2, 2, 128, 256), BF16),
            pltpu.VMEM((2, 2, 2, 8, 256), F32),
            pltpu.VMEM((2, 2, 2, 8, 256), F32),
            pltpu.VMEM((NX, 2, 144, 128), BF16),
            pltpu.VMEM((2, 136, 128), F32),
            pltpu.VMEM((2, 136, 128), F32),
            pltpu.VMEM((2, 144, 128), BF16),
            pltpu.VMEM((2, 144, 128), BF16),
            pltpu.VMEM((2, 128, 128), BF16),
            pltpu.VMEM((2, 128, 128), BF16),
            pltpu.VMEM((LEN, 128), BF16),
            pltpu.VMEM((LEN, 128), BF16),
            pltpu.VMEM((8, ROWS, 128), BF16),
            pltpu.VMEM((8, ROWS, 128), BF16),
            pltpu.VMEM((1024, D), BF16),
            pltpu.VMEM((1024, D), BF16),
            dma((10,)), dma, dma((14,)), dma, dma((13,)), dma, dma((NX,)), dma, dma,
            dma((2,)), dma((2,)), dma((2,)), dma((2,)),
            dma((2,)), dma((2, 2)), dma((2,)), dma((2, 2, 2)), dma((2,)), dma((2,)),
        ],
        compiler_params=pltpu.CompilerParams(
            collective_id=0, has_side_effects=True, vmem_limit_bytes=VMEM_LIMIT,
        ),
        name="layer",
    )(
        lambdas.reshape(1, 1), tokens, norm_gain.reshape(1, D), rotary_tables(), gate_leak,
        log_decay.reshape(8, 128), att_gain.reshape(1, 128), rec_gain.reshape(1, 128), *weights,
        out_rec, out_att,
    )


def solution(mesh):
    torus = Mesh(mesh.devices.reshape(NZ, NX, mesh.shape["tp"]), SP_TP)
    tp = P(None, "tp")
    in_specs = (
        P(SP_TP, None), P(), tp, tp, tp, tp, tp, P(None, SP, "tp"), P(), tp, tp, tp, P("tp"), P(),
        P(), P(),
    )
    return jax.shard_map(
        on_device, mesh=torus, in_specs=in_specs, out_specs=P(SP_TP, None), check_vma=False
    )
```

```python
import math

import jax
import jax.numpy as jnp
import numpy as np
from jax import lax
from jax.experimental import pallas as pl
from jax.experimental.pallas import tpu as pltpu
from jax.sharding import Mesh
from jax.sharding import PartitionSpec as P

HK = 128
AK = 64
BLOCK = 64
SP = ("sp_0", "sp_1")
SP_TP = ("sp_0", "sp_1", "tp")
NZ, NX, NY = 8, 4, 4
ROWS = 64
LEN = 512
D = 2048
NCOL = 896
EPS = 1e-06
THETA = 500000.0
LOG2E = 1.4426950408889634
F32 = jnp.float32
BF16 = jnp.bfloat16
MESH = pl.DeviceIdType.MESH
VMEM_SPEC = pl.BlockSpec(memory_space=pltpu.VMEM)
ANY_SPEC = pl.BlockSpec(memory_space=pl.ANY)
VMEM_LIMIT = 60 * 1024 * 1024


def remote(src, dst, send_sem, recv_sem, device):
    return pltpu.make_async_remote_copy(
        src_ref=src,
        dst_ref=dst,
        send_sem=send_sem,
        recv_sem=recv_sem,
        device_id=device,
        device_id_type=MESH,
    )


def meet(devices):
    barrier = pltpu.get_barrier_semaphore()
    for device in devices:
        pl.semaphore_signal(barrier, inc=1, device_id=device, device_id_type=MESH)
    pl.semaphore_wait(barrier, len(devices))


def dot(a, b):
    return jnp.dot(a, b, preferred_element_type=F32)


def dot_nt(a, b):
    return lax.dot_general(a, b, (((1,), (1,)), ((), ())), preferred_element_type=F32)


def rotary_tables():
    i = np.arange(AK // 2, dtype=np.float64)
    freq = THETA ** (-(i * 2.0 / AK))
    freq = np.tile(freq, 4)[None, :]
    within = np.arange(LEN, dtype=np.float64)[:, None] * freq
    starts = np.arange(NZ * NX, dtype=np.float64)[:, None] * LEN * freq
    tables = [f(v) for v in (within, starts) for f in (np.cos, np.sin)]
    return jnp.asarray(np.concatenate(tables, axis=0).astype(np.float32))


def exact_cumulative(triangle, logs):
    first = logs.astype(BF16)
    rest = logs - first.astype(F32)
    second = rest.astype(BF16)
    third = (rest - second.astype(F32)).astype(BF16)
    return dot(triangle, first) + dot(triangle, second) + dot(triangle, third)


def recurrence(rec_ref, leak_ref, decay_ref, out_ref, read_ref, state_ref, done):
    blocks = LEN // BLOCK
    raw_q = rec_ref[:, 0:128].astype(F32)
    rq = raw_q / (1.0 + jnp.exp(-raw_q))
    value = rec_ref[:, 384:512]
    value_t = value.astype(F32).T.astype(BF16)
    row = lax.broadcasted_iota(jnp.int32, (256, 256), 0)
    col = lax.broadcasted_iota(jnp.int32, (256, 256), 1)
    same = (row // BLOCK) == (col // BLOCK)
    upper = lax.broadcasted_iota(jnp.int32, (128, 1), 0) < BLOCK
    total_out = None
    for side in range(2):
        raw = rec_ref[:, 128 * (side + 1) : 128 * (side + 2)].astype(F32)
        key = leak_ref[side : side + 1, :] / (1.0 + jnp.exp(raw))
        added_log = jnp.concatenate(
            [
                jnp.broadcast_to(decay_ref[4 * side + k : 4 * side + k + 1, :], (128, 128)).T
                for k in range(4)
            ],
            axis=0,
        )
        logs = jnp.log1p(-key) + added_log
        mask = same & ((row >= col) if side == 0 else (row <= col))
        triangle = mask.astype(F32).astype(BF16)
        cum = jnp.concatenate(
            [exact_cumulative(triangle, logs[256 * h : 256 * (h + 1)]) for h in range(2)], axis=0
        )
        cum3 = cum.reshape(blocks, BLOCK, 128)
        at_mid, at_last = (BLOCK // 2 - 1, BLOCK - 1) if side == 0 else (BLOCK // 2, 0)
        middle = cum3[:, at_mid : at_mid + 1, :]
        last = cum3[:, at_last : at_last + 1, :]
        key3, rq3 = key.reshape(cum3.shape), rq.reshape(cum3.shape)
        qs = (rq3 * jnp.exp(cum3 - middle)).reshape(LEN, 128).astype(BF16)
        ks = (key3 * jnp.exp(middle - cum3)).reshape(LEN, 128).astype(BF16)
        kl = (key3 * jnp.exp(last - cum3)).reshape(LEN, 128)
        qc = (rq3 * jnp.exp(cum3)).reshape(LEN, 128).astype(BF16)
        within = []
        for h in range(2):
            part = slice(256 * h, 256 * (h + 1))
            scores = jnp.where(mask, dot_nt(qs[part], ks[part]), 0.0).astype(BF16)
            within.append(dot(scores, value[part]))
        order = range(blocks) if side == 0 else reversed(range(blocks))
        state = jnp.zeros((128, 128), F32)
        carried, before = [None] * blocks, [None] * blocks
        running = jnp.zeros((1, 128), F32)
        for b in order:
            carried[b] = dot_nt(qc[BLOCK * b : BLOCK * (b + 1)], state.astype(BF16))
            pair = b // 2
            keys = kl[128 * pair : 128 * (pair + 1)]
            keys = jnp.where(upper if b % 2 == 0 else ~upper, keys, 0.0).astype(BF16)
            added = dot(value_t[:, 128 * pair : 128 * (pair + 1)], keys)
            before[b] = running
            running = running + last[b]
            state = state * jnp.exp(last[b]) + added
        out = jnp.concatenate(within, axis=0) + jnp.concatenate(carried, axis=0)
        total_out = out if total_out is None else total_out + out
        reach = (cum3 + jnp.stack(before, axis=0)).reshape(LEN, 128)
        read_ref[side] = (rq * jnp.exp(reach)).astype(BF16)
        state_ref[side, 0:128, :] = state.astype(BF16)
        state_ref[side, 128:144, :] = jnp.broadcast_to(jnp.exp(running), (16, 128)).astype(BF16)
        done(side)
    out_ref[...] = total_out


def flash(plan, kvbuf, qz, acc, peak):
    ones = jnp.ones((16, 256), BF16)
    tiles, ahead, behind = [], {}, {}
    for item in plan:
        if item[0] == "pre":
            ahead.setdefault(len(tiles), []).append(item[1])
        elif item[0] == "post":
            behind.setdefault(len(tiles) - 1, []).append(item[1])
        else:
            tiles += [(item[0], k, item[1], item[2]) for k in (item[3:] or range(4))]
    count = len(tiles)
    tops, olds, sums = [None] * count, [None] * count, [None] * count
    scores, weights = [{} for _ in tiles], [{} for _ in tiles]

    def has(i, n):
        return 0 <= i < count and n < len(tiles[i][2])

    def score(i, n):
        q, k, pieces, first = tiles[i]
        if n == 0 and not first:
            before = [b for b in range(max(0, i - 2), i) if tiles[b][:2] == (q, k)]
            olds[i] = tops[i] = tops[before[-1]] if before else peak[q, k, 0:1, :]
        r, s = pieces[n]
        keys = jnp.concatenate([kvbuf[r, 2 * s, 0:128, :], kvbuf[r, 2 * s + 1, 0:128, :]], axis=0)
        scores[i][n] = dot(keys, qz[q, k])
        here = jnp.max(scores[i][n], axis=0, keepdims=True)
        tops[i] = here if tops[i] is None else jnp.maximum(tops[i], here)

    def weigh(i, n):
        weights[i][n] = jnp.exp2(scores[i].pop(n) - tops[i]).astype(BF16)

    def gather(i, n):
        q, k, pieces, first = tiles[i]
        r, s = pieces[n]
        values = [kvbuf[r, 2 * s, 128:256, :], kvbuf[r, 2 * s + 1, 128:256, :]]
        values = jnp.concatenate(values, axis=1)
        term = dot(jnp.concatenate([values, ones], axis=0), weights[i].pop(n))
        sums[i] = term if sums[i] is None else sums[i] + term
        if n == len(pieces) - 1:
            if first:
                acc[q, k] = sums[i]
            else:
                acc[q, k] = acc[q, k] * jnp.exp2(olds[i] - tops[i]) + sums[i]
            peak[q, k] = jnp.broadcast_to(tops[i], (8, 256))

    longest = max(len(t[2]) for t in tiles)
    for i in range(-2, count):
        for call in ahead.get(i + 2, []):
            call()
        for n in range(longest):
            for stage, at in ((score, i + 2), (weigh, i + 1), (gather, i)):
                if has(at, n):
                    stage(at, n)
        for call in behind.get(i, []):
            call()


REACH = (2, 1, 3, 0)


def layer_kernel(
    lam_ref, tok_ref, *refs,
):
    small, weights, (wrec_ref, watt_ref, out_ref) = refs[:6], refs[6:13], refs[13:16]
    (
        gain_ref, tables, leak_ref, decay_ref, attgain_ref, recgain_ref,
        xbuf, wbuf, recraw, recout, read,
        kvbuf, qown, qbuf, qz, acc, peak, farout, farin, farouts, farins, nearout, nearin,
        nearouts, nearins, stbuf, totals, inside, chain_in, chain_out, half_in, half_out,
        mixrec, mixatt, gotrec, gotatt, wr, wa,
        wsem, y_send, y_recv, k_send, k_recv, q_send, q_recv, s_send, s_recv,
        c_send, c_recv, h_send, h_recv, f_send, f_recv, n_send, n_recv,
        t_send, t_recv,
    ) = refs[16:]
    z, x, t = lax.axis_index("sp_0"), lax.axis_index("sp_1"), lax.axis_index("tp")
    y, c = t // 2, t % 2
    right = lax.rem(y + 1, NY) * 2 + c
    left = lax.rem(y + NY - 1, NY) * 2 + c
    far = lax.rem(y + 2, NY) * 2 + c
    partner = 2 * y + 1 - c
    up = {"sp_0": lax.rem(z + 1, NZ)}
    down = {"sp_0": lax.rem(z + NZ - 1, NZ)}
    beside = [None] + [{"sp_1": lax.rem(x + p, NX)} for p in range(1, NX)]
    mates = [None] + [lax.rem(t + d, 8) for d in range(1, 8)]

    own_load = pltpu.make_async_copy(tok_ref, xbuf.at[t], wsem.at[0])
    own_load.start()
    loads = [
        pltpu.make_async_copy(w, wbuf.at[:, pl.ds(128 * k, 128)], wsem.at[1])
        for k, w in enumerate(weights)
    ]
    homes = (gain_ref, tables, leak_ref, decay_ref, attgain_ref, recgain_ref)
    small_loads = [
        pltpu.make_async_copy(a, b, wsem.at[4 + k]) for k, (a, b) in enumerate(zip(small, homes))
    ]
    late_loads = [
        pltpu.make_async_copy(wrec_ref, wr, wsem.at[2]),
        pltpu.make_async_copy(watt_ref, wa, wsem.at[3]),
    ]
    for load in loads + small_loads:
        load.start()
    meet([up, down] + beside[1:] + [{"tp": m} for m in mates[1:]])

    def drain(ref, sem):
        pltpu.make_async_copy(ref, ref, sem).wait()

    own_load.wait()

    half = ROWS // 2
    part = (pl.ds(0, half), pl.ds(half, half))
    own = [xbuf.at[t, p] for p in part]

    def to(src, slot, k, number, device):
        return remote(
            src, xbuf.at[slot, part[k]], y_send, y_recv.at[number], {"tp": device}
        )

    def launch(src, slot, k, number, device):
        to(src, slot, k, number, device).start()

    def arrived(slot, k, number):
        to(own[k], slot, k, number, right).wait_recv()

    launch(own[0], t, 0, 0, right)
    launch(own[1], t, 1, 3, left)
    launch(own[1], t, 1, 1, right)
    launch(own[0], t, 0, 2, left)
    launch(own[0], t, 0, 4, partner)
    launch(own[1], t, 1, 5, partner)
    for load in small_loads:
        load.wait()
    drain(wbuf, wsem.at[1])
    for load in late_loads:
        load.start()

    block = z * NX + x
    cb = tables[pl.ds(2 * LEN + block, 1), :]
    sb = tables[pl.ds(2 * LEN + NZ * NX + block, 1), :]
    lane = lax.broadcasted_iota(jnp.int32, (1, 128), 1)
    low = lax.rem(lane, 64) < 32

    def turned(v, cosine, sine):
        other = jnp.where(low, pltpu.roll(v, 96, 1), pltpu.roll(v, 32, 1))
        return v * cosine + other * sine

    def arrival(step, j):
        return k_recv.at[4 * step + j if step < 3 else 12]

    def start_right(step, j):
        src = kvbuf.at[(NZ - step) % NZ, j]
        remote(src, kvbuf.at[NZ - 1 - step, j], k_send, arrival(step, j), up).start()

    def start_left(step, j):
        src = kvbuf.at[step, j]
        remote(src, kvbuf.at[step + 1, j], k_send, arrival(step, j), down).start()

    def forward(step, j):
        drain(kvbuf.at[0, 0:2], arrival(step - 1, j))
        if step < 3 or j < 2:
            start_right(step, j)
        if step < 3 or j >= 2:
            start_left(step, j)

    def process(yy, j):
        pair = xbuf[pl.ds(2 * yy, 2)].reshape(2 * ROWS, D).astype(F32)
        scale = lax.rsqrt(jnp.mean(pair * pair, axis=1, keepdims=True) + EPS)
        normed = (pair * scale * gain_ref[...]).astype(BF16)
        out = dot(normed, wbuf[...])
        rows = pl.ds(pl.multiple_of(yy * 128, 128), 128)
        ca = tables[rows, :]
        sa = tables[pl.ds(pl.multiple_of(LEN + yy * 128, 128), 128), :]
        cosine = ca * cb - sa * sb
        sine = sa * cb + ca * sb
        signed = jnp.where(low, -sine, sine)
        raw = out[:, 512:].astype(BF16).astype(F32)
        kvbuf[0, j, 0:128, :] = turned(raw[:, 128:256], cosine, signed).astype(BF16)
        kvbuf[0, j, 128:256, :] = raw[:, 256:384].T.astype(BF16)
        query = turned(raw[:, 0:128], cosine, signed) * (AK**-0.5 * LOG2E)
        qown[j] = query.T.astype(BF16)
        recraw[rows, :] = out[:, :512].astype(BF16)
        start_right(0, j)
        start_left(0, j)
        for p in (2, 1, 3):
            remote(
                qown.at[j], qbuf.at[NX - p, j], q_send, q_recv.at[NX - p], beside[p]
            ).start()

    arrived(partner, 0, 4)
    arrived(partner, 1, 5)
    process(y, 0)
    arrived(left, 0, 0)
    launch(xbuf.at[left, part[0]], left, 0, 6, right)
    launch(xbuf.at[left, part[0]], left, 0, 8, partner)
    arrived(right, 1, 3)
    launch(xbuf.at[right, part[1]], right, 1, 7, left)
    launch(xbuf.at[right, part[1]], right, 1, 9, partner)
    forward(1, 0)
    arrived(left, 1, 1)
    launch(xbuf.at[left, part[1]], left, 1, 10, partner)
    arrived(right, 0, 2)
    launch(xbuf.at[right, part[0]], right, 0, 11, partner)
    mate_l, mate_r, mate_far = left + 1 - 2 * c, right + 1 - 2 * c, far + 1 - 2 * c
    arrived(mate_l, 0, 8)
    arrived(mate_l, 1, 10)
    process(left // 2, 1)
    arrived(mate_r, 1, 9)
    arrived(mate_r, 0, 11)
    process(right // 2, 2)
    forward(2, 0)
    arrived(far, 0, 6)
    launch(xbuf.at[far, part[0]], far, 0, 12, partner)
    arrived(far, 1, 7)
    launch(xbuf.at[far, part[1]], far, 1, 13, partner)
    arrived(mate_far, 0, 12)
    arrived(mate_far, 1, 13)
    process(far // 2, 3)
    forward(1, 1)

    def one_side(side):
        for p in range(1, NX):
            remote(
                stbuf.at[0, side], stbuf.at[NX - p, side], s_send, s_recv, beside[p]
            ).start()
        if side == 0:
            forward(3, 0)
            forward(1, 2)

    recurrence(recraw, leak_ref, decay_ref, recout, read, stbuf.at[0], one_side)

    upper = lax.broadcasted_iota(jnp.int32, (128, 1), 0) < AK

    def spread(q, source):
        for h in range(2):
            piece = jnp.concatenate([source(2 * h), source(2 * h + 1)], axis=1).astype(F32)
            qz[q, h] = jnp.where(upper, piece, 0.0).astype(BF16)
            qz[q, 2 + h] = jnp.where(upper, 0.0, piece).astype(BF16)

    def pieces(*slots):
        return [(r, s) for r in slots for s in range(2)]

    spread(3, lambda j: qown[j])

    def queries(q):
        def call():
            p = REACH[q]
            drain(qbuf.at[p], q_recv.at[p])
            spread(q, lambda j: qbuf[p, j])

        return call

    def join_states():
        drain(stbuf.at[1:4], s_recv)
        for side in range(2):
            order = range(NX) if side == 0 else reversed(range(NX))
            total_s, total_d = jnp.zeros((128, 128), F32), jnp.ones((1, 128), F32)
            inside_s, inside_d = total_s, total_d
            for k in order:
                rel = lax.rem(k - x + NX, NX)
                piece_s = stbuf[rel, side, 0:128, :].astype(F32)
                piece_d = stbuf[rel, side, 128:144, :].astype(F32)[0:1, :]
                total_s = total_s * piece_d + piece_s
                total_d = total_d * piece_d
                passed = (k < x) if side == 0 else (k > x)
                inside_s = jnp.where(passed, total_s, inside_s)
                inside_d = jnp.where(passed, total_d, inside_d)
            totals[side, 0:128, :] = total_s
            totals[side, 128:136, :] = jnp.broadcast_to(total_d, (8, 128))
            inside[side, 0:128, :] = inside_s
            inside[side, 128:136, :] = jnp.broadcast_to(inside_d, (8, 128))
        chain(0)

    quarter = NZ // 2
    place = (lax.rem(z, quarter), quarter - 1 - lax.rem(z, quarter))
    giver = (quarter - 1, quarter)
    takes = (z >= quarter, z < quarter)

    for side in range(2):

        @pl.when(place[side] == 0)
        def _():
            chain_in[side, 0:128, :] = jnp.zeros((128, 128), BF16)
            chain_in[side, 128:144, :] = jnp.ones((16, 128), BF16)

        @pl.when(jnp.logical_not(takes[side]))
        def _():
            half_in[side] = jnp.zeros((128, 128), BF16)

    def chain_copy(side):
        return remote(
            chain_out.at[side], chain_in.at[side], c_send.at[side], c_recv.at[side],
            up if side == 0 else down,
        )

    def half_copy(side, k):
        device = quarter + k if side == 0 else quarter - 1 - k
        return remote(
            half_out.at[side], half_in.at[side], h_send.at[side], h_recv.at[side],
            {"sp_0": device},
        )

    def chain(hop):
        for side in range(2):

            @pl.when(place[side] == hop)
            def _():
                if hop > 0:
                    chain_copy(side).wait_recv()
                entered = chain_in[side].astype(F32)
                decay = totals[side, 128:129, :]
                state = entered[0:128, :] * decay + totals[side, 0:128, :]
                if hop < quarter - 1:
                    chain_out[side, 0:128, :] = state.astype(BF16)
                    chain_out[side, 128:144, :] = (entered[128:144, :] * decay).astype(BF16)
                    chain_copy(side).start()
                else:

                    @pl.when(z == giver[side])
                    def _():
                        half_out[side] = state.astype(BF16)
                        for k in range(quarter):
                            half_copy(side, k).start()

    row8 = lax.broadcasted_iota(jnp.int32, (8, 256), 0)

    def statistics(tops, totals_of):
        first = jnp.where(row8 == 0, tops[0], totals_of[0])
        return jnp.where(row8 < 2, first, jnp.where(row8 == 2, tops[1], totals_of[1]))

    def pack(q, m, out, stat):
        tops, sums = [], []
        for h in range(2):
            k = 2 * m + h
            tops.append(peak[q, k, 0:1, :])
            sums.append(acc[q, k, 128:129, :])
            out[h] = (acc[q, k, 0:128, :] * (1.0 / sums[h])).astype(BF16)
        stat[...] = statistics(tops, sums)

    def pack_merged(q, m, out, stat, other, others):
        tops, sums = [], []
        for h in range(2):
            k = 2 * m + h
            top_a, top_b = peak[q, k, 0:1, :], others[2 * h : 2 * h + 1, :]
            top = jnp.maximum(top_a, top_b)
            scale = jnp.exp2(top_a - top)
            share = others[2 * h + 1 : 2 * h + 2, :] * jnp.exp2(top_b - top)
            total = acc[q, k, 128:129, :] * scale + share
            inverse = 1.0 / total
            merged = acc[q, k, 0:128, :] * (scale * inverse)
            merged = merged + other[h].astype(F32) * (share * inverse)
            out[h] = merged.astype(BF16)
            tops.append(top)
            sums.append(total)
        stat[...] = statistics(tops, sums)

    def far_copies(m):
        device = beside[1] if m == 0 else beside[3]
        return [
            remote(farout.at[m], farin.at[m], f_send.at[0], f_recv.at[m, 0], device),
            remote(farouts.at[m], farins.at[m], f_send.at[1], f_recv.at[m, 1], device),
        ]

    def near_copies(w, m):
        device = beside[1] if w == 0 else beside[3]
        return [
            remote(nearout.at[w, m], nearin.at[w, m], n_send.at[0], n_recv.at[w, m, 0], device),
            remote(nearouts.at[w, m], nearins.at[w, m], n_send.at[1], n_recv.at[w, m, 1], device),
        ]

    def post(pair):
        for copy in pair:
            copy.start()

    def received(pair):
        for copy in pair:
            copy.wait_recv()

    def give_far():
        for m in range(2):
            pack(0, m, farout.at[m], farouts.at[m])
            post(far_copies(m))

    def give_near(w, m):
        def call():
            pack(w + 1, m, nearout.at[w, m], nearouts.at[w, m])
            post(near_copies(w, m))

        return call

    def merge_near(w, m):
        received(far_copies(w))
        pack_merged(w + 1, m, nearout.at[w, m], nearouts.at[w, m], farin.at[w], farins.at[w])
        post(near_copies(w, m))

    def pre(call, *args):
        return ("pre", lambda: call(*args))

    flash(
        [
            (3, pieces(0), True),
            ("pre", queries(0)), (0, pieces(0), True),
            ("pre", queries(1)), pre(forward, 1, 3), (1, pieces(0), True),
            ("pre", queries(2)), pre(forward, 2, 1), (2, pieces(0), True),
            (0, pieces(7, 1), False),
            (1, pieces(7, 1), False),
            pre(forward, 2, 2), (2, pieces(7, 1), False),
            pre(forward, 2, 3), (3, pieces(7, 1), False),
            pre(join_states), pre(forward, 3, 1), (0, pieces(6, 2), False),
            pre(forward, 3, 2), (1, pieces(6, 2), False),
            (2, pieces(6, 2), False, 0, 1),
            pre(forward, 3, 3), pre(chain, 1), (2, pieces(6, 2), False, 2, 3),
            (1, pieces(5, 3), False),
            pre(chain, 2), (0, pieces(5, 3), False),
            pre(drain, kvbuf.at[0], arrival(3, 0)), (0, pieces(4), False),
            ("post", give_far),
            (1, pieces(4), False),
            ("post", give_near(0, 1)),
            (2, pieces(5, 3, 4), False),
            ("post", give_near(1, 0)),
            pre(chain, 3), (3, pieces(6, 2), False),
            (3, pieces(5, 3, 4), False),
        ],
        kvbuf, qz, acc, peak,
    )
    merge_near(0, 0)
    merge_near(1, 1)

    for side in range(2):

        @pl.when(takes[side])
        def _():
            half_copy(side, 0).wait_recv()

    out = recout[...]
    for side in range(2):
        entered = chain_in[side].astype(F32)
        entry = entered[0:128, :] + half_in[side].astype(F32) * entered[128:129, :]
        entry = entry * inside[side, 128:129, :] + inside[side, 0:128, :]
        out = out + dot_nt(read[side], entry.astype(BF16))
    out = out * lax.rsqrt(jnp.mean(out * out, axis=1, keepdims=True) + EPS) * recgain_ref[...]
    mixrec[...] = out.astype(BF16)

    def rows_of(device):
        return pl.ds(pl.multiple_of(device * ROWS, ROWS), ROWS)

    def deal(source, got, which, devices):
        for device in devices:
            remote(
                source.at[rows_of(device), :], got.at[t], t_send.at[which], t_recv.at[which],
                {"tp": device},
            ).start()

    deal(mixrec, gotrec, 0, mates[1:])
    gotrec[t] = mixrec[rows_of(t), :]

    drain(xbuf.at[0:7], y_send)
    drain(kvbuf.at[0:7], k_send)
    drain(qbuf.at[0:3], q_send)
    drain(stbuf.at[0:3], s_send)
    drain(farout, f_send.at[0])
    drain(farouts, f_send.at[1])
    for load in late_loads:
        load.wait()
    for side in range(2):

        @pl.when(place[side] < quarter - 1)
        def _():
            chain_copy(side).wait_send()

        @pl.when(z == giver[side])
        def _():
            drain(qbuf.at[0], h_send.at[side])

    lam = lam_ref[0:1, 0:1]
    for w, m in ((0, 1), (1, 0), (0, 0), (1, 1)):
        received(near_copies(w, m))
    for h in (1, 0):
        maps = []
        for m in range(2):
            k = 2 * m + h
            tops = [peak[3, k, 0:1, :]] + [nearins[w, m, 2 * h : 2 * h + 1, :] for w in range(2)]
            sums = [acc[3, k, 128:129, :]] + [nearins[w, m, 2 * h + 1 : 2 * h + 2, :] for w in range(2)]
            top = jnp.maximum(jnp.maximum(tops[0], tops[1]), tops[2])
            shares = [a * jnp.exp2(b - top) for a, b in zip(sums, tops)]
            inverse = 1.0 / (shares[0] + shares[1] + shares[2])
            value = acc[3, k, 0:128, :] * (jnp.exp2(tops[0] - top) * inverse)
            for w in range(2):
                value = value + nearin[w, m, h].astype(F32) * (shares[w + 1] * inverse)
            maps.append(value)
        mixed = maps[0] - lam * maps[1]
        mixed = mixed * lax.rsqrt(jnp.mean(mixed * mixed, axis=0, keepdims=True) + EPS)
        rows = (mixed.T * attgain_ref[...]).astype(BF16)
        for half_of, yy in zip(range(2), ((y, left // 2), (right // 2, far // 2))[h]):
            at = pl.ds(pl.multiple_of(yy * 128, 128), 128)
            mixatt[at, :] = rows[128 * half_of : 128 * (half_of + 1), :]
        deal(mixatt, gotatt, 1, ((left, mate_l, partner), (far, mate_far, right, mate_r))[h])
    gotatt[t] = mixatt[rows_of(t), :]
    drain(nearout, n_send.at[0])
    drain(nearouts, n_send.at[1])
    drain(gotrec.at[0:7], t_recv.at[0])
    rec_term = dot(jnp.concatenate([gotrec[k] for k in range(8)], axis=1), wr[...])
    drain(gotatt.at[0:7], t_recv.at[1])
    att_term = dot(jnp.concatenate([gotatt[k] for k in range(8)], axis=1), wa[...])
    out_ref[...] = (rec_term + att_term).astype(BF16)
    drain(gotrec.at[0:7], t_send.at[0])
    drain(gotatt.at[0:7], t_send.at[1])


def on_device(
    tokens, norm_gain, rec_query, fwd_gate, bwd_gate, rec_value, gate_leak, log_decay, rec_gain,
    att_query, att_key, att_value, lambdas, att_gain, out_rec, out_att,
):
    weights = (rec_query, fwd_gate, bwd_gate, rec_value, att_query, att_key, att_value)
    dma = pltpu.SemaphoreType.DMA
    return pl.pallas_call(
        layer_kernel,
        out_shape=jax.ShapeDtypeStruct((ROWS, D), BF16),
        in_specs=[VMEM_SPEC] + [ANY_SPEC] * 16,
        out_specs=VMEM_SPEC,
        scratch_shapes=[
            pltpu.VMEM((1, D), F32),
            pltpu.VMEM((2 * LEN + 2 * NZ * NX, 128), F32),
            pltpu.VMEM((2, 128), F32),
            pltpu.VMEM((8, 128), F32),
            pltpu.VMEM((1, 128), F32),
            pltpu.VMEM((1, 128), F32),
            pltpu.VMEM((8, ROWS, D), BF16),
            pltpu.VMEM((D, NCOL), BF16),
            pltpu.VMEM((LEN, 512), BF16),
            pltpu.VMEM((LEN, 128), F32),
            pltpu.VMEM((2, LEN, 128), BF16),
            pltpu.VMEM((NZ, 4, 256, 128), BF16),
            pltpu.VMEM((4, 128, 128), BF16),
            pltpu.VMEM((NX, 4, 128, 128), BF16),
            pltpu.VMEM((NX, 4, 128, 256), BF16),
            pltpu.VMEM((NX, 4, 144, 256), F32),
            pltpu.VMEM((NX, 4, 8, 256), F32),
            pltpu.VMEM((2, 2, 128, 256), BF16),
            pltpu.VMEM((2, 2, 128, 256), BF16),
            pltpu.VMEM((2, 8, 256), F32),
            pltpu.VMEM((2, 8, 256), F32),
            pltpu.VMEM((2, 2, 2, 128, 256), BF16),
            pltpu.VMEM((2, 2, 2, 128, 256), BF16),
            pltpu.VMEM((2, 2, 8, 256), F32),
            pltpu.VMEM((2, 2, 8, 256), F32),
            pltpu.VMEM((NX, 2, 144, 128), BF16),
            pltpu.VMEM((2, 136, 128), F32),
            pltpu.VMEM((2, 136, 128), F32),
            pltpu.VMEM((2, 144, 128), BF16),
            pltpu.VMEM((2, 144, 128), BF16),
            pltpu.VMEM((2, 128, 128), BF16),
            pltpu.VMEM((2, 128, 128), BF16),
            pltpu.VMEM((LEN, 128), BF16),
            pltpu.VMEM((LEN, 128), BF16),
            pltpu.VMEM((8, ROWS, 128), BF16),
            pltpu.VMEM((8, ROWS, 128), BF16),
            pltpu.VMEM((1024, D), BF16),
            pltpu.VMEM((1024, D), BF16),
            dma((10,)), dma, dma((14,)), dma, dma((13,)), dma, dma((NX,)), dma, dma,
            dma((2,)), dma((2,)), dma((2,)), dma((2,)),
            dma((2,)), dma((2, 2)), dma((2,)), dma((2, 2, 2)), dma((2,)), dma((2,)),
        ],
        compiler_params=pltpu.CompilerParams(
            collective_id=0, has_side_effects=True, vmem_limit_bytes=VMEM_LIMIT,
        ),
        name="layer",
    )(
        lambdas.reshape(1, 1), tokens, norm_gain.reshape(1, D), rotary_tables(), gate_leak,
        log_decay.reshape(8, 128), att_gain.reshape(1, 128), rec_gain.reshape(1, 128), *weights,
        out_rec, out_att,
    )


def solution(mesh):
    torus = Mesh(mesh.devices.reshape(NZ, NX, mesh.shape["tp"]), SP_TP)
    tp = P(None, "tp")
    in_specs = (
        P(SP_TP, None), P(), tp, tp, tp, tp, tp, P(None, SP, "tp"), P(), tp, tp, tp, P("tp"), P(),
        P(), P(),
    )
    return jax.shard_map(
        on_device, mesh=torus, in_specs=in_specs, out_specs=P(SP_TP, None), check_vma=False
    )
```

```python
import math

import jax
import jax.numpy as jnp
import numpy as np
from jax import lax
from jax.experimental import pallas as pl
from jax.experimental.pallas import tpu as pltpu
from jax.sharding import Mesh
from jax.sharding import PartitionSpec as P

HK = 128
AK = 64
BLOCK = 64
SP = ("sp_0", "sp_1")
SP_TP = ("sp_0", "sp_1", "tp")
NZ, NX, NY = 8, 4, 4
ROWS = 64
LEN = 512
D = 2048
NCOL = 896
EPS = 1e-06
THETA = 500000.0
LOG2E = 1.4426950408889634
F32 = jnp.float32
BF16 = jnp.bfloat16
MESH = pl.DeviceIdType.MESH
VMEM_SPEC = pl.BlockSpec(memory_space=pltpu.VMEM)
ANY_SPEC = pl.BlockSpec(memory_space=pl.ANY)
VMEM_LIMIT = 60 * 1024 * 1024


def remote(src, dst, send_sem, recv_sem, device):
    return pltpu.make_async_remote_copy(
        src_ref=src,
        dst_ref=dst,
        send_sem=send_sem,
        recv_sem=recv_sem,
        device_id=device,
        device_id_type=MESH,
    )


def meet(devices):
    barrier = pltpu.get_barrier_semaphore()
    for device in devices:
        pl.semaphore_signal(barrier, inc=1, device_id=device, device_id_type=MESH)
    pl.semaphore_wait(barrier, len(devices))


def dot(a, b):
    return jnp.dot(a, b, preferred_element_type=F32)


def dot_nt(a, b):
    return lax.dot_general(a, b, (((1,), (1,)), ((), ())), preferred_element_type=F32)


def rotary_tables():
    i = np.arange(AK // 2, dtype=np.float64)
    freq = THETA ** (-(i * 2.0 / AK))
    freq = np.tile(freq, 4)[None, :]
    within = np.arange(LEN, dtype=np.float64)[:, None] * freq
    starts = np.arange(NZ * NX, dtype=np.float64)[:, None] * LEN * freq
    tables = [f(v) for v in (within, starts) for f in (np.cos, np.sin)]
    return jnp.asarray(np.concatenate(tables, axis=0).astype(np.float32))


def exact_cumulative(triangle, logs):
    first = logs.astype(BF16)
    rest = logs - first.astype(F32)
    second = rest.astype(BF16)
    third = (rest - second.astype(F32)).astype(BF16)
    return dot(triangle, first) + dot(triangle, second) + dot(triangle, third)


def recurrence(rec_ref, leak_ref, decay_ref, out_ref, read_ref, state_ref, done):
    blocks = LEN // BLOCK
    raw_q = rec_ref[:, 0:128].astype(F32)
    rq = raw_q / (1.0 + jnp.exp(-raw_q))
    value = rec_ref[:, 384:512]
    value_t = value.astype(F32).T.astype(BF16)
    row = lax.broadcasted_iota(jnp.int32, (256, 256), 0)
    col = lax.broadcasted_iota(jnp.int32, (256, 256), 1)
    same = (row // BLOCK) == (col // BLOCK)
    upper = lax.broadcasted_iota(jnp.int32, (128, 1), 0) < BLOCK
    total_out = None
    for side in range(2):
        raw = rec_ref[:, 128 * (side + 1) : 128 * (side + 2)].astype(F32)
        key = leak_ref[side : side + 1, :] / (1.0 + jnp.exp(raw))
        added_log = jnp.concatenate(
            [
                jnp.broadcast_to(decay_ref[4 * side + k : 4 * side + k + 1, :], (128, 128)).T
                for k in range(4)
            ],
            axis=0,
        )
        logs = jnp.log1p(-key) + added_log
        mask = same & ((row >= col) if side == 0 else (row <= col))
        triangle = mask.astype(F32).astype(BF16)
        cum = jnp.concatenate(
            [exact_cumulative(triangle, logs[256 * h : 256 * (h + 1)]) for h in range(2)], axis=0
        )
        cum3 = cum.reshape(blocks, BLOCK, 128)
        at_mid, at_last = (BLOCK // 2 - 1, BLOCK - 1) if side == 0 else (BLOCK // 2, 0)
        middle = cum3[:, at_mid : at_mid + 1, :]
        last = cum3[:, at_last : at_last + 1, :]
        key3, rq3 = key.reshape(cum3.shape), rq.reshape(cum3.shape)
        qs = (rq3 * jnp.exp(cum3 - middle)).reshape(LEN, 128).astype(BF16)
        ks = (key3 * jnp.exp(middle - cum3)).reshape(LEN, 128).astype(BF16)
        kl = (key3 * jnp.exp(last - cum3)).reshape(LEN, 128)
        qc = (rq3 * jnp.exp(cum3)).reshape(LEN, 128).astype(BF16)
        within = []
        for h in range(2):
            part = slice(256 * h, 256 * (h + 1))
            scores = jnp.where(mask, dot_nt(qs[part], ks[part]), 0.0).astype(BF16)
            within.append(dot(scores, value[part]))
        order = range(blocks) if side == 0 else reversed(range(blocks))
        state = jnp.zeros((128, 128), F32)
        carried, before = [None] * blocks, [None] * blocks
        running = jnp.zeros((1, 128), F32)
        for b in order:
            carried[b] = dot_nt(qc[BLOCK * b : BLOCK * (b + 1)], state.astype(BF16))
            pair = b // 2
            keys = kl[128 * pair : 128 * (pair + 1)]
            keys = jnp.where(upper if b % 2 == 0 else ~upper, keys, 0.0).astype(BF16)
            added = dot(value_t[:, 128 * pair : 128 * (pair + 1)], keys)
            before[b] = running
            running = running + last[b]
            state = state * jnp.exp(last[b]) + added
        out = jnp.concatenate(within, axis=0) + jnp.concatenate(carried, axis=0)
        total_out = out if total_out is None else total_out + out
        reach = (cum3 + jnp.stack(before, axis=0)).reshape(LEN, 128)
        read_ref[side] = (rq * jnp.exp(reach)).astype(BF16)
        state_ref[side, 0:128, :] = state.astype(BF16)
        state_ref[side, 128:144, :] = jnp.broadcast_to(jnp.exp(running), (16, 128)).astype(BF16)
        done(side)
    out_ref[...] = total_out


def flash(plan, kvbuf, qz, acc, peak):
    ones = jnp.ones((16, 256), BF16)
    tiles, ahead, behind = [], {}, {}
    for item in plan:
        if item[0] == "pre":
            ahead.setdefault(len(tiles), []).append(item[1])
        elif item[0] == "post":
            behind.setdefault(len(tiles) - 1, []).append(item[1])
        else:
            tiles += [(item[0], k, item[1], item[2]) for k in (item[3:] or range(4))]
    count = len(tiles)
    tops, olds, sums = [None] * count, [None] * count, [None] * count
    scores, weights = [{} for _ in tiles], [{} for _ in tiles]

    def has(i, n):
        return 0 <= i < count and n < len(tiles[i][2])

    def score(i, n):
        q, k, pieces, first = tiles[i]
        if n == 0 and not first:
            before = [b for b in range(max(0, i - 2), i) if tiles[b][:2] == (q, k)]
            olds[i] = tops[i] = tops[before[-1]] if before else peak[q, k, 0:1, :]
        r, s = pieces[n]
        keys = jnp.concatenate([kvbuf[r, 2 * s, 0:128, :], kvbuf[r, 2 * s + 1, 0:128, :]], axis=0)
        scores[i][n] = dot(keys, qz[q, k])
        here = jnp.max(scores[i][n], axis=0, keepdims=True)
        tops[i] = here if tops[i] is None else jnp.maximum(tops[i], here)

    def weigh(i, n):
        weights[i][n] = jnp.exp2(scores[i].pop(n) - tops[i]).astype(BF16)

    def gather(i, n):
        q, k, pieces, first = tiles[i]
        r, s = pieces[n]
        values = [kvbuf[r, 2 * s, 128:256, :], kvbuf[r, 2 * s + 1, 128:256, :]]
        values = jnp.concatenate(values, axis=1)
        term = dot(jnp.concatenate([values, ones], axis=0), weights[i].pop(n))
        sums[i] = term if sums[i] is None else sums[i] + term
        if n == len(pieces) - 1:
            if first:
                acc[q, k] = sums[i]
            else:
                acc[q, k] = acc[q, k] * jnp.exp2(olds[i] - tops[i]) + sums[i]
            peak[q, k] = jnp.broadcast_to(tops[i], (8, 256))

    longest = max(len(t[2]) for t in tiles)
    for i in range(-2, count):
        for call in ahead.get(i + 2, []):
            call()
        for n in range(longest):
            for stage, at in ((score, i + 2), (weigh, i + 1), (gather, i)):
                if has(at, n):
                    stage(at, n)
        for call in behind.get(i, []):
            call()


REACH = (2, 1, 3, 0)


def layer_kernel(
    lam_ref, tok_ref, *refs,
):
    small, weights, (wrec_ref, watt_ref, out_ref) = refs[:6], refs[6:13], refs[13:16]
    (
        gain_ref, tables, leak_ref, decay_ref, attgain_ref, recgain_ref,
        xbuf, wbuf, recraw, recout, read,
        kvbuf, qown, qbuf, qz, acc, peak, farout, farin, farouts, farins, nearout, nearin,
        nearouts, nearins, stbuf, totals, inside, chain_in, chain_out, half_in, half_out,
        mixrec, mixatt, gotrec, gotatt, wr, wa,
        wsem, y_send, y_recv, k_send, k_recv, q_send, q_recv, s_send, s_recv,
        c_send, c_recv, h_send, h_recv, f_send, f_recv, n_send, n_recv,
        t_send, t_recv,
    ) = refs[16:]
    z, x, t = lax.axis_index("sp_0"), lax.axis_index("sp_1"), lax.axis_index("tp")
    y, c = t // 2, t % 2
    right = lax.rem(y + 1, NY) * 2 + c
    left = lax.rem(y + NY - 1, NY) * 2 + c
    far = lax.rem(y + 2, NY) * 2 + c
    partner = 2 * y + 1 - c
    up = {"sp_0": lax.rem(z + 1, NZ)}
    down = {"sp_0": lax.rem(z + NZ - 1, NZ)}
    beside = [None] + [{"sp_1": lax.rem(x + p, NX)} for p in range(1, NX)]
    mates = [None] + [lax.rem(t + d, 8) for d in range(1, 8)]

    own_load = pltpu.make_async_copy(tok_ref, xbuf.at[t], wsem.at[0])
    own_load.start()
    loads = [
        pltpu.make_async_copy(w, wbuf.at[:, pl.ds(128 * k, 128)], wsem.at[1])
        for k, w in enumerate(weights)
    ]
    homes = (gain_ref, tables, leak_ref, decay_ref, attgain_ref, recgain_ref)
    small_loads = [
        pltpu.make_async_copy(a, b, wsem.at[4 + k]) for k, (a, b) in enumerate(zip(small, homes))
    ]
    late_loads = [
        pltpu.make_async_copy(wrec_ref, wr, wsem.at[2]),
        pltpu.make_async_copy(watt_ref, wa, wsem.at[3]),
    ]
    for load in loads + small_loads:
        load.start()
    meet([up, down] + beside[1:] + [{"tp": m} for m in mates[1:]])

    def drain(ref, sem):
        pltpu.make_async_copy(ref, ref, sem).wait()

    own_load.wait()

    quarter_rows = ROWS // 4

    def rows_at(slot, first, count):
        return xbuf.at[slot, pl.ds(first * quarter_rows, count * quarter_rows)]

    def launch(slot, first, count, number, device):
        here = rows_at(slot, first, count)
        remote(here, here, y_send, y_recv.at[number], {"tp": device}).start()

    def arrived(slot, first, count, number):
        drain(rows_at(slot, first, count), y_recv.at[number])

    launch(t, 0, 1, 0, right)
    launch(t, 3, 1, 3, left)
    launch(t, 1, 1, 1, right)
    launch(t, 2, 1, 4, left)
    launch(t, 2, 2, 2, right)
    launch(t, 0, 2, 5, left)
    launch(t, 0, 4, 8, partner)
    for load in small_loads:
        load.wait()
    drain(wbuf, wsem.at[1])

    block = z * NX + x
    cb = tables[pl.ds(2 * LEN + block, 1), :]
    sb = tables[pl.ds(2 * LEN + NZ * NX + block, 1), :]
    lane = lax.broadcasted_iota(jnp.int32, (1, 128), 1)
    low = lax.rem(lane, 64) < 32

    def turned(v, cosine, sine):
        other = jnp.where(low, pltpu.roll(v, 96, 1), pltpu.roll(v, 32, 1))
        return v * cosine + other * sine

    def arrival(step, j):
        return k_recv.at[4 * step + j if step < 3 else 12]

    def start_right(step, j):
        src = kvbuf.at[(NZ - step) % NZ, j]
        remote(src, kvbuf.at[NZ - 1 - step, j], k_send, arrival(step, j), up).start()

    def start_left(step, j):
        src = kvbuf.at[step, j]
        remote(src, kvbuf.at[step + 1, j], k_send, arrival(step, j), down).start()

    def forward(step, j):
        drain(kvbuf.at[0, 0:2], arrival(step - 1, j))
        if step < 3 or j < 2:
            start_right(step, j)
        if step < 3 or j >= 2:
            start_left(step, j)

    def process(yy, j):
        pair = xbuf[pl.ds(2 * yy, 2)].reshape(2 * ROWS, D).astype(F32)
        scale = lax.rsqrt(jnp.mean(pair * pair, axis=1, keepdims=True) + EPS)
        normed = (pair * scale * gain_ref[...]).astype(BF16)
        out = dot(normed, wbuf[...])
        rows = pl.ds(pl.multiple_of(yy * 128, 128), 128)
        ca = tables[rows, :]
        sa = tables[pl.ds(pl.multiple_of(LEN + yy * 128, 128), 128), :]
        cosine = ca * cb - sa * sb
        sine = sa * cb + ca * sb
        signed = jnp.where(low, -sine, sine)
        raw = out[:, 512:].astype(BF16).astype(F32)
        kvbuf[0, j, 0:128, :] = turned(raw[:, 128:256], cosine, signed).astype(BF16)
        kvbuf[0, j, 128:256, :] = raw[:, 256:384].T.astype(BF16)
        query = turned(raw[:, 0:128], cosine, signed) * (AK**-0.5 * LOG2E)
        qown[j] = query.T.astype(BF16)
        recraw[rows, :] = out[:, :512].astype(BF16)
        start_right(0, j)
        start_left(0, j)
        for p in (2, 1, 3):
            remote(
                qown.at[j], qbuf.at[NX - p, j], q_send, q_recv.at[NX - p], beside[p]
            ).start()

    arrived(partner, 0, 4, 8)
    process(y, 0)
    arrived(left, 0, 1, 0)
    launch(left, 0, 1, 6, right)
    arrived(right, 3, 1, 3)
    launch(right, 3, 1, 7, left)
    arrived(left, 1, 1, 1)
    launch(left, 1, 1, 6, right)
    launch(left, 0, 2, 9, partner)
    arrived(right, 2, 1, 4)
    launch(right, 2, 1, 7, left)
    launch(right, 2, 2, 11, partner)
    forward(1, 0)
    arrived(left, 2, 2, 2)
    launch(left, 2, 2, 10, partner)
    arrived(right, 0, 2, 5)
    launch(right, 0, 2, 12, partner)
    mate_l, mate_r, mate_far = left + 1 - 2 * c, right + 1 - 2 * c, far + 1 - 2 * c
    arrived(mate_l, 0, 2, 9)
    arrived(mate_l, 2, 2, 10)
    process(left // 2, 1)
    arrived(mate_r, 2, 2, 11)
    arrived(mate_r, 0, 2, 12)
    process(right // 2, 2)
    forward(2, 0)
    arrived(far, 0, 2, 6)
    launch(far, 0, 2, 13, partner)
    arrived(far, 2, 2, 7)
    launch(far, 2, 2, 14, partner)
    arrived(mate_far, 0, 2, 13)
    arrived(mate_far, 2, 2, 14)
    process(far // 2, 3)
    for load in late_loads:
        load.start()
    forward(1, 1)

    def one_side(side):
        for p in range(1, NX):
            remote(
                stbuf.at[0, side], stbuf.at[NX - p, side], s_send, s_recv, beside[p]
            ).start()
        if side == 0:
            forward(1, 2)

    recurrence(recraw, leak_ref, decay_ref, recout, read, stbuf.at[0], one_side)

    upper = lax.broadcasted_iota(jnp.int32, (128, 1), 0) < AK

    def spread(q, source):
        for h in range(2):
            piece = jnp.concatenate([source(2 * h), source(2 * h + 1)], axis=1).astype(F32)
            qz[q, h] = jnp.where(upper, piece, 0.0).astype(BF16)
            qz[q, 2 + h] = jnp.where(upper, 0.0, piece).astype(BF16)

    def pieces(*slots):
        return [(r, s) for r in slots for s in range(2)]

    spread(3, lambda j: qown[j])

    def queries(q):
        def call():
            p = REACH[q]
            drain(qbuf.at[p], q_recv.at[p])
            spread(q, lambda j: qbuf[p, j])

        return call

    def join_states():
        drain(stbuf.at[1:4], s_recv)
        for side in range(2):
            order = range(NX) if side == 0 else reversed(range(NX))
            total_s, total_d = jnp.zeros((128, 128), F32), jnp.ones((1, 128), F32)
            inside_s, inside_d = total_s, total_d
            for k in order:
                rel = lax.rem(k - x + NX, NX)
                piece_s = stbuf[rel, side, 0:128, :].astype(F32)
                piece_d = stbuf[rel, side, 128:144, :].astype(F32)[0:1, :]
                total_s = total_s * piece_d + piece_s
                total_d = total_d * piece_d
                passed = (k < x) if side == 0 else (k > x)
                inside_s = jnp.where(passed, total_s, inside_s)
                inside_d = jnp.where(passed, total_d, inside_d)
            totals[side, 0:128, :] = total_s
            totals[side, 128:136, :] = jnp.broadcast_to(total_d, (8, 128))
            inside[side, 0:128, :] = inside_s
            inside[side, 128:136, :] = jnp.broadcast_to(inside_d, (8, 128))
        chain(0)

    quarter = NZ // 2
    place = (lax.rem(z, quarter), quarter - 1 - lax.rem(z, quarter))
    giver = (quarter - 1, quarter)
    takes = (z >= quarter, z < quarter)

    for side in range(2):

        @pl.when(place[side] == 0)
        def _():
            chain_in[side, 0:128, :] = jnp.zeros((128, 128), BF16)
            chain_in[side, 128:144, :] = jnp.ones((16, 128), BF16)

        @pl.when(jnp.logical_not(takes[side]))
        def _():
            half_in[side] = jnp.zeros((128, 128), BF16)

    def chain_copy(side):
        return remote(
            chain_out.at[side], chain_in.at[side], c_send.at[side], c_recv.at[side],
            up if side == 0 else down,
        )

    def half_copy(side, k):
        device = quarter + k if side == 0 else quarter - 1 - k
        return remote(
            half_out.at[side], half_in.at[side], h_send.at[side], h_recv.at[side],
            {"sp_0": device},
        )

    def chain(hop):
        for side in range(2):

            @pl.when(place[side] == hop)
            def _():
                if hop > 0:
                    chain_copy(side).wait_recv()
                entered = chain_in[side].astype(F32)
                decay = totals[side, 128:129, :]
                state = entered[0:128, :] * decay + totals[side, 0:128, :]
                if hop < quarter - 1:
                    chain_out[side, 0:128, :] = state.astype(BF16)
                    chain_out[side, 128:144, :] = (entered[128:144, :] * decay).astype(BF16)
                    chain_copy(side).start()
                else:

                    @pl.when(z == giver[side])
                    def _():
                        half_out[side] = state.astype(BF16)
                        for k in range(quarter):
                            half_copy(side, k).start()

    row8 = lax.broadcasted_iota(jnp.int32, (8, 256), 0)

    def statistics(tops, totals_of):
        first = jnp.where(row8 == 0, tops[0], totals_of[0])
        return jnp.where(row8 < 2, first, jnp.where(row8 == 2, tops[1], totals_of[1]))

    def pack(q, m, out, stat):
        tops, sums = [], []
        for h in range(2):
            k = 2 * m + h
            tops.append(peak[q, k, 0:1, :])
            sums.append(acc[q, k, 128:129, :])
            out[h] = (acc[q, k, 0:128, :] * (1.0 / sums[h])).astype(BF16)
        stat[...] = statistics(tops, sums)

    def pack_merged(q, m, out, stat, other, others):
        tops, sums = [], []
        for h in range(2):
            k = 2 * m + h
            top_a, top_b = peak[q, k, 0:1, :], others[2 * h : 2 * h + 1, :]
            top = jnp.maximum(top_a, top_b)
            scale = jnp.exp2(top_a - top)
            share = others[2 * h + 1 : 2 * h + 2, :] * jnp.exp2(top_b - top)
            total = acc[q, k, 128:129, :] * scale + share
            inverse = 1.0 / total
            merged = acc[q, k, 0:128, :] * (scale * inverse)
            merged = merged + other[h].astype(F32) * (share * inverse)
            out[h] = merged.astype(BF16)
            tops.append(top)
            sums.append(total)
        stat[...] = statistics(tops, sums)

    def far_copies(m):
        device = beside[1] if m == 0 else beside[3]
        return [
            remote(farout.at[m], farin.at[m], f_send.at[0], f_recv.at[m, 0], device),
            remote(farouts.at[m], farins.at[m], f_send.at[1], f_recv.at[m, 1], device),
        ]

    def near_copies(w, m):
        device = beside[1] if w == 0 else beside[3]
        return [
            remote(nearout.at[w, m], nearin.at[w, m], n_send.at[0], n_recv.at[w, m, 0], device),
            remote(nearouts.at[w, m], nearins.at[w, m], n_send.at[1], n_recv.at[w, m, 1], device),
        ]

    def post(pair):
        for copy in pair:
            copy.start()

    def received(pair):
        for copy in pair:
            copy.wait_recv()

    def give_far():
        for m in range(2):
            pack(0, m, farout.at[m], farouts.at[m])
            post(far_copies(m))

    def give_near(w, m):
        def call():
            pack(w + 1, m, nearout.at[w, m], nearouts.at[w, m])
            post(near_copies(w, m))

        return call

    def merge_near(w, m):
        received(far_copies(w))
        pack_merged(w + 1, m, nearout.at[w, m], nearouts.at[w, m], farin.at[w], farins.at[w])
        post(near_copies(w, m))

    def pre(call, *args):
        return ("pre", lambda: call(*args))

    flash(
        [
            (3, pieces(0), True),
            ("pre", queries(0)), (0, pieces(0), True),
            ("pre", queries(1)), pre(forward, 1, 3), pre(forward, 3, 0), (1, pieces(0), True),
            ("pre", queries(2)), pre(forward, 2, 1), (2, pieces(0), True),
            (0, pieces(7, 1), False),
            (1, pieces(7, 1), False),
            pre(forward, 2, 2), (2, pieces(7, 1), False),
            pre(forward, 2, 3), pre(join_states), (0, pieces(6, 2), False),
            pre(forward, 3, 1), pre(forward, 3, 2), (1, pieces(6, 2), False),
            (2, pieces(6, 2), False, 0, 1),
            pre(forward, 3, 3), pre(chain, 1), (2, pieces(6, 2), False, 2, 3),
            (1, pieces(5, 3), False),
            pre(chain, 2), (0, pieces(5, 3), False),
            pre(drain, kvbuf.at[0], arrival(3, 0)), (0, pieces(4), False),
            ("post", give_far),
            (1, pieces(4), False),
            ("post", give_near(0, 1)),
            (2, pieces(5, 3, 4), False),
            ("post", give_near(1, 0)),
            (3, pieces(7, 1), False),
            pre(chain, 3), (3, pieces(6, 2), False),
            (3, pieces(5, 3, 4), False),
        ],
        kvbuf, qz, acc, peak,
    )
    merge_near(0, 0)
    merge_near(1, 1)

    for side in range(2):

        @pl.when(takes[side])
        def _():
            half_copy(side, 0).wait_recv()

    out = recout[...]
    for side in range(2):
        entered = chain_in[side].astype(F32)
        entry = entered[0:128, :] + half_in[side].astype(F32) * entered[128:129, :]
        entry = entry * inside[side, 128:129, :] + inside[side, 0:128, :]
        out = out + dot_nt(read[side], entry.astype(BF16))
    out = out * lax.rsqrt(jnp.mean(out * out, axis=1, keepdims=True) + EPS) * recgain_ref[...]
    mixrec[...] = out.astype(BF16)

    def rows_of(device):
        return pl.ds(pl.multiple_of(device * ROWS, ROWS), ROWS)

    def deal(source, got, which, devices):
        for device in devices:
            remote(
                source.at[rows_of(device), :], got.at[t], t_send.at[which], t_recv.at[which],
                {"tp": device},
            ).start()

    deal(mixrec, gotrec, 0, mates[1:])
    gotrec[t] = mixrec[rows_of(t), :]

    drain(xbuf.at[0:7], y_send)
    drain(kvbuf.at[0:7], k_send)
    drain(qbuf.at[0:3], q_send)
    drain(stbuf.at[0:3], s_send)
    drain(farout, f_send.at[0])
    drain(farouts, f_send.at[1])
    for load in late_loads:
        load.wait()
    for side in range(2):

        @pl.when(place[side] < quarter - 1)
        def _():
            chain_copy(side).wait_send()

        @pl.when(z == giver[side])
        def _():
            drain(qbuf.at[0], h_send.at[side])

    lam = lam_ref[0:1, 0:1]
    for w, m in ((0, 1), (1, 0), (0, 0), (1, 1)):
        received(near_copies(w, m))
    for h in (1, 0):
        maps = []
        for m in range(2):
            k = 2 * m + h
            tops = [peak[3, k, 0:1, :]] + [nearins[w, m, 2 * h : 2 * h + 1, :] for w in range(2)]
            sums = [acc[3, k, 128:129, :]] + [nearins[w, m, 2 * h + 1 : 2 * h + 2, :] for w in range(2)]
            top = jnp.maximum(jnp.maximum(tops[0], tops[1]), tops[2])
            shares = [a * jnp.exp2(b - top) for a, b in zip(sums, tops)]
            inverse = 1.0 / (shares[0] + shares[1] + shares[2])
            value = acc[3, k, 0:128, :] * (jnp.exp2(tops[0] - top) * inverse)
            for w in range(2):
                value = value + nearin[w, m, h].astype(F32) * (shares[w + 1] * inverse)
            maps.append(value)
        mixed = maps[0] - lam * maps[1]
        mixed = mixed * lax.rsqrt(jnp.mean(mixed * mixed, axis=0, keepdims=True) + EPS)
        rows = (mixed.T * attgain_ref[...]).astype(BF16)
        for half_of, yy in zip(range(2), ((y, left // 2), (right // 2, far // 2))[h]):
            at = pl.ds(pl.multiple_of(yy * 128, 128), 128)
            mixatt[at, :] = rows[128 * half_of : 128 * (half_of + 1), :]
        deal(mixatt, gotatt, 1, ((left, mate_l, partner), (far, mate_far, right, mate_r))[h])
    gotatt[t] = mixatt[rows_of(t), :]
    drain(nearout, n_send.at[0])
    drain(nearouts, n_send.at[1])
    drain(gotrec.at[0:7], t_recv.at[0])
    rec_term = dot(jnp.concatenate([gotrec[k] for k in range(8)], axis=1), wr[...])
    drain(gotatt.at[0:7], t_recv.at[1])
    att_term = dot(jnp.concatenate([gotatt[k] for k in range(8)], axis=1), wa[...])
    out_ref[...] = (rec_term + att_term).astype(BF16)
    drain(gotrec.at[0:7], t_send.at[0])
    drain(gotatt.at[0:7], t_send.at[1])


def on_device(
    tokens, norm_gain, rec_query, fwd_gate, bwd_gate, rec_value, gate_leak, log_decay, rec_gain,
    att_query, att_key, att_value, lambdas, att_gain, out_rec, out_att,
):
    weights = (rec_query, fwd_gate, bwd_gate, rec_value, att_query, att_key, att_value)
    dma = pltpu.SemaphoreType.DMA
    return pl.pallas_call(
        layer_kernel,
        out_shape=jax.ShapeDtypeStruct((ROWS, D), BF16),
        in_specs=[VMEM_SPEC] + [ANY_SPEC] * 16,
        out_specs=VMEM_SPEC,
        scratch_shapes=[
            pltpu.VMEM((1, D), F32),
            pltpu.VMEM((2 * LEN + 2 * NZ * NX, 128), F32),
            pltpu.VMEM((2, 128), F32),
            pltpu.VMEM((8, 128), F32),
            pltpu.VMEM((1, 128), F32),
            pltpu.VMEM((1, 128), F32),
            pltpu.VMEM((8, ROWS, D), BF16),
            pltpu.VMEM((D, NCOL), BF16),
            pltpu.VMEM((LEN, 512), BF16),
            pltpu.VMEM((LEN, 128), F32),
            pltpu.VMEM((2, LEN, 128), BF16),
            pltpu.VMEM((NZ, 4, 256, 128), BF16),
            pltpu.VMEM((4, 128, 128), BF16),
            pltpu.VMEM((NX, 4, 128, 128), BF16),
            pltpu.VMEM((NX, 4, 128, 256), BF16),
            pltpu.VMEM((NX, 4, 144, 256), F32),
            pltpu.VMEM((NX, 4, 8, 256), F32),
            pltpu.VMEM((2, 2, 128, 256), BF16),
            pltpu.VMEM((2, 2, 128, 256), BF16),
            pltpu.VMEM((2, 8, 256), F32),
            pltpu.VMEM((2, 8, 256), F32),
            pltpu.VMEM((2, 2, 2, 128, 256), BF16),
            pltpu.VMEM((2, 2, 2, 128, 256), BF16),
            pltpu.VMEM((2, 2, 8, 256), F32),
            pltpu.VMEM((2, 2, 8, 256), F32),
            pltpu.VMEM((NX, 2, 144, 128), BF16),
            pltpu.VMEM((2, 136, 128), F32),
            pltpu.VMEM((2, 136, 128), F32),
            pltpu.VMEM((2, 144, 128), BF16),
            pltpu.VMEM((2, 144, 128), BF16),
            pltpu.VMEM((2, 128, 128), BF16),
            pltpu.VMEM((2, 128, 128), BF16),
            pltpu.VMEM((LEN, 128), BF16),
            pltpu.VMEM((LEN, 128), BF16),
            pltpu.VMEM((8, ROWS, 128), BF16),
            pltpu.VMEM((8, ROWS, 128), BF16),
            pltpu.VMEM((1024, D), BF16),
            pltpu.VMEM((1024, D), BF16),
            dma((10,)), dma, dma((15,)), dma, dma((13,)), dma, dma((NX,)), dma, dma,
            dma((2,)), dma((2,)), dma((2,)), dma((2,)),
            dma((2,)), dma((2, 2)), dma((2,)), dma((2, 2, 2)), dma((2,)), dma((2,)),
        ],
        compiler_params=pltpu.CompilerParams(
            collective_id=0, has_side_effects=True, vmem_limit_bytes=VMEM_LIMIT,
        ),
        name="layer",
    )(
        lambdas.reshape(1, 1), tokens, norm_gain.reshape(1, D), rotary_tables(), gate_leak,
        log_decay.reshape(8, 128), att_gain.reshape(1, 128), rec_gain.reshape(1, 128), *weights,
        out_rec, out_att,
    )


def solution(mesh):
    torus = Mesh(mesh.devices.reshape(NZ, NX, mesh.shape["tp"]), SP_TP)
    tp = P(None, "tp")
    in_specs = (
        P(SP_TP, None), P(), tp, tp, tp, tp, tp, P(None, SP, "tp"), P(), tp, tp, tp, P("tp"), P(),
        P(), P(),
    )
    return jax.shard_map(
        on_device, mesh=torus, in_specs=in_specs, out_specs=P(SP_TP, None), check_vma=False
    )
```

```python
import math

import jax
import jax.numpy as jnp
import numpy as np
from jax import lax
from jax.experimental import pallas as pl
from jax.experimental.pallas import tpu as pltpu
from jax.sharding import Mesh
from jax.sharding import PartitionSpec as P

HK = 128
AK = 64
BLOCK = 64
SP = ("sp_0", "sp_1")
SP_TP = ("sp_0", "sp_1", "tp")
NZ, NX, NY = 8, 4, 4
ROWS = 64
LEN = 512
D = 2048
NCOL = 896
EPS = 1e-06
THETA = 500000.0
LOG2E = 1.4426950408889634
F32 = jnp.float32
BF16 = jnp.bfloat16
MESH = pl.DeviceIdType.MESH
VMEM_SPEC = pl.BlockSpec(memory_space=pltpu.VMEM)
ANY_SPEC = pl.BlockSpec(memory_space=pl.ANY)
VMEM_LIMIT = 60 * 1024 * 1024


def remote(src, dst, send_sem, recv_sem, device):
    return pltpu.make_async_remote_copy(
        src_ref=src,
        dst_ref=dst,
        send_sem=send_sem,
        recv_sem=recv_sem,
        device_id=device,
        device_id_type=MESH,
    )


def meet(devices):
    barrier = pltpu.get_barrier_semaphore()
    for device in devices:
        pl.semaphore_signal(barrier, inc=1, device_id=device, device_id_type=MESH)
    pl.semaphore_wait(barrier, len(devices))


def dot(a, b):
    return jnp.dot(a, b, preferred_element_type=F32)


def dot_nt(a, b):
    return lax.dot_general(a, b, (((1,), (1,)), ((), ())), preferred_element_type=F32)


def rotary_tables():
    i = np.arange(AK // 2, dtype=np.float64)
    freq = THETA ** (-(i * 2.0 / AK))
    freq = np.tile(freq, 4)[None, :]
    within = np.arange(LEN, dtype=np.float64)[:, None] * freq
    starts = np.arange(NZ * NX, dtype=np.float64)[:, None] * LEN * freq
    tables = [f(v) for v in (within, starts) for f in (np.cos, np.sin)]
    return jnp.asarray(np.concatenate(tables, axis=0).astype(np.float32))


def exact_cumulative(triangle, logs):
    first = logs.astype(BF16)
    rest = logs - first.astype(F32)
    second = rest.astype(BF16)
    third = (rest - second.astype(F32)).astype(BF16)
    return dot(triangle, first) + dot(triangle, second) + dot(triangle, third)


def recurrence(rec_ref, leak_ref, decay_ref, out_ref, read_ref, state_ref, done):
    blocks = LEN // BLOCK
    raw_q = rec_ref[:, 0:128].astype(F32)
    rq = raw_q / (1.0 + jnp.exp(-raw_q))
    value = rec_ref[:, 384:512]
    value_t = value.astype(F32).T.astype(BF16)
    row = lax.broadcasted_iota(jnp.int32, (256, 256), 0)
    col = lax.broadcasted_iota(jnp.int32, (256, 256), 1)
    same = (row // BLOCK) == (col // BLOCK)
    upper = lax.broadcasted_iota(jnp.int32, (128, 1), 0) < BLOCK
    total_out = None
    for side in range(2):
        raw = rec_ref[:, 128 * (side + 1) : 128 * (side + 2)].astype(F32)
        key = leak_ref[side : side + 1, :] / (1.0 + jnp.exp(raw))
        added_log = jnp.concatenate(
            [
                jnp.broadcast_to(decay_ref[4 * side + k : 4 * side + k + 1, :], (128, 128)).T
                for k in range(4)
            ],
            axis=0,
        )
        logs = jnp.log1p(-key) + added_log
        mask = same & ((row >= col) if side == 0 else (row <= col))
        triangle = mask.astype(F32).astype(BF16)
        cum = jnp.concatenate(
            [exact_cumulative(triangle, logs[256 * h : 256 * (h + 1)]) for h in range(2)], axis=0
        )
        cum3 = cum.reshape(blocks, BLOCK, 128)
        at_mid, at_last = (BLOCK // 2 - 1, BLOCK - 1) if side == 0 else (BLOCK // 2, 0)
        middle = cum3[:, at_mid : at_mid + 1, :]
        last = cum3[:, at_last : at_last + 1, :]
        key3, rq3 = key.reshape(cum3.shape), rq.reshape(cum3.shape)
        qs = (rq3 * jnp.exp(cum3 - middle)).reshape(LEN, 128).astype(BF16)
        ks = (key3 * jnp.exp(middle - cum3)).reshape(LEN, 128).astype(BF16)
        kl = (key3 * jnp.exp(last - cum3)).reshape(LEN, 128)
        qc = (rq3 * jnp.exp(cum3)).reshape(LEN, 128).astype(BF16)
        within = []
        for h in range(2):
            part = slice(256 * h, 256 * (h + 1))
            scores = jnp.where(mask, dot_nt(qs[part], ks[part]), 0.0).astype(BF16)
            within.append(dot(scores, value[part]))
        order = range(blocks) if side == 0 else reversed(range(blocks))
        state = jnp.zeros((128, 128), F32)
        carried, before = [None] * blocks, [None] * blocks
        running = jnp.zeros((1, 128), F32)
        for b in order:
            carried[b] = dot_nt(qc[BLOCK * b : BLOCK * (b + 1)], state.astype(BF16))
            pair = b // 2
            keys = kl[128 * pair : 128 * (pair + 1)]
            keys = jnp.where(upper if b % 2 == 0 else ~upper, keys, 0.0).astype(BF16)
            added = dot(value_t[:, 128 * pair : 128 * (pair + 1)], keys)
            before[b] = running
            running = running + last[b]
            state = state * jnp.exp(last[b]) + added
        out = jnp.concatenate(within, axis=0) + jnp.concatenate(carried, axis=0)
        total_out = out if total_out is None else total_out + out
        reach = (cum3 + jnp.stack(before, axis=0)).reshape(LEN, 128)
        read_ref[side] = (rq * jnp.exp(reach)).astype(BF16)
        state_ref[side, 0:128, :] = state.astype(BF16)
        state_ref[side, 128:144, :] = jnp.broadcast_to(jnp.exp(running), (16, 128)).astype(BF16)
        done(side)
    out_ref[...] = total_out


def flash(plan, kvbuf, qz, acc, peak):
    ones = jnp.ones((16, 256), BF16)
    tiles, ahead, behind = [], {}, {}
    for item in plan:
        if item[0] == "pre":
            ahead.setdefault(len(tiles), []).append(item[1])
        elif item[0] == "post":
            behind.setdefault(len(tiles) - 1, []).append(item[1])
        else:
            tiles += [(item[0], k, item[1], item[2]) for k in (item[3:] or range(4))]
    count = len(tiles)
    tops, olds, sums = [None] * count, [None] * count, [None] * count
    scores, weights = [{} for _ in tiles], [{} for _ in tiles]

    def has(i, n):
        return 0 <= i < count and n < len(tiles[i][2])

    def score(i, n):
        q, k, pieces, first = tiles[i]
        if n == 0 and not first:
            before = [b for b in range(max(0, i - 2), i) if tiles[b][:2] == (q, k)]
            olds[i] = tops[i] = tops[before[-1]] if before else peak[q, k, 0:1, :]
        r, s = pieces[n]
        keys = jnp.concatenate([kvbuf[r, 2 * s, 0:128, :], kvbuf[r, 2 * s + 1, 0:128, :]], axis=0)
        scores[i][n] = dot(keys, qz[q, k])
        here = jnp.max(scores[i][n], axis=0, keepdims=True)
        tops[i] = here if tops[i] is None else jnp.maximum(tops[i], here)

    def weigh(i, n):
        weights[i][n] = jnp.exp2(scores[i].pop(n) - tops[i]).astype(BF16)

    def gather(i, n):
        q, k, pieces, first = tiles[i]
        r, s = pieces[n]
        values = [kvbuf[r, 2 * s, 128:256, :], kvbuf[r, 2 * s + 1, 128:256, :]]
        values = jnp.concatenate(values, axis=1)
        term = dot(jnp.concatenate([values, ones], axis=0), weights[i].pop(n))
        sums[i] = term if sums[i] is None else sums[i] + term
        if n == len(pieces) - 1:
            if first:
                acc[q, k] = sums[i]
            else:
                acc[q, k] = acc[q, k] * jnp.exp2(olds[i] - tops[i]) + sums[i]
            peak[q, k] = jnp.broadcast_to(tops[i], (8, 256))

    longest = max(len(t[2]) for t in tiles)
    for i in range(-2, count):
        for call in ahead.get(i + 2, []):
            call()
        for n in range(longest):
            for stage, at in ((score, i + 2), (weigh, i + 1), (gather, i)):
                if has(at, n):
                    stage(at, n)
        for call in behind.get(i, []):
            call()


REACH = (2, 1, 3, 0)


def layer_kernel(
    lam_ref, tok_ref, *refs,
):
    small, weights, (wrec_ref, watt_ref, out_ref) = refs[:6], refs[6:13], refs[13:16]
    (
        gain_ref, tables, leak_ref, decay_ref, attgain_ref, recgain_ref,
        xbuf, wbuf, recraw, recout, read,
        kvbuf, qown, qbuf, qz, acc, peak, farout, farin, farouts, farins, nearout, nearin,
        nearouts, nearins, stbuf, totals, inside, chain_in, chain_out, half_in, half_out,
        mixrec, mixatt, gotrec, gotatt, wr, wa,
        wsem, y_send, y_recv, k_send, k_recv, q_send, q_recv, s_send, s_recv,
        c_send, c_recv, h_send, h_recv, f_send, f_recv, n_send, n_recv,
        t_send, t_recv,
    ) = refs[16:]
    z, x, t = lax.axis_index("sp_0"), lax.axis_index("sp_1"), lax.axis_index("tp")
    y, c = t // 2, t % 2
    right = lax.rem(y + 1, NY) * 2 + c
    left = lax.rem(y + NY - 1, NY) * 2 + c
    far = lax.rem(y + 2, NY) * 2 + c
    partner = 2 * y + 1 - c
    up = {"sp_0": lax.rem(z + 1, NZ)}
    down = {"sp_0": lax.rem(z + NZ - 1, NZ)}
    beside = [None] + [{"sp_1": lax.rem(x + p, NX)} for p in range(1, NX)]
    mates = [None] + [lax.rem(t + d, 8) for d in range(1, 8)]

    own_load = pltpu.make_async_copy(tok_ref, xbuf.at[t], wsem.at[0])
    own_load.start()
    loads = [
        pltpu.make_async_copy(w, wbuf.at[:, pl.ds(128 * k, 128)], wsem.at[1])
        for k, w in enumerate(weights)
    ]
    homes = (gain_ref, tables, leak_ref, decay_ref, attgain_ref, recgain_ref)
    small_loads = [
        pltpu.make_async_copy(a, b, wsem.at[4 + k]) for k, (a, b) in enumerate(zip(small, homes))
    ]
    late_loads = [
        pltpu.make_async_copy(wrec_ref, wr, wsem.at[2]),
        pltpu.make_async_copy(watt_ref, wa, wsem.at[3]),
    ]
    for load in loads + small_loads:
        load.start()
    meet([up, down] + beside[1:] + [{"tp": m} for m in mates[1:]])

    def drain(ref, sem):
        pltpu.make_async_copy(ref, ref, sem).wait()

    own_load.wait()

    quarter_rows = ROWS // 4

    def rows_at(slot, first, count):
        return xbuf.at[slot, pl.ds(first * quarter_rows, count * quarter_rows)]

    def launch(slot, first, count, number, device):
        here = rows_at(slot, first, count)
        remote(here, here, y_send, y_recv.at[number], {"tp": device}).start()

    def arrived(slot, first, count, number):
        drain(rows_at(slot, first, count), y_recv.at[number])

    launch(t, 0, 1, 0, right)
    launch(t, 3, 1, 3, left)
    launch(t, 1, 1, 1, right)
    launch(t, 2, 1, 4, left)
    launch(t, 2, 2, 2, right)
    launch(t, 0, 2, 5, left)
    launch(t, 0, 4, 8, partner)
    for load in small_loads:
        load.wait()
    drain(wbuf, wsem.at[1])

    block = z * NX + x
    cb = tables[pl.ds(2 * LEN + block, 1), :]
    sb = tables[pl.ds(2 * LEN + NZ * NX + block, 1), :]
    lane = lax.broadcasted_iota(jnp.int32, (1, 128), 1)
    low = lax.rem(lane, 64) < 32

    def turned(v, cosine, sine):
        other = jnp.where(low, pltpu.roll(v, 96, 1), pltpu.roll(v, 32, 1))
        return v * cosine + other * sine

    def arrival(step, j):
        return k_recv.at[4 * step + j if step < 3 else 12]

    def start_right(step, j):
        src = kvbuf.at[(NZ - step) % NZ, j]
        remote(src, kvbuf.at[NZ - 1 - step, j], k_send, arrival(step, j), up).start()

    def start_left(step, j):
        src = kvbuf.at[step, j]
        remote(src, kvbuf.at[step + 1, j], k_send, arrival(step, j), down).start()

    def forward(step, j):
        drain(kvbuf.at[0, 0:2], arrival(step - 1, j))
        if step < 3 or j < 2:
            start_right(step, j)
        if step < 3 or j >= 2:
            start_left(step, j)

    def process(yy, j):
        pair = xbuf[pl.ds(2 * yy, 2)].reshape(2 * ROWS, D).astype(F32)
        scale = lax.rsqrt(jnp.mean(pair * pair, axis=1, keepdims=True) + EPS)
        normed = (pair * scale * gain_ref[...]).astype(BF16)
        out = dot(normed, wbuf[...])
        rows = pl.ds(pl.multiple_of(yy * 128, 128), 128)
        ca = tables[rows, :]
        sa = tables[pl.ds(pl.multiple_of(LEN + yy * 128, 128), 128), :]
        cosine = ca * cb - sa * sb
        sine = sa * cb + ca * sb
        signed = jnp.where(low, -sine, sine)
        raw = out[:, 512:].astype(BF16).astype(F32)
        kvbuf[0, j, 0:128, :] = turned(raw[:, 128:256], cosine, signed).astype(BF16)
        kvbuf[0, j, 128:256, :] = raw[:, 256:384].T.astype(BF16)
        query = turned(raw[:, 0:128], cosine, signed) * (AK**-0.5 * LOG2E)
        qown[j] = query.T.astype(BF16)
        recraw[rows, :] = out[:, :512].astype(BF16)
        start_right(0, j)
        start_left(0, j)
        for p in (2, 1, 3):
            remote(
                qown.at[j], qbuf.at[NX - p, j], q_send, q_recv.at[NX - p], beside[p]
            ).start()

    arrived(partner, 0, 4, 8)
    process(y, 0)
    arrived(left, 0, 1, 0)
    launch(left, 0, 1, 6, right)
    arrived(right, 3, 1, 3)
    launch(right, 3, 1, 7, left)
    arrived(left, 1, 1, 1)
    launch(left, 1, 1, 6, right)
    launch(left, 0, 2, 9, partner)
    arrived(right, 2, 1, 4)
    launch(right, 2, 1, 7, left)
    launch(right, 2, 2, 11, partner)
    forward(1, 0)
    arrived(left, 2, 2, 2)
    launch(left, 2, 2, 10, partner)
    arrived(right, 0, 2, 5)
    launch(right, 0, 2, 12, partner)
    mate_l, mate_r, mate_far = left + 1 - 2 * c, right + 1 - 2 * c, far + 1 - 2 * c
    arrived(mate_l, 0, 2, 9)
    arrived(mate_l, 2, 2, 10)
    process(left // 2, 1)
    arrived(mate_r, 2, 2, 11)
    arrived(mate_r, 0, 2, 12)
    process(right // 2, 2)
    forward(2, 0)
    arrived(far, 0, 2, 6)
    launch(far, 0, 2, 13, partner)
    arrived(far, 2, 2, 7)
    launch(far, 2, 2, 14, partner)
    arrived(mate_far, 0, 2, 13)
    arrived(mate_far, 2, 2, 14)
    process(far // 2, 3)
    for load in late_loads:
        load.start()
    forward(1, 1)

    def one_side(side):
        for p in range(1, NX):
            remote(
                stbuf.at[0, side], stbuf.at[NX - p, side], s_send, s_recv, beside[p]
            ).start()
        if side == 0:
            forward(1, 2)

    recurrence(recraw, leak_ref, decay_ref, recout, read, stbuf.at[0], one_side)

    upper = lax.broadcasted_iota(jnp.int32, (128, 1), 0) < AK

    def spread(q, source):
        for h in range(2):
            piece = jnp.concatenate([source(2 * h), source(2 * h + 1)], axis=1).astype(F32)
            qz[q, h] = jnp.where(upper, piece, 0.0).astype(BF16)
            qz[q, 2 + h] = jnp.where(upper, 0.0, piece).astype(BF16)

    def pieces(*slots):
        return [(r, s) for r in slots for s in range(2)]

    spread(3, lambda j: qown[j])

    def queries(q):
        def call():
            p = REACH[q]
            drain(qbuf.at[p], q_recv.at[p])
            spread(q, lambda j: qbuf[p, j])

        return call

    def join_states():
        drain(stbuf.at[1:4], s_recv)
        for side in range(2):
            order = range(NX) if side == 0 else reversed(range(NX))
            total_s, total_d = jnp.zeros((128, 128), F32), jnp.ones((1, 128), F32)
            inside_s, inside_d = total_s, total_d
            for k in order:
                rel = lax.rem(k - x + NX, NX)
                piece_s = stbuf[rel, side, 0:128, :].astype(F32)
                piece_d = stbuf[rel, side, 128:144, :].astype(F32)[0:1, :]
                total_s = total_s * piece_d + piece_s
                total_d = total_d * piece_d
                passed = (k < x) if side == 0 else (k > x)
                inside_s = jnp.where(passed, total_s, inside_s)
                inside_d = jnp.where(passed, total_d, inside_d)
            totals[side, 0:128, :] = total_s
            totals[side, 128:136, :] = jnp.broadcast_to(total_d, (8, 128))
            inside[side, 0:128, :] = inside_s
            inside[side, 128:136, :] = jnp.broadcast_to(inside_d, (8, 128))
        chain(0)

    quarter = NZ // 2
    place = (lax.rem(z, quarter), quarter - 1 - lax.rem(z, quarter))
    giver = (quarter - 1, quarter)
    takes = (z >= quarter, z < quarter)

    for side in range(2):

        @pl.when(place[side] == 0)
        def _():
            chain_in[side, 0:128, :] = jnp.zeros((128, 128), BF16)
            chain_in[side, 128:144, :] = jnp.ones((16, 128), BF16)

        @pl.when(jnp.logical_not(takes[side]))
        def _():
            half_in[side] = jnp.zeros((128, 128), BF16)

    def chain_copy(side):
        return remote(
            chain_out.at[side], chain_in.at[side], c_send.at[side], c_recv.at[side],
            up if side == 0 else down,
        )

    def half_copy(side, k):
        device = quarter + k if side == 0 else quarter - 1 - k
        return remote(
            half_out.at[side], half_in.at[side], h_send.at[side], h_recv.at[side],
            {"sp_0": device},
        )

    def chain(hop):
        for side in range(2):

            @pl.when(place[side] == hop)
            def _():
                if hop > 0:
                    chain_copy(side).wait_recv()
                entered = chain_in[side].astype(F32)
                decay = totals[side, 128:129, :]
                state = entered[0:128, :] * decay + totals[side, 0:128, :]
                if hop < quarter - 1:
                    chain_out[side, 0:128, :] = state.astype(BF16)
                    chain_out[side, 128:144, :] = (entered[128:144, :] * decay).astype(BF16)
                    chain_copy(side).start()
                else:

                    @pl.when(z == giver[side])
                    def _():
                        half_out[side] = state.astype(BF16)
                        for k in range(quarter):
                            half_copy(side, k).start()

    row8 = lax.broadcasted_iota(jnp.int32, (8, 256), 0)

    def statistics(tops, totals_of):
        first = jnp.where(row8 == 0, tops[0], totals_of[0])
        return jnp.where(row8 < 2, first, jnp.where(row8 == 2, tops[1], totals_of[1]))

    def pack(q, m, out, stat):
        tops, sums = [], []
        for h in range(2):
            k = 2 * m + h
            tops.append(peak[q, k, 0:1, :])
            sums.append(acc[q, k, 128:129, :])
            out[h] = (acc[q, k, 0:128, :] * (1.0 / sums[h])).astype(BF16)
        stat[...] = statistics(tops, sums)

    def pack_merged(q, m, out, stat, other, others):
        tops, sums = [], []
        for h in range(2):
            k = 2 * m + h
            top_a, top_b = peak[q, k, 0:1, :], others[2 * h : 2 * h + 1, :]
            top = jnp.maximum(top_a, top_b)
            scale = jnp.exp2(top_a - top)
            share = others[2 * h + 1 : 2 * h + 2, :] * jnp.exp2(top_b - top)
            total = acc[q, k, 128:129, :] * scale + share
            inverse = 1.0 / total
            merged = acc[q, k, 0:128, :] * (scale * inverse)
            merged = merged + other[h].astype(F32) * (share * inverse)
            out[h] = merged.astype(BF16)
            tops.append(top)
            sums.append(total)
        stat[...] = statistics(tops, sums)

    def far_copies(m):
        device = beside[1] if m == 0 else beside[3]
        return [
            remote(farout.at[m], farin.at[m], f_send.at[0], f_recv.at[m, 0], device),
            remote(farouts.at[m], farins.at[m], f_send.at[1], f_recv.at[m, 1], device),
        ]

    def near_copies(w, m):
        device = beside[1] if w == 0 else beside[3]
        return [
            remote(nearout.at[w, m], nearin.at[w, m], n_send.at[0], n_recv.at[w, m, 0], device),
            remote(nearouts.at[w, m], nearins.at[w, m], n_send.at[1], n_recv.at[w, m, 1], device),
        ]

    def post(pair):
        for copy in pair:
            copy.start()

    def received(pair):
        for copy in pair:
            copy.wait_recv()

    def give_far():
        for m in range(2):
            pack(0, m, farout.at[m], farouts.at[m])
            post(far_copies(m))

    def give_near(w, m):
        def call():
            pack(w + 1, m, nearout.at[w, m], nearouts.at[w, m])
            post(near_copies(w, m))

        return call

    def merge_near(w, m):
        received(far_copies(w))
        pack_merged(w + 1, m, nearout.at[w, m], nearouts.at[w, m], farin.at[w], farins.at[w])
        post(near_copies(w, m))

    def pre(call, *args):
        return ("pre", lambda: call(*args))

    flash(
        [
            (3, pieces(0), True),
            ("pre", queries(0)), (0, pieces(0), True),
            ("pre", queries(1)), pre(forward, 1, 3), pre(forward, 3, 0), (1, pieces(0), True),
            ("pre", queries(2)), pre(forward, 2, 1), (2, pieces(0), True),
            (0, pieces(7, 1), False),
            (1, pieces(7, 1), False),
            pre(forward, 2, 2), (2, pieces(7, 1), False),
            pre(forward, 2, 3), (3, pieces(7, 1), False),
            pre(join_states), pre(forward, 3, 1), (0, pieces(6, 2), False),
            pre(forward, 3, 2), (1, pieces(6, 2), False),
            (2, pieces(6, 2), False, 0, 1),
            pre(forward, 3, 3), pre(chain, 1), (2, pieces(6, 2), False, 2, 3),
            (1, pieces(5, 3), False),
            pre(chain, 2), (0, pieces(5, 3), False),
            pre(drain, kvbuf.at[0], arrival(3, 0)), (0, pieces(4), False),
            ("post", give_far),
            (1, pieces(4), False),
            ("post", give_near(0, 1)),
            (2, pieces(5, 3, 4), False),
            ("post", give_near(1, 0)),
            pre(chain, 3), (3, pieces(6, 2), False),
            (3, pieces(5, 3, 4), False),
        ],
        kvbuf, qz, acc, peak,
    )
    merge_near(0, 0)
    merge_near(1, 1)

    for side in range(2):

        @pl.when(takes[side])
        def _():
            half_copy(side, 0).wait_recv()

    out = recout[...]
    for side in range(2):
        entered = chain_in[side].astype(F32)
        entry = entered[0:128, :] + half_in[side].astype(F32) * entered[128:129, :]
        entry = entry * inside[side, 128:129, :] + inside[side, 0:128, :]
        out = out + dot_nt(read[side], entry.astype(BF16))
    out = out * lax.rsqrt(jnp.mean(out * out, axis=1, keepdims=True) + EPS) * recgain_ref[...]
    mixrec[...] = out.astype(BF16)

    def rows_of(device):
        return pl.ds(pl.multiple_of(device * ROWS, ROWS), ROWS)

    def deal(source, got, which, devices):
        for device in devices:
            remote(
                source.at[rows_of(device), :], got.at[t], t_send.at[which], t_recv.at[which],
                {"tp": device},
            ).start()

    deal(mixrec, gotrec, 0, mates[1:])
    gotrec[t] = mixrec[rows_of(t), :]

    drain(xbuf.at[0:7], y_send)
    drain(kvbuf.at[0:7], k_send)
    drain(qbuf.at[0:3], q_send)
    drain(stbuf.at[0:3], s_send)
    drain(farout, f_send.at[0])
    drain(farouts, f_send.at[1])
    for load in late_loads:
        load.wait()
    for side in range(2):

        @pl.when(place[side] < quarter - 1)
        def _():
            chain_copy(side).wait_send()

        @pl.when(z == giver[side])
        def _():
            drain(qbuf.at[0], h_send.at[side])

    lam = lam_ref[0:1, 0:1]
    for w, m in ((0, 1), (1, 0), (0, 0), (1, 1)):
        received(near_copies(w, m))
    for h in (1, 0):
        maps = []
        for m in range(2):
            k = 2 * m + h
            tops = [peak[3, k, 0:1, :]] + [nearins[w, m, 2 * h : 2 * h + 1, :] for w in range(2)]
            sums = [acc[3, k, 128:129, :]] + [nearins[w, m, 2 * h + 1 : 2 * h + 2, :] for w in range(2)]
            top = jnp.maximum(jnp.maximum(tops[0], tops[1]), tops[2])
            shares = [a * jnp.exp2(b - top) for a, b in zip(sums, tops)]
            inverse = 1.0 / (shares[0] + shares[1] + shares[2])
            value = acc[3, k, 0:128, :] * (jnp.exp2(tops[0] - top) * inverse)
            for w in range(2):
                value = value + nearin[w, m, h].astype(F32) * (shares[w + 1] * inverse)
            maps.append(value)
        mixed = maps[0] - lam * maps[1]
        mixed = mixed * lax.rsqrt(jnp.mean(mixed * mixed, axis=0, keepdims=True) + EPS)
        rows = (mixed.T * attgain_ref[...]).astype(BF16)
        for half_of, yy in zip(range(2), ((y, left // 2), (right // 2, far // 2))[h]):
            at = pl.ds(pl.multiple_of(yy * 128, 128), 128)
            mixatt[at, :] = rows[128 * half_of : 128 * (half_of + 1), :]
        deal(mixatt, gotatt, 1, ((left, mate_l, partner), (far, mate_far, right, mate_r))[h])
    gotatt[t] = mixatt[rows_of(t), :]
    drain(nearout, n_send.at[0])
    drain(nearouts, n_send.at[1])
    drain(gotrec.at[0:7], t_recv.at[0])
    rec_term = dot(jnp.concatenate([gotrec[k] for k in range(8)], axis=1), wr[...])
    drain(gotatt.at[0:7], t_recv.at[1])
    att_term = dot(jnp.concatenate([gotatt[k] for k in range(8)], axis=1), wa[...])
    out_ref[...] = (rec_term + att_term).astype(BF16)
    drain(gotrec.at[0:7], t_send.at[0])
    drain(gotatt.at[0:7], t_send.at[1])


def on_device(
    tokens, norm_gain, rec_query, fwd_gate, bwd_gate, rec_value, gate_leak, log_decay, rec_gain,
    att_query, att_key, att_value, lambdas, att_gain, out_rec, out_att,
):
    weights = (rec_query, fwd_gate, bwd_gate, rec_value, att_query, att_key, att_value)
    dma = pltpu.SemaphoreType.DMA
    return pl.pallas_call(
        layer_kernel,
        out_shape=jax.ShapeDtypeStruct((ROWS, D), BF16),
        in_specs=[VMEM_SPEC] + [ANY_SPEC] * 16,
        out_specs=VMEM_SPEC,
        scratch_shapes=[
            pltpu.VMEM((1, D), F32),
            pltpu.VMEM((2 * LEN + 2 * NZ * NX, 128), F32),
            pltpu.VMEM((2, 128), F32),
            pltpu.VMEM((8, 128), F32),
            pltpu.VMEM((1, 128), F32),
            pltpu.VMEM((1, 128), F32),
            pltpu.VMEM((8, ROWS, D), BF16),
            pltpu.VMEM((D, NCOL), BF16),
            pltpu.VMEM((LEN, 512), BF16),
            pltpu.VMEM((LEN, 128), F32),
            pltpu.VMEM((2, LEN, 128), BF16),
            pltpu.VMEM((NZ, 4, 256, 128), BF16),
            pltpu.VMEM((4, 128, 128), BF16),
            pltpu.VMEM((NX, 4, 128, 128), BF16),
            pltpu.VMEM((NX, 4, 128, 256), BF16),
            pltpu.VMEM((NX, 4, 144, 256), F32),
            pltpu.VMEM((NX, 4, 8, 256), F32),
            pltpu.VMEM((2, 2, 128, 256), BF16),
            pltpu.VMEM((2, 2, 128, 256), BF16),
            pltpu.VMEM((2, 8, 256), F32),
            pltpu.VMEM((2, 8, 256), F32),
            pltpu.VMEM((2, 2, 2, 128, 256), BF16),
            pltpu.VMEM((2, 2, 2, 128, 256), BF16),
            pltpu.VMEM((2, 2, 8, 256), F32),
            pltpu.VMEM((2, 2, 8, 256), F32),
            pltpu.VMEM((NX, 2, 144, 128), BF16),
            pltpu.VMEM((2, 136, 128), F32),
            pltpu.VMEM((2, 136, 128), F32),
            pltpu.VMEM((2, 144, 128), BF16),
            pltpu.VMEM((2, 144, 128), BF16),
            pltpu.VMEM((2, 128, 128), BF16),
            pltpu.VMEM((2, 128, 128), BF16),
            pltpu.VMEM((LEN, 128), BF16),
            pltpu.VMEM((LEN, 128), BF16),
            pltpu.VMEM((8, ROWS, 128), BF16),
            pltpu.VMEM((8, ROWS, 128), BF16),
            pltpu.VMEM((1024, D), BF16),
            pltpu.VMEM((1024, D), BF16),
            dma((10,)), dma, dma((15,)), dma, dma((13,)), dma, dma((NX,)), dma, dma,
            dma((2,)), dma((2,)), dma((2,)), dma((2,)),
            dma((2,)), dma((2, 2)), dma((2,)), dma((2, 2, 2)), dma((2,)), dma((2,)),
        ],
        compiler_params=pltpu.CompilerParams(
            collective_id=0, has_side_effects=True, vmem_limit_bytes=VMEM_LIMIT,
        ),
        name="layer",
    )(
        lambdas.reshape(1, 1), tokens, norm_gain.reshape(1, D), rotary_tables(), gate_leak,
        log_decay.reshape(8, 128), att_gain.reshape(1, 128), rec_gain.reshape(1, 128), *weights,
        out_rec, out_att,
    )


def solution(mesh):
    torus = Mesh(mesh.devices.reshape(NZ, NX, mesh.shape["tp"]), SP_TP)
    tp = P(None, "tp")
    in_specs = (
        P(SP_TP, None), P(), tp, tp, tp, tp, tp, P(None, SP, "tp"), P(), tp, tp, tp, P("tp"), P(),
        P(), P(),
    )
    return jax.shard_map(
        on_device, mesh=torus, in_specs=in_specs, out_specs=P(SP_TP, None), check_vma=False
    )
```
